256 devices in a mesh: sp: 32 (over z, x), tp: 8 (over y, core).
Axes of the slice: x: 4, y: 4, z: 8, core: 2. Of those that a mesh axis runs over, the one named last changes fastest.
Arguments:
- tokens: bfloat16 [32768, 2048], P('sp', 'tp'), may hold values from -70 to 70
- w_query: bfloat16 [2048, 1024], P(None, 'tp'), may hold values from -0.125 to 0.125
- w_key: bfloat16 [2048, 1024], P(None, 'tp'), may hold values from -0.125 to 0.125
- w_value: bfloat16 [2048, 1024], P(None, 'tp'), may hold values from -0.125 to 0.125
- w_delta_gate: bfloat16 [2048, 1024], P(None, 'tp'), may hold values from -0.125 to 0.125
- w_glu_value: bfloat16 [2048, 1024], P(None, 'tp'), may hold values from -0.125 to 0.125
- w_glu_gate: bfloat16 [2048, 1024], P(None, 'tp'), may hold values from -0.125 to 0.125
- w_conv_gate: bfloat16 [2048, 1024], P(None, 'tp'), may hold values from -0.125 to 0.125
- w_beta: bfloat16 [2048, 8], replicated, may hold values from -0.125 to 0.125
- w_decay: bfloat16 [2048, 8], replicated, may hold values from -0.125 to 0.125
- decay_log: float32 [8], replicated, may hold values from -12 to -3
- head_gain: float32 [128], replicated, may hold values from 0.1 to 1.9
- conv_taps: bfloat16 [31, 1024], P(None, 'tp'), may hold values from -2.5 to 2.5
- ln_gain: float32 [1024], P('tp'), may hold values from 0.1 to 1.9
- ln_shift: float32 [1024], P('tp'), may hold values from -3 to 3
- out_delta: bfloat16 [1024, 2048], P('tp'), may hold values from -0.125 to 0.125
- out_conv: bfloat16 [1024, 2048], P('tp'), may hold values from -0.125 to 0.125
Outputs:
- mixed_out: bfloat16 [32768, 2048], P(('sp', 'tp'))
The draws below stay inside these ranges and needn't reach their ends.
All inputs are finite; a program needn't handle non-finite values.
Results may differ from the reference program's by a relative error of at most 0.024.
Values may be sent and summed in bfloat16 or wider, within the bound.
No kernel may reach another device: no remote copies, remote signals or barrier semaphores. Data moves between devices by JAX's collectives and lax.ppermute only.
A program may use at most 64 MiB of HBM per device.

```python
import jax
import jax.numpy as jnp
from jax import lax

D = 2048
HEADS = 8
DK = 128
CV = 1024
KERNEL = 31
SPAN = 64
TOKENS = 32768
N_TP = 8


def draw_tokens(key, part):
    keys = jax.random.split(key, 3)
    span_rows = 4 * SPAN
    groups = (TOKENS + span_rows - 1) // span_rows
    shifts = jnp.clip(jax.random.normal(keys[1], (groups, D), jnp.float32), -6.0, 6.0) * 1.5
    shifts = jnp.repeat(shifts, span_rows, axis=0)[:TOKENS]
    noise = jnp.clip(jax.random.normal(keys[0], (TOKENS, D), jnp.float32), -6.0, 6.0)
    spread = 0.7
    scales = jnp.exp(jax.random.uniform(keys[2], (TOKENS, 1), jnp.float32, -spread, spread))
    return ((noise + shifts) * scales).astype(jnp.bfloat16)


def draw_decay_log(key, part):
    keys = jax.random.split(key, 3)
    order = jax.random.permutation(keys[0], HEADS)
    fast_heads = HEADS // 2
    slow_rate = jax.random.uniform(keys[1], (HEADS,), jnp.float32, 0.3, 1.0) * 2.3 / TOKENS
    fast_rate = jax.random.uniform(keys[2], (HEADS,), jnp.float32, 0.015, 0.04)
    return jnp.log(jnp.where(order < fast_heads, fast_rate, slow_rate)).astype(jnp.float32)


def draw_conv_taps(key, part):
    keys = jax.random.split(key, 2)
    noise = jnp.clip(jax.random.normal(keys[0], (KERNEL, CV), jnp.float32), -4.0, 4.0)
    spread = 1.2
    levels = jnp.exp(jax.random.uniform(keys[1], (16,), jnp.float32, -spread, spread))
    group_ids = jnp.arange(CV) * 16 // CV
    column_scale = jnp.take(levels, group_ids)
    return (noise * column_scale[None, :] * KERNEL ** (-0.5)).astype(jnp.bfloat16)


def level_of(key, shape, shards, smallest, high):
    def one(axis_at, shards_of):
        heights = jax.random.uniform(jax.random.fold_in(jax.random.fold_in(key, 6), axis_at), (shards_of,), jnp.float32, smallest / len(shards), high / len(shards))
        return jnp.repeat(jnp.exp(heights), shape[axis_at] // shards_of).reshape((-1,) + (1,) * (len(shape) - axis_at - 1))

    loudness = one(*shards[0])
    for cut in shards[1:]:
        loudness = loudness * one(*cut)
    return loudness


def gaussian(own_key, shape, scale, reach, shards=(), kind=jnp.bfloat16):
    entries = scale * jax.random.normal(own_key, shape, jnp.float32)
    if shards:
        entries = entries * level_of(own_key, shape, shards, -0.22, 0.18)
    return jnp.clip(entries, -reach, reach).astype(kind)


def setup_inputs(seed: int = 0) -> dict:
    splits = jax.random.split(jax.random.key(seed), 18)
    tokens = draw_tokens(jax.random.fold_in(splits[17], 71), 0)
    w_query = gaussian(splits[1], (D, HEADS * DK), D ** -0.5, 0.125, ((1, 8),))
    w_key = gaussian(splits[2], (D, HEADS * DK), D ** -0.5, 0.125, ((1, 8),))
    w_value = gaussian(splits[3], (D, HEADS * DK), D ** -0.5, 0.125, ((1, 8),))
    w_delta_gate = gaussian(splits[4], (D, HEADS * DK), D ** -0.5, 0.125, ((1, 8),))
    w_glu_value = gaussian(splits[5], (D, CV), D ** -0.5, 0.125, ((1, 8),))
    w_glu_gate = gaussian(splits[6], (D, CV), D ** -0.5, 0.125, ((1, 8),))
    w_conv_gate = gaussian(splits[7], (D, CV), D ** -0.5, 0.125, ((1, 8),))
    w_beta = gaussian(splits[8], (D, HEADS), D ** -0.5, 0.125)
    w_decay = gaussian(splits[9], (D, HEADS), D ** -0.5, 0.125)
    decay_log = draw_decay_log(jax.random.fold_in(splits[17], 71), 0)
    head_gain = jnp.clip(1.0 + 0.18 * jax.random.normal(splits[11], (DK,), jnp.float32), 0.1, 1.9)
    conv_taps = draw_conv_taps(jax.random.fold_in(splits[17], 71), 0)
    ln_gain = jnp.clip(1.0 + 0.18 * jax.random.normal(splits[13], (CV,), jnp.float32), 0.1, 1.9)
    ln_shift = gaussian(splits[14], (CV,), 0.5, 3.0, ((0, 8),), jnp.float32)
    out_delta = gaussian(splits[15], (HEADS * DK, D), (HEADS * DK + CV) ** -0.5, 0.125, ((0, 8),))
    out_conv = gaussian(splits[16], (CV, D), (HEADS * DK + CV) ** -0.5, 0.125, ((0, 8),))
    return {"tokens": tokens, "w_query": w_query, "w_key": w_key, "w_value": w_value, "w_delta_gate": w_delta_gate, "w_glu_value": w_glu_value, "w_glu_gate": w_glu_gate, "w_conv_gate": w_conv_gate, "w_beta": w_beta, "w_decay": w_decay, "decay_log": decay_log, "head_gain": head_gain, "conv_taps": conv_taps, "ln_gain": ln_gain, "ln_shift": ln_shift, "out_delta": out_delta, "out_conv": out_conv}


TINY_NORM = 1e-06
TINY_VAR = 1e-05
HIGHEST = lax.Precision.HIGHEST

def head_rule(query, keys, values, strength, log_decay):
    blocks = query.shape[0] // SPAN

    def split_blocks(array):
        return array.reshape((blocks, SPAN) + array.shape[1:])
    query, keys, values = (split_blocks(query), split_blocks(keys), split_blocks(values))
    strength, log_decay = (split_blocks(strength), split_blocks(log_decay))
    log_sum = jnp.cumsum(log_decay, axis=-1)
    offsets = jnp.arange(SPAN)
    causal = offsets[:, None] >= offsets[None, :]
    strict = offsets[:, None] > offsets[None, :]
    spread = log_sum[:, :, None] - log_sum[:, None, :]
    damping = jnp.where(causal, jnp.exp(jnp.where(causal, spread, 0.0)), 0.0)
    scaled_keys = keys * strength[..., None]
    lower = jnp.where(strict, jnp.einsum('nid,njd->nij', scaled_keys, keys, precision=HIGHEST) * damping, 0.0)
    identity = jnp.eye(SPAN, dtype=jnp.float32)
    right = jnp.concatenate([values * strength[..., None], scaled_keys * jnp.exp(log_sum)[..., None]], axis=-1)
    solved = jax.scipy.linalg.solve_triangular(identity + lower, right, lower=True, unit_diagonal=True)
    width = values.shape[-1]
    corrected = solved[..., :width]
    key_terms = solved[..., width:]
    scores = jnp.einsum('nid,njd->nij', query, keys, precision=HIGHEST) * damping

    def advance(memory, inputs):
        query_block, keys_block, corrected_block, terms_block, scores_block, log_block = inputs
        fresh = corrected_block - jnp.dot(terms_block, memory, precision=HIGHEST)
        output = jnp.dot(query_block * jnp.exp(log_block)[:, None], memory, precision=HIGHEST)
        output = output + jnp.dot(scores_block, fresh, precision=HIGHEST)
        tail_log = log_block[-1]
        weighted = keys_block * jnp.exp(tail_log - log_block)[:, None]
        memory = memory * jnp.exp(tail_log) + jnp.dot(weighted.T, fresh, precision=HIGHEST)
        return (memory, output)
    start = jnp.zeros((keys.shape[-1], width), jnp.float32)
    ignored, outputs = lax.scan(advance, start, (query, keys, corrected, key_terms, scores, log_sum))
    return outputs.reshape(blocks * SPAN, width)

def reference(tokens, w_query, w_key, w_value, w_delta_gate, w_glu_value, w_glu_gate, w_conv_gate, w_beta, w_decay, decay_log, head_gain, conv_taps, ln_gain, ln_shift, out_delta, out_conv):
    length = tokens.shape[0]
    floats = tokens.astype(jnp.float32)
    inv_rms = lax.rsqrt(lax.optimization_barrier(jnp.mean(floats * floats, axis=1, keepdims=True)) + TINY_NORM)

    def project(weight):
        return jnp.dot(tokens.astype(jnp.float32), weight.astype(jnp.float32), preferred_element_type=jnp.float32) * inv_rms
    query_raw = project(w_query).astype(jnp.bfloat16)
    key_raw = project(w_key).astype(jnp.bfloat16)
    value_raw = project(w_value).astype(jnp.bfloat16)
    delta_gate_raw = project(w_delta_gate).astype(jnp.bfloat16)
    glu_value_raw = project(w_glu_value).astype(jnp.bfloat16)
    glu_gate_raw = project(w_glu_gate).astype(jnp.bfloat16)
    conv_gate_raw = project(w_conv_gate).astype(jnp.bfloat16)
    strength = jax.nn.sigmoid(project(w_beta))
    log_decay = -jnp.exp(decay_log)[None, :] * jax.nn.softplus(project(w_decay))

    def to_heads(raw):
        return raw.astype(jnp.float32).reshape(length, HEADS, DK)

    def unit_rows(array):
        return array * lax.rsqrt(lax.optimization_barrier(jnp.sum(array * array, axis=-1, keepdims=True)) + TINY_NORM)
    query = unit_rows(to_heads(query_raw)) * DK ** (-0.5)
    keys = unit_rows(to_heads(key_raw))
    values = to_heads(value_raw)
    heads_out = lax.map(lambda inputs: head_rule(*inputs), (jnp.moveaxis(query, 1, 0), jnp.moveaxis(keys, 1, 0), jnp.moveaxis(values, 1, 0), strength.T, log_decay.T))
    output = jnp.moveaxis(heads_out, 0, 1)
    output = output * lax.rsqrt(lax.optimization_barrier(jnp.mean(output * output, axis=-1, keepdims=True)) + TINY_NORM) * head_gain
    delta_mixed = (output.reshape(length, HEADS * DK) * jax.nn.silu(delta_gate_raw.astype(jnp.float32))).astype(jnp.bfloat16)
    gated_units = (glu_value_raw.astype(jnp.float32) * jax.nn.sigmoid(glu_gate_raw.astype(jnp.float32))).astype(jnp.bfloat16)
    padded = jnp.concatenate([jnp.zeros((KERNEL - 1, CV), jnp.bfloat16), gated_units], axis=0)
    filtered = jnp.zeros((length, CV), jnp.float32)
    for offset in range(KERNEL):
        filtered = filtered + padded[offset:offset + length].astype(jnp.float32) * conv_taps[offset].astype(jnp.float32)
    center = lax.optimization_barrier(jnp.sum(filtered, axis=1)) / CV
    variance = jnp.maximum(lax.optimization_barrier(jnp.sum(filtered * filtered, axis=1)) / CV - center * center, 0.0)
    normed = (filtered - center[:, None]) * lax.rsqrt(variance + TINY_VAR)[:, None] * ln_gain + ln_shift
    conv_mixed = (jax.nn.silu(normed) * jax.nn.silu(conv_gate_raw.astype(jnp.float32))).astype(jnp.bfloat16)
    head_block = HEADS * DK // N_TP
    chan_block = CV // N_TP
    summed = jnp.zeros((length, D), jnp.float32)
    for group in range(N_TP):
        partial_value = jnp.dot(delta_mixed[:, group * head_block:(group + 1) * head_block].astype(jnp.float32), out_delta[group * head_block:(group + 1) * head_block].astype(jnp.float32), preferred_element_type=jnp.float32)
        partial_value = partial_value + jnp.dot(conv_mixed[:, group * chan_block:(group + 1) * chan_block].astype(jnp.float32), out_conv[group * chan_block:(group + 1) * chan_block].astype(jnp.float32), preferred_element_type=jnp.float32)
        partial_value = lax.optimization_barrier(partial_value.astype(jnp.bfloat16))
        summed = summed + partial_value.astype(jnp.float32)
    return summed.astype(jnp.bfloat16)
```

```python
import functools

import jax
import jax.numpy as jnp
from jax import lax
from jax.experimental import pallas as pl
from jax.experimental.pallas import tpu as pltpu
from jax.sharding import Mesh
from jax.sharding import PartitionSpec as P

SP = ("z", "x")
TP = ("y", "c")
TINY_NORM = 1e-06
TINY_VAR = 1e-05
CHUNK = 128
F32 = jnp.float32
BF16 = jnp.bfloat16
VMEM = pltpu.VMEM


def whole():
    return pl.BlockSpec(memory_space=pltpu.VMEM)


def scalars():
    return pl.BlockSpec(memory_space=pltpu.SMEM)


def params(mib):
    return pltpu.CompilerParams(vmem_limit_bytes=mib * 1024 * 1024)


def cost(flops, bytes_accessed):
    return pl.CostEstimate(flops=flops, bytes_accessed=bytes_accessed, transcendentals=0)


def dot(a, b):
    return jnp.dot(a, b, preferred_element_type=F32)


def dot_nt(a, b):
    return lax.dot_general(a, b, (((1,), (1,)), ((), ())), preferred_element_type=F32)


def dot_tn(a, b):
    return lax.dot_general(a, b, (((0,), (0,)), ((), ())), preferred_element_type=F32)


def low(a):
    return a.astype(BF16)


def split_two(a):
    high = a.astype(BF16)
    return high, (a - high.astype(F32)).astype(BF16)


def split_three(a):
    high = a.astype(BF16)
    rest = a - high.astype(F32)
    middle = rest.astype(BF16)
    return high, middle, (rest - middle.astype(F32)).astype(BF16)


def dot_fine(a, b):
    a_high, a_low = split_two(a)
    b_high, b_low = split_two(b)
    return dot(a_high, b_high) + (dot(a_high, b_low) + dot(a_low, b_high))


def project_kernel(width_all, head_size, block_ref, rate_ref, *refs):
    own, sw, r1, sr1, l1, sl1, fa, sfa, fb, sfb, weights = refs[:11]
    q_ref, k_ref, v_ref, dg_ref, gu_ref, cg_ref, bl_ref = refs[11:18]
    gathered = refs[18]
    first = pl.program_id(0) == 0
    piece_width = own.shape[1]
    rows = own.shape[0]
    squares = jnp.zeros((rows, 1), F32)

    def put(slot, piece):
        offset = pl.multiple_of(block_ref[slot] * piece_width, piece_width)
        gathered[:, pl.ds(offset, piece_width)] = piece
        wide = piece.astype(F32)
        return jnp.sum(wide * wide, axis=1, keepdims=True)

    for slot, ref in enumerate((own, sw, r1, sr1, l1, sl1)):
        squares = squares + put(slot, ref[...])
    squares = squares + put(6, jnp.where(first, fa[...], fb[...]))
    squares = squares + put(7, jnp.where(first, sfa[...], sfb[...]))
    inv_rms = lax.rsqrt(squares / width_all + TINY_NORM)
    features = gathered[...]

    def pair(n):
        both = dot(features, weights[:, n * 256 : (n + 1) * 256]) * inv_rms
        return both[:, :128], both[:, 128:]

    def unit_rows(raw):
        wide = low(raw).astype(F32)
        return wide * lax.rsqrt(jnp.sum(wide * wide, axis=-1, keepdims=True) + TINY_NORM)

    q, k = pair(0)
    q_ref[...] = low(unit_rows(q) * head_size ** (-0.5))
    k_ref[...] = low(unit_rows(k))
    v, dg = pair(1)
    v_ref[...] = low(v)
    dg_ref[...] = low(dg)
    gv, gg = pair(2)
    gu_ref[...] = low(low(gv).astype(F32) * jax.nn.sigmoid(low(gg).astype(F32)))
    cg, bl = pair(3)
    cg_ref[...] = low(cg)
    lane = lax.broadcasted_iota(jnp.int32, bl.shape, 1)
    bl_ref[...] = jnp.where(lane == 0, jax.nn.sigmoid(bl), -rate_ref[0] * jax.nn.softplus(bl))


def project(pieces, weights, blocks, rate, width_all, head_size):
    rows = pieces[0].shape[0]
    half = rows // 2
    piece_width = pieces[0].shape[1]
    full = pl.BlockSpec((half, piece_width), lambda i: (i, 0))
    fixed = pl.BlockSpec((half, piece_width), lambda i: (0, 0))
    out = pl.BlockSpec((half, 128), lambda i: (i, 0))
    kinds = [BF16] * 6 + [F32]
    return pl.pallas_call(
        functools.partial(project_kernel, width_all, head_size),
        grid=(2,),
        in_specs=[scalars(), scalars()]
        + [full] * 6
        + [fixed] * 4
        + [pl.BlockSpec(weights.shape, lambda i: (0, 0))],
        out_specs=[out] * 7,
        out_shape=[jax.ShapeDtypeStruct((rows, 128), kind) for kind in kinds],
        scratch_shapes=[pltpu.VMEM((half, width_all), BF16)],
        compiler_params=params(40),
        cost_estimate=cost(2 * rows * width_all * 1024, 12 << 20),
        name="project",
    )(blocks, rate, *pieces, weights)


def write_state(ref, state):
    total, lost, made = state
    size = lost.shape[0]
    ref[0:size, 0:size] = low(lost)
    ref[0:size, size:] = low(made)
    row = lax.broadcasted_iota(jnp.int32, (16, 2 * size), 0)
    high, middle, rest = split_three(jnp.broadcast_to(total, (16, 2 * size)))
    packed = jnp.where(
        row == 0,
        high.astype(F32),
        jnp.where(row == 1, middle.astype(F32), rest.astype(F32)),
    )
    ref[size : size + 16, :] = low(packed)


def read_state(ref):
    size = ref.shape[1] // 2
    packed = ref[size : size + 16, 0:128].astype(F32)
    total = packed[0:1, 0:1] + packed[1:2, 0:1] + packed[2:3, 0:1]
    return (total, ref[0:size, 0:size].astype(F32), ref[0:size, size:].astype(F32))


def or_nothing(valid, state):
    total, lost, made = state
    return (
        jnp.where(valid, total, 1.0),
        jnp.where(valid, lost, 0.0),
        jnp.where(valid, made, 0.0),
    )


def compose(later, earlier):
    total2, lost2, made2 = later
    total1, lost1, made1 = earlier
    size = lost1.shape[0]
    both = dot(low(lost2), low(jnp.concatenate([lost1, made1], axis=1)))
    lost = total2 * lost1 + total1 * lost2 - both[:, :size]
    made = total2 * made1 - both[:, size:] + made2
    return (total1 * total2, lost, made)


def delta_kernel(q_ref, k_ref, v_ref, bl_ref, coef_p_ref, coef_q_ref, state_ref):
    rows, size = q_ref.shape
    chunks = rows // CHUNK
    row = lax.broadcasted_iota(jnp.int32, (CHUNK, CHUNK), 0)
    column = lax.broadcasted_iota(jnp.int32, (CHUNK, CHUNK), 1)
    causal = row >= column
    strict = row > column
    ones = jnp.where(causal, 1.0, 0.0).astype(BF16)
    lowers, inverses, scores, grown, tails = [], [], [], [], []
    betas = []
    for n in range(chunks):
        here = slice(n * CHUNK, (n + 1) * CHUNK)
        both = bl_ref[here, :]
        beta = both[:, 0:1]
        high, middle, rest = split_three(both)
        sums = dot(ones, high) + (dot(ones, middle) + dot(ones, rest))
        log_sum = jnp.broadcast_to(sums[:, 1:2], (CHUNK, CHUNK))
        damping = jnp.where(causal, jnp.exp(jnp.minimum(log_sum - log_sum.T, 0.0)), 0.0)
        k = k_ref[here, :]
        lower = jnp.where(strict, dot_nt(k, k) * damping, 0.0) * beta
        scores.append(low(dot_nt(q_ref[here, :], k) * damping))
        lowers.append(lower)
        betas.append(beta)
        grown.append(log_sum)
        tails.append(log_sum[CHUNK - 1 : CHUNK, :])
        below = ((row & 1) == 1) & (column == row - 1)
        inverses.append(jnp.where(row == column, 1.0, 0.0) - jnp.where(below, lower, 0.0))
    level = 2
    while level < CHUNK:
        shift = level.bit_length() - 1
        part = row >> shift
        below = ((part & 1) == 1) & ((column >> shift) == part - 1)
        multiply = dot_fine if level >= 16 else (lambda a, b: dot(low(a), low(b)))
        moved = [
            multiply(inverse, jnp.where(below, lower, 0.0))
            for inverse, lower in zip(inverses, lowers)
        ]
        inverses = [
            inverse - multiply(middle, inverse) for inverse, middle in zip(inverses, moved)
        ]
        level *= 2
    queries, starts, losts, mades = [], [], [], []
    for n in range(chunks):
        here = slice(n * CHUNK, (n + 1) * CHUNK)
        k = k_ref[here, :].astype(F32)
        grow = jnp.exp(grown[n])
        right = jnp.concatenate(
            [v_ref[here, :].astype(F32) * betas[n], k * (betas[n] * grow)], axis=1
        )
        solved = low(dot(low(inverses[n]), low(right)))
        seen = dot(scores[n], solved)
        starts.append(seen[:, :size])
        queries.append(low(q_ref[here, :].astype(F32) * grow - seen[:, size:]))
        weighted = low(k * jnp.exp(tails[n] - grown[n]))
        written = dot_tn(weighted, solved)
        mades.append(written[:, :size])
        losts.append(low(written[:, size:]))
    carried = jnp.where(row == column, 1.0, 0.0)
    made = jnp.zeros((CHUNK, size), F32)
    log_total = jnp.zeros((1, CHUNK), F32)
    for n in range(chunks):
        here = slice(n * CHUNK, (n + 1) * CHUNK)
        rounded = low(jnp.concatenate([carried, made], axis=1))
        seen = dot(queries[n], rounded)
        coef_p_ref[here, :] = low(seen[:, :size])
        coef_q_ref[here, :] = seen[:, size:] + starts[n]
        moved = dot(losts[n], rounded)
        keep = jnp.exp(tails[n])
        carried = carried * keep - moved[:, :size]
        made = made * keep - moved[:, size:] + mades[n]
        log_total = log_total + tails[n]
    total = jnp.exp(log_total)[:, 0:1]
    lost = jnp.where(row == column, total, 0.0) - carried
    write_state(state_ref, (total, lost, made))


def delta(q, k, v, bl):
    rows, size = q.shape
    return pl.pallas_call(
        delta_kernel,
        in_specs=[whole()] * 4,
        out_specs=[whole()] * 3,
        out_shape=[
            jax.ShapeDtypeStruct((rows, size), BF16),
            jax.ShapeDtypeStruct((rows, size), F32),
            jax.ShapeDtypeStruct((size + 16, 2 * size), BF16),
        ],
        compiler_params=params(32),
        cost_estimate=cost(2 * rows * size * size * 60, 3 << 20),
        name="delta",
    )(q, k, v, bl)


def along_x_kernel(place_ref, p0, p1, p2, p3, before_ref, total_ref, held):
    me = place_ref[1]
    for j, piece in enumerate((p0, p1, p2, p3)):
        held[(me - j + 4) & 3] = piece[...]
    size = p0.shape[1] // 2
    nothing = (jnp.ones((1, 1), F32), jnp.zeros((size, size), F32), jnp.zeros((size, size), F32))
    before = nothing
    so_far = read_state(held.at[0])
    for m in range(1, 4):
        before = tuple(jnp.where(me == m, a, b) for a, b in zip(so_far, before))
        so_far = compose(read_state(held.at[m]), so_far)
    write_state(before_ref, before)
    write_state(total_ref, so_far)


def along_z_kernel(reach, place_ref, near_ref, far_ref, out_ref):
    me = place_ref[0]
    near = or_nothing(me >= reach[0], read_state(near_ref))
    far = or_nothing(me >= reach[1], read_state(far_ref))
    write_state(out_ref, compose(near, far))


def small_call(kernel, shapes, scratch, name, *args):
    return pl.pallas_call(
        kernel,
        in_specs=[scalars()] + [whole()] * (len(args) - 1),
        out_specs=[whole()] * len(shapes),
        out_shape=[jax.ShapeDtypeStruct(shape, BF16) for shape in shapes],
        scratch_shapes=scratch,
        compiler_params=params(16),
        cost_estimate=cost(16 << 20, 1 << 18),
        name=name,
    )(*args)


def cyclic(block, axis, distance):
    count = lax.axis_size(axis)
    return lax.ppermute(block, axis, [(i, (i + distance) % count) for i in range(count)])


def shifted(block, axis, distance):
    devices = range(lax.axis_size(axis))
    return lax.ppermute(block, axis, [(i, i + distance) for i in devices if i + distance in devices])


def swapped(block):
    return lax.ppermute(block, "c", [(0, 1), (1, 0)])


def finish_kernel(coef_p_ref, coef_q_ref, dg_ref, gain_ref, reach_ref, far_ref, before_ref, out_ref):
    total, lost, made = read_state(reach_ref)
    far = far_ref[...].astype(F32)
    state = total * far - dot(low(lost), far_ref[...]) + made
    total, lost, made = read_state(before_ref)
    state = low(total * state - dot(low(lost), low(state)) + made)
    result = coef_q_ref[...] + dot(coef_p_ref[...], state)
    mean = jnp.sum(result * result, axis=-1, keepdims=True) * (1.0 / result.shape[1])
    result = result * lax.rsqrt(mean + TINY_NORM) * gain_ref[...]
    out_ref[...] = low(result * jax.nn.silu(dg_ref[...].astype(F32)))


def finish(*args):
    return pl.pallas_call(
        finish_kernel,
        in_specs=[whole()] * len(args),
        out_specs=whole(),
        out_shape=jax.ShapeDtypeStruct(args[2].shape, BF16),
        compiler_params=params(16),
        cost_estimate=cost(64 << 20, 2 << 20),
        name="finish",
    )(*args)


def conv_kernel(gu_ref, before_ref, taps_ref, cg_ref, out_ref, padded):
    rows, size = gu_ref.shape
    head = before_ref.shape[0]
    count = taps_ref.shape[0]
    padded[0:head, :] = before_ref[...].astype(F32)
    padded[head:, :] = gu_ref[...].astype(F32)
    taps = taps_ref[...].astype(F32)
    step = 64
    skip = head - (count - 1)
    for base in range(0, rows, step):
        total = jnp.zeros((step, size), F32)
        for j in range(count):
            total = total + padded[base + skip + j : base + skip + j + step, :] * taps[j : j + 1, :]
        out_ref[base : base + step, 0:size] = low(total)
    out_ref[:, size:] = cg_ref[...]


def conv(gu, before, taps, cg):
    rows, size = gu.shape
    return pl.pallas_call(
        conv_kernel,
        in_specs=[whole()] * 4,
        out_specs=whole(),
        out_shape=jax.ShapeDtypeStruct((rows, 2 * size), BF16),
        scratch_shapes=[pltpu.VMEM((rows + before.shape[0], size), F32)],
        compiler_params=params(16),
        cost_estimate=cost(256 << 20, 1 << 20),
        name="conv",
    )(gu, before, taps, cg)


def order_of(weight_refs):
    return list(enumerate(weight_refs))


def conv_out_kernel(block_ref, got_ref, *refs):
    weight_refs, out_ref, mixed = refs[:8], refs[8], refs[9]
    groups, rows, size = mixed.shape
    total = jnp.zeros((rows, 1), F32)
    total_square = jnp.zeros((rows, 1), F32)
    for g in range(groups):
        part = got_ref[g, :, 0:size].astype(F32)
        total = total + jnp.sum(part, axis=1, keepdims=True)
        total_square = total_square + jnp.sum(part * part, axis=1, keepdims=True)
    scale = 1.0 / (groups * size)
    center = total * scale
    variance = jnp.maximum(total_square * scale - center * center, 0.0)
    factor = lax.rsqrt(variance + TINY_VAR)
    for slot, ref in order_of(weight_refs):
        g = block_ref[slot]
        extra = ref[size : size + 16, :].astype(F32)
        gain = extra[0:1, 0:size] + extra[1:2, 0:size] + extra[2:3, 0:size]
        shift = extra[3:4, 0:size] + extra[4:5, 0:size] + extra[5:6, 0:size]
        normed = (got_ref[g, :, 0:size].astype(F32) - center) * factor * gain + shift
        gate = got_ref[g, :, size:].astype(F32)
        mixed[slot] = low(jax.nn.silu(normed) * jax.nn.silu(gate))
    width = out_ref.shape[1]
    for base in range(0, width, 512):
        acc = jnp.zeros((rows, 512), F32)
        for slot, ref in order_of(weight_refs):
            acc = acc + dot(mixed[slot], ref[0:size, base : base + 512])
        out_ref[:, base : base + 512] = acc


def delta_out_kernel(block_ref, got_ref, conv_ref, *refs):
    weight_refs, out_ref = refs[:8], refs[8]
    width = out_ref.shape[1]
    for base in range(0, width, 512):
        acc = conv_ref[:, base : base + 512]
        for slot, ref in order_of(weight_refs):
            acc = acc + dot(got_ref[block_ref[slot]], ref[:, base : base + 512])
        out_ref[:, base : base + 512] = low(acc)


def out_call(kernel, kind, scratch, name, blocks, *args):
    rows, width = args[0].shape[1], args[-1].shape[1]
    return pl.pallas_call(
        kernel,
        in_specs=[scalars()] + [whole()] * len(args),
        out_specs=whole(),
        out_shape=jax.ShapeDtypeStruct((rows, width), kind),
        scratch_shapes=scratch,
        compiler_params=params(24),
        cost_estimate=cost(2 * rows * 1024 * width, 6 << 20),
        name=name,
    )(blocks, *args)


def local(
    tokens,
    w_query,
    w_key,
    w_value,
    w_delta_gate,
    w_glu_value,
    w_glu_gate,
    w_conv_gate,
    w_beta,
    w_decay,
    decay_log,
    head_gain,
    conv_taps,
    ln_gain,
    ln_shift,
    out_delta,
    out_conv,
):
    rows = tokens.shape[0]
    half = rows // 2
    size = w_query.shape[1]
    y, core = lax.axis_index("y"), lax.axis_index("c")
    x, z = lax.axis_index("x"), lax.axis_index("z")
    count_y = lax.axis_size("y")
    head = y * 2 + core
    chips = [y, (y - 1) % count_y, (y + 1) % count_y, (y + 2) % count_y]
    blocks = jnp.stack([chip * 2 + side for chip in chips for side in (core, 1 - core)])
    blocks = blocks.astype(jnp.int32)
    place = jnp.stack([z, x]).astype(jnp.int32)

    beta_decay = jnp.concatenate(
        [
            lax.dynamic_slice_in_dim(w_beta, head, 1, 1),
            lax.dynamic_slice_in_dim(w_decay, head, 1, 1),
            jnp.zeros((w_beta.shape[0], 126), BF16),
        ],
        axis=1,
    )
    weights = jnp.concatenate(
        [
            w_query,
            w_key,
            w_value,
            w_delta_gate,
            w_glu_value,
            w_glu_gate,
            w_conv_gate,
            beta_decay,
        ],
        axis=1,
    )
    rate = jnp.exp(lax.dynamic_slice_in_dim(decay_log, head, 1, 0))

    own = tokens
    r1, l1 = cyclic(own, "y", 1), cyclic(own, "y", -1)
    sw = swapped(own)
    fa, fb = cyclic(r1[:half], "y", 1), cyclic(l1[half:], "y", -1)
    sr1, sl1 = swapped(r1), swapped(l1)
    sfa, sfb = swapped(fa), swapped(fb)
    pieces = [own, sw, r1, sr1, l1, sl1, fa, sfa, fb, sfb]
    q, k, v, dg, gu, cg, bl = project(pieces, weights, blocks, rate, 2048, size)

    def three(vector):
        high = lax.reduce_precision(vector, 8, 7)
        rest = vector - high
        middle = lax.reduce_precision(rest, 8, 7)
        return [high, middle, rest - middle]

    extra = jnp.stack(three(ln_gain) + three(ln_shift)).astype(BF16)
    extra = jnp.pad(extra, ((0, 10), (0, out_conv.shape[1] - extra.shape[1])))
    last = jnp.concatenate([out_delta, out_conv, extra], axis=0)
    last, q = lax.optimization_barrier((last, q))
    wr, wl = cyclic(last, "y", 1), cyclic(last, "y", -1)
    ws = swapped(last)
    wfa, wfb = cyclic(wr[:size], "y", 1), cyclic(wl[size:], "y", -1)
    wsr, wsl = swapped(wr), swapped(wl)
    wsfa, wsfb = swapped(wfa), swapped(wfb)
    near = [last, ws, wr, wsr, wl, wsl]
    delta_weights = [a[:size] for a in near] + [wfa, wsfa]
    conv_weights = [a[size:] for a in near] + [wfb, wsfb]

    coef_p, coef_q, state = delta(q, k, v, bl)

    p1, p2, p3 = (cyclic(state, "x", j) for j in (1, 2, 3))
    kind = state.shape
    before, total = small_call(
        along_x_kernel,
        [kind, kind],
        [pltpu.VMEM((4,) + kind, BF16)],
        "along_x",
        place,
        state,
        p1,
        p2,
        p3,
    )
    (two,) = small_call(
        functools.partial(along_z_kernel, (1, 2)),
        [kind],
        [],
        "along_z",
        place,
        shifted(total, "z", 1),
        shifted(total, "z", 2),
    )
    (four,) = small_call(
        functools.partial(along_z_kernel, (0, 2)),
        [kind],
        [],
        "along_z_far",
        place,
        two,
        shifted(two, "z", 2),
    )
    far = shifted(four[:size, size:], "z", 4)

    halo = lax.ppermute(gu[rows - 32 :], SP, [(i, i + 1) for i in range(31)])
    filtered = conv(gu, halo, conv_taps, cg)
    groups = 8
    got = lax.all_to_all(filtered.reshape(groups, rows // groups, 2 * size), TP, 0, 0, tiled=True)
    conv_part = out_call(
        conv_out_kernel,
        F32,
        [pltpu.VMEM((groups, rows // groups, size), BF16)],
        "conv_out",
        blocks,
        got,
        *conv_weights,
    )

    mixed = finish(coef_p, coef_q, dg, head_gain[None, :], four, far, before)
    mixed = lax.all_to_all(mixed.reshape(groups, rows // groups, size), TP, 0, 0, tiled=True)
    return out_call(delta_out_kernel, BF16, [], "delta_out", blocks, mixed, conv_part, *delta_weights)


def solution(mesh):
    finer = Mesh(mesh.devices.reshape(8, 4, 4, 2), ("z", "x", "y", "c"))
    placed = (
        P(SP, TP),
        P(None, TP),
        P(None, TP),
        P(None, TP),
        P(None, TP),
        P(None, TP),
        P(None, TP),
        P(None, TP),
        P(),
        P(),
        P(),
        P(),
        P(None, TP),
        P(TP),
        P(TP),
        P(TP, None),
        P(TP, None),
    )
    return jax.shard_map(
        local, mesh=finer, in_specs=placed, out_specs=P(SP + TP, None), check_vma=False
    )
```

```python
import functools

import jax
import jax.numpy as jnp
from jax import lax
from jax.experimental import pallas as pl
from jax.experimental.pallas import tpu as pltpu
from jax.sharding import Mesh
from jax.sharding import PartitionSpec as P


SP = ("z", "x")
TP = ("y", "c")
TINY_NORM = 1e-06
TINY_VAR = 1e-05
CHUNK = 128
F32 = jnp.float32
BF16 = jnp.bfloat16


def whole():
    return pl.BlockSpec(memory_space=pltpu.VMEM)


def scalars():
    return pl.BlockSpec(memory_space=pltpu.SMEM)


def params(mib):
    return pltpu.CompilerParams(vmem_limit_bytes=mib * 1024 * 1024)


def cost(flops, bytes_accessed):
    return pl.CostEstimate(flops=flops, bytes_accessed=bytes_accessed, transcendentals=0)


def dot(a, b):
    return jnp.dot(a, b, preferred_element_type=F32)


def dot_nt(a, b):
    return lax.dot_general(a, b, (((1,), (1,)), ((), ())), preferred_element_type=F32)


def dot_tn(a, b):
    return lax.dot_general(a, b, (((0,), (0,)), ((), ())), preferred_element_type=F32)


def low(a):
    return a.astype(BF16)


def split_two(a):
    high = a.astype(BF16)
    return high, (a - high.astype(F32)).astype(BF16)


def split_three(a):
    high = a.astype(BF16)
    rest = a - high.astype(F32)
    middle = rest.astype(BF16)
    return high, middle, (rest - middle.astype(F32)).astype(BF16)


def dot_fine(a, b):
    a_high, a_low = split_two(a)
    b_high, b_low = split_two(b)
    return dot(a_high, b_high) + (dot(a_high, b_low) + dot(a_low, b_high))


def project_kernel(width_all, head_size, block_ref, rate_ref, *refs):
    own, sw, r1, sr1, l1, sl1, fa, sfa, fb, sfb, weights = refs[:11]
    q_ref, k_ref, v_ref, dg_ref, gu_ref, cg_ref, bl_ref = refs[11:18]
    gathered = refs[18]
    first = pl.program_id(0) == 0
    piece_width = own.shape[1]
    rows = own.shape[0]
    squares = jnp.zeros((rows, 1), F32)

    def put(slot, piece):
        offset = pl.multiple_of(block_ref[slot] * piece_width, piece_width)
        gathered[:, pl.ds(offset, piece_width)] = piece
        wide = piece.astype(F32)
        return jnp.sum(wide * wide, axis=1, keepdims=True)

    for slot, ref in enumerate((own, sw, r1, sr1, l1, sl1)):
        squares = squares + put(slot, ref[...])
    squares = squares + put(6, jnp.where(first, fa[...], fb[...]))
    squares = squares + put(7, jnp.where(first, sfa[...], sfb[...]))
    inv_rms = lax.rsqrt(squares / width_all + TINY_NORM)
    features = gathered[...]

    def pair(n):
        both = dot(features, weights[:, n * 256 : (n + 1) * 256]) * inv_rms
        return both[:, :128], both[:, 128:]

    def unit_rows(raw):
        wide = low(raw).astype(F32)
        return wide * lax.rsqrt(jnp.sum(wide * wide, axis=-1, keepdims=True) + TINY_NORM)

    q, k = pair(0)
    q_ref[...] = low(unit_rows(q) * head_size ** (-0.5))
    k_ref[...] = low(unit_rows(k))
    v, dg = pair(1)
    v_ref[...] = low(v)
    dg_ref[...] = low(dg)
    gv, gg = pair(2)
    gu_ref[...] = low(low(gv).astype(F32) * jax.nn.sigmoid(low(gg).astype(F32)))
    cg, bl = pair(3)
    cg_ref[...] = low(cg)
    lane = lax.broadcasted_iota(jnp.int32, bl.shape, 1)
    bl_ref[...] = jnp.where(lane == 0, jax.nn.sigmoid(bl), -rate_ref[0] * jax.nn.softplus(bl))


def project(pieces, weights, blocks, rate, width_all, head_size):
    rows = pieces[0].shape[0]
    half = rows // 2
    piece_width = pieces[0].shape[1]
    full = pl.BlockSpec((half, piece_width), lambda i: (i, 0))
    fixed = pl.BlockSpec((half, piece_width), lambda i: (0, 0))
    out = pl.BlockSpec((half, 128), lambda i: (i, 0))
    kinds = [BF16] * 6 + [F32]
    return pl.pallas_call(
        functools.partial(project_kernel, width_all, head_size),
        grid=(2,),
        in_specs=[scalars(), scalars()]
        + [full] * 6
        + [fixed] * 4
        + [pl.BlockSpec(weights.shape, lambda i: (0, 0))],
        out_specs=[out] * 7,
        out_shape=[jax.ShapeDtypeStruct((rows, 128), kind) for kind in kinds],
        scratch_shapes=[pltpu.VMEM((half, width_all), BF16)],
        compiler_params=params(28),
        cost_estimate=cost(2 * rows * width_all * 1024, 12 << 20),
        name="project",
    )(blocks, rate, *pieces, weights)


def write_state(ref, state):
    total, lost, made = state
    size = lost.shape[0]
    ref[0:size, 0:size] = low(lost)
    ref[0:size, size:] = low(made)
    row = lax.broadcasted_iota(jnp.int32, (16, 2 * size), 0)
    high, middle, rest = split_three(jnp.broadcast_to(total, (16, 2 * size)))
    packed = jnp.where(
        row == 0,
        high.astype(F32),
        jnp.where(row == 1, middle.astype(F32), rest.astype(F32)),
    )
    ref[size : size + 16, :] = low(packed)


def read_state(ref):
    size = ref.shape[1] // 2
    packed = ref[size : size + 16, 0:128].astype(F32)
    total = packed[0:1, 0:1] + packed[1:2, 0:1] + packed[2:3, 0:1]
    return (total, ref[0:size, 0:size].astype(F32), ref[0:size, size:].astype(F32))


def compose(later, earlier):
    total2, lost2, made2 = later
    total1, lost1, made1 = earlier
    size = lost1.shape[0]
    both = dot(low(lost2), low(jnp.concatenate([lost1, made1], axis=1)))
    lost = total2 * lost1 + total1 * lost2 - both[:, :size]
    made = total2 * made1 - both[:, size:] + made2
    return (total1 * total2, lost, made)


def delta_kernel(q_ref, k_ref, v_ref, bl_ref, coef_p_ref, coef_q_ref, state_ref):
    rows, size = q_ref.shape
    chunks = rows // CHUNK
    row = lax.broadcasted_iota(jnp.int32, (CHUNK, CHUNK), 0)
    column = lax.broadcasted_iota(jnp.int32, (CHUNK, CHUNK), 1)
    causal = row >= column
    strict = row > column
    ones = jnp.where(causal, 1.0, 0.0).astype(BF16)
    lowers, inverses, scores, grown, tails = [], [], [], [], []
    betas = []
    for n in range(chunks):
        here = slice(n * CHUNK, (n + 1) * CHUNK)
        both = bl_ref[here, :]
        beta = both[:, 0:1]
        high, middle, rest = split_three(both)
        sums = dot(ones, high) + (dot(ones, middle) + dot(ones, rest))
        log_sum = jnp.broadcast_to(sums[:, 1:2], (CHUNK, CHUNK))
        damping = jnp.where(causal, jnp.exp(jnp.minimum(log_sum - log_sum.T, 0.0)), 0.0)
        k = k_ref[here, :]
        lower = jnp.where(strict, dot_nt(k, k) * damping, 0.0) * beta
        scores.append(low(dot_nt(q_ref[here, :], k) * damping))
        lowers.append(lower)
        betas.append(beta)
        grown.append(log_sum)
        tails.append(log_sum[CHUNK - 1 : CHUNK, :])
        below = ((row & 1) == 1) & (column == row - 1)
        inverses.append(jnp.where(row == column, 1.0, 0.0) - jnp.where(below, lower, 0.0))
    level = 2
    while level < CHUNK:
        shift = level.bit_length() - 1
        part = row >> shift
        below = ((part & 1) == 1) & ((column >> shift) == part - 1)
        multiply = dot_fine if level >= 16 else (lambda a, b: dot(low(a), low(b)))
        moved = [
            multiply(inverse, jnp.where(below, lower, 0.0))
            for inverse, lower in zip(inverses, lowers)
        ]
        inverses = [
            inverse - multiply(middle, inverse) for inverse, middle in zip(inverses, moved)
        ]
        level *= 2
    queries, starts, losts, mades = [], [], [], []
    for n in range(chunks):
        here = slice(n * CHUNK, (n + 1) * CHUNK)
        k = k_ref[here, :].astype(F32)
        grow = jnp.exp(grown[n])
        right = jnp.concatenate(
            [v_ref[here, :].astype(F32) * betas[n], k * (betas[n] * grow)], axis=1
        )
        solved = low(dot(low(inverses[n]), low(right)))
        seen = dot(scores[n], solved)
        starts.append(seen[:, :size])
        queries.append(low(q_ref[here, :].astype(F32) * grow - seen[:, size:]))
        weighted = low(k * jnp.exp(tails[n] - grown[n]))
        written = dot_tn(weighted, solved)
        mades.append(written[:, :size])
        losts.append(low(written[:, size:]))
    carried = jnp.where(row == column, 1.0, 0.0)
    made = jnp.zeros((CHUNK, size), F32)
    log_total = jnp.zeros((1, CHUNK), F32)
    for n in range(chunks):
        here = slice(n * CHUNK, (n + 1) * CHUNK)
        rounded = low(jnp.concatenate([carried, made], axis=1))
        seen = dot(queries[n], rounded)
        coef_p_ref[here, :] = low(seen[:, :size])
        coef_q_ref[here, :] = seen[:, size:] + starts[n]
        moved = dot(losts[n], rounded)
        keep = jnp.exp(tails[n])
        carried = carried * keep - moved[:, :size]
        made = made * keep - moved[:, size:] + mades[n]
        log_total = log_total + tails[n]
    total = jnp.exp(log_total)[:, 0:1]
    lost = jnp.where(row == column, total, 0.0) - carried
    write_state(state_ref, (total, lost, made))


def delta(q, k, v, bl):
    rows, size = q.shape
    return pl.pallas_call(
        delta_kernel,
        in_specs=[whole()] * 4,
        out_specs=[whole()] * 3,
        out_shape=[
            jax.ShapeDtypeStruct((rows, size), BF16),
            jax.ShapeDtypeStruct((rows, size), F32),
            jax.ShapeDtypeStruct((size + 16, 2 * size), BF16),
        ],
        compiler_params=params(16),
        cost_estimate=cost(2 * rows * size * size * 60, 3 << 20),
        name="delta",
    )(q, k, v, bl)


def along_kernel(place_ref, p0, p1, p2, p3, before_ref, total_ref, held):
    me = place_ref[0]
    for j, piece in ((0, p0), (2, p1), (3, p2), (1, p3)):
        held[(me - j + 4) & 3] = piece[...]
    size = p0.shape[1] // 2
    nothing = (jnp.ones((1, 1), F32), jnp.zeros((size, size), F32), jnp.zeros((size, size), F32))
    before = nothing
    so_far = read_state(held.at[0])
    for m in range(1, 4):
        before = tuple(jnp.where(me == m, a, b) for a, b in zip(so_far, before))
        so_far = compose(read_state(held.at[m]), so_far)
    write_state(before_ref, before)
    write_state(total_ref, so_far)


def small_call(kernel, shapes, scratch, *args):
    return pl.pallas_call(
        kernel,
        in_specs=[scalars()] + [whole()] * (len(args) - 1),
        out_specs=[whole()] * len(shapes),
        out_shape=[jax.ShapeDtypeStruct(shape, BF16) for shape in shapes],
        scratch_shapes=scratch,
        compiler_params=params(4),
        cost_estimate=cost(16 << 20, 1 << 18),
    )(*args)


def cyclic(block, axis, distance):
    count = lax.axis_size(axis)
    return lax.ppermute(block, axis, [(i, (i + distance) % count) for i in range(count)])


def shifted(block, axis, distance):
    devices = range(lax.axis_size(axis))
    return lax.ppermute(block, axis, [(i, i + distance) for i in devices if i + distance in devices])


def swapped(block):
    return lax.ppermute(block, "c", [(0, 1), (1, 0)])


def finish_kernel(coef_p_ref, coef_q_ref, dg_ref, gain_ref, reach_ref, far_ref, before_ref, out_ref):
    total, lost, made = read_state(reach_ref)
    far = far_ref[...].astype(F32)
    state = total * far - dot(low(lost), far_ref[...]) + made
    total, lost, made = read_state(before_ref)
    state = low(total * state - dot(low(lost), low(state)) + made)
    result = coef_q_ref[...] + dot(coef_p_ref[...], state)
    mean = jnp.sum(result * result, axis=-1, keepdims=True) * (1.0 / result.shape[1])
    result = result * lax.rsqrt(mean + TINY_NORM) * gain_ref[...]
    out_ref[...] = low(result * jax.nn.silu(dg_ref[...].astype(F32)))


def finish(*args):
    return pl.pallas_call(
        finish_kernel,
        in_specs=[whole()] * len(args),
        out_specs=whole(),
        out_shape=jax.ShapeDtypeStruct(args[2].shape, BF16),
        compiler_params=params(4),
        cost_estimate=cost(64 << 20, 2 << 20),
        name="finish",
    )(*args)


def conv_kernel(gu_ref, before_ref, taps_ref, cg_ref, out_ref, padded):
    rows, size = gu_ref.shape
    head = before_ref.shape[0]
    count = taps_ref.shape[0]
    padded[0:head, :] = before_ref[...].astype(F32)
    padded[head:, :] = gu_ref[...].astype(F32)
    taps = taps_ref[...].astype(F32)
    step = 64
    skip = head - (count - 1)
    for base in range(0, rows, step):
        total = jnp.zeros((step, size), F32)
        for j in range(count):
            total = total + padded[base + skip + j : base + skip + j + step, :] * taps[j : j + 1, :]
        out_ref[base : base + step, 0:size] = low(total)
    out_ref[:, size:] = cg_ref[...]


def conv(gu, before, taps, cg):
    rows, size = gu.shape
    return pl.pallas_call(
        conv_kernel,
        in_specs=[whole()] * 4,
        out_specs=whole(),
        out_shape=jax.ShapeDtypeStruct((rows, 2 * size), BF16),
        scratch_shapes=[pltpu.VMEM((rows + before.shape[0], size), F32)],
        compiler_params=params(4),
        cost_estimate=cost(256 << 20, 1 << 20),
        name="conv",
    )(gu, before, taps, cg)


def order_of(weight_refs):
    return list(enumerate(weight_refs))


def conv_out_kernel(block_ref, got_ref, *refs):
    weight_refs, out_ref, mixed = refs[:8], refs[8], refs[9]
    starts = [128] * 6 + [0] * 2
    groups, rows, size = mixed.shape
    total = jnp.zeros((rows, 1), F32)
    total_square = jnp.zeros((rows, 1), F32)
    for g in range(groups):
        part = got_ref[g, :, 0:size].astype(F32)
        total = total + jnp.sum(part, axis=1, keepdims=True)
        total_square = total_square + jnp.sum(part * part, axis=1, keepdims=True)
    scale = 1.0 / (groups * size)
    center = total * scale
    variance = jnp.maximum(total_square * scale - center * center, 0.0)
    factor = lax.rsqrt(variance + TINY_VAR)
    for slot, ref in order_of(weight_refs):
        g = block_ref[slot]
        top = starts[slot] + size
        extra = ref[top : top + 16, :].astype(F32)
        gain = extra[0:1, 0:size] + extra[1:2, 0:size] + extra[2:3, 0:size]
        shift = extra[3:4, 0:size] + extra[4:5, 0:size] + extra[5:6, 0:size]
        normed = (got_ref[g, :, 0:size].astype(F32) - center) * factor * gain + shift
        gate = got_ref[g, :, size:].astype(F32)
        mixed[slot] = low(jax.nn.silu(normed) * jax.nn.silu(gate))
    width = out_ref.shape[1]
    for base in range(0, width, 512):
        acc = jnp.zeros((rows, 512), F32)
        for slot, ref in order_of(weight_refs):
            top = starts[slot]
            acc = acc + dot(mixed[slot], ref[top : top + size, base : base + 512])
        out_ref[:, base : base + 512] = acc


def delta_out_kernel(block_ref, got_ref, conv_ref, *refs):
    weight_refs, out_ref = refs[:8], refs[8]
    width = out_ref.shape[1]
    for base in range(0, width, 512):
        acc = conv_ref[:, base : base + 512]
        for slot, ref in order_of(weight_refs):
            acc = acc + dot(got_ref[block_ref[slot]], ref[0:128, base : base + 512])
        out_ref[:, base : base + 512] = low(acc)


def out_call(kernel, kind, scratch, blocks, *args):
    rows, width = args[0].shape[1], args[-1].shape[1]
    return pl.pallas_call(
        kernel,
        in_specs=[scalars()] + [whole()] * len(args),
        out_specs=whole(),
        out_shape=jax.ShapeDtypeStruct((rows, width), kind),
        scratch_shapes=scratch,
        compiler_params=params(8),
        cost_estimate=cost(2 * rows * 1024 * width, 6 << 20),
    )(blocks, *args)


def local(
    tokens,
    w_query,
    w_key,
    w_value,
    w_delta_gate,
    w_glu_value,
    w_glu_gate,
    w_conv_gate,
    w_beta,
    w_decay,
    decay_log,
    head_gain,
    conv_taps,
    ln_gain,
    ln_shift,
    out_delta,
    out_conv,
):
    rows = tokens.shape[0]
    half = rows // 2
    size = w_query.shape[1]
    y, core = lax.axis_index("y"), lax.axis_index("c")
    x, z = lax.axis_index("x"), lax.axis_index("z")
    count_y = lax.axis_size("y")
    head = y * 2 + core
    chips = [y, (y - 1) % count_y, (y + 1) % count_y, (y + 2) % count_y]
    blocks = jnp.stack([chip * 2 + side for chip in chips for side in (core, 1 - core)])
    blocks = blocks.astype(jnp.int32)

    beta_decay = jnp.concatenate(
        [
            lax.dynamic_slice_in_dim(w_beta, head, 1, 1),
            lax.dynamic_slice_in_dim(w_decay, head, 1, 1),
            jnp.zeros((w_beta.shape[0], 126), BF16),
        ],
        axis=1,
    )
    weights = jnp.concatenate(
        [
            w_query,
            w_key,
            w_value,
            w_delta_gate,
            w_glu_value,
            w_glu_gate,
            w_conv_gate,
            beta_decay,
        ],
        axis=1,
    )
    rate = jnp.exp(lax.dynamic_slice_in_dim(decay_log, head, 1, 0))

    def three(vector):
        high = lax.reduce_precision(vector, 8, 7)
        rest = vector - high
        middle = lax.reduce_precision(rest, 8, 7)
        return [high, middle, rest - middle]

    extra = jnp.stack(three(ln_gain) + three(ln_shift)).astype(BF16)
    extra = jnp.pad(extra, ((0, 10), (0, out_conv.shape[1] - extra.shape[1])))
    last = jnp.concatenate([out_delta, out_conv, extra], axis=0)

    own = tokens
    r1, l1 = cyclic(own, "y", 1), cyclic(own, "y", -1)
    sw = swapped(own)
    r1, l1, weights, last = lax.optimization_barrier((r1, l1, weights, last))
    fa, fb = cyclic(r1[:half], "y", 1), cyclic(l1[half:], "y", -1)
    sr1, sl1 = swapped(r1), swapped(l1)
    sfa, sfb = swapped(fa), swapped(fb)
    pieces = [own, sw, r1, sr1, l1, sl1, fa, sfa, fb, sfb]
    wr, wl = cyclic(last, "y", 1), cyclic(last, "y", -1)
    q, k, v, dg, gu, cg, bl = project(pieces, weights, blocks, rate, 2048, size)

    coef_p, coef_q, state = delta(q, k, v, bl)

    gu, last, state = lax.optimization_barrier((gu, last, state))

    kind = state.shape

    def among_four(place, state, others):
        return small_call(
            along_kernel,
            [kind, kind],
            [pltpu.VMEM((4,) + kind, BF16)],
            place[None].astype(jnp.int32),
            state,
            *others,
        )

    before, total = among_four(x, state, [cyclic(state, "x", j) for j in (2, 3, 1)])
    route = lambda j: [(h + i, h + (i + j) % 4) for h in (0, 4) for i in range(4)]
    around = []
    for j in (2, 3, 1):
        around.append(lax.ppermute(total, "z", route(j)))
    before_z, total_z = among_four(z % 4, total, around)
    far = shifted(total_z[:size, size:], "z", 4)

    ws = swapped(last)
    wfa, wfb = cyclic(wr[:size], "y", 1), cyclic(wl[size:], "y", -1)
    wsr, wsl = swapped(wr), swapped(wl)
    wsfa, wsfb = swapped(wfa), swapped(wfb)
    near = [last, ws, wr, wsr, wl, wsl]
    delta_weights = near + [wfa, wsfa]
    conv_weights = near + [wfb, wsfb]

    halo = lax.ppermute(gu[rows - 32 :], SP, [(i, i + 1) for i in range(31)])
    filtered = conv(gu, halo, conv_taps, cg)
    groups = 8
    got = lax.all_to_all(filtered.reshape(groups, rows // groups, 2 * size), TP, 0, 0, tiled=True)
    conv_part = out_call(
        conv_out_kernel,
        F32,
        [pltpu.VMEM((groups, rows // groups, size), BF16)],
        blocks,
        got,
        *conv_weights,
    )

    mixed = finish(coef_p, coef_q, dg, head_gain[None, :], before_z, far, before)
    mixed = lax.all_to_all(mixed.reshape(groups, rows // groups, size), TP, 0, 0, tiled=True)
    return out_call(delta_out_kernel, BF16, [], blocks, mixed, conv_part, *delta_weights)


def solution(mesh):
    finer = Mesh(mesh.devices.reshape(8, 4, 4, 2), ("z", "x", "y", "c"))
    placed = (
        P(SP, TP),
        P(None, TP),
        P(None, TP),
        P(None, TP),
        P(None, TP),
        P(None, TP),
        P(None, TP),
        P(None, TP),
        P(),
        P(),
        P(),
        P(),
        P(None, TP),
        P(TP),
        P(TP),
        P(TP, None),
        P(TP, None),
    )
    return jax.shard_map(
        local, mesh=finer, in_specs=placed, out_specs=P(SP + TP, None), check_vma=False
    )
```

```python
import functools

import jax
import jax.numpy as jnp
from jax import lax
from jax.experimental import pallas as pl
from jax.experimental.pallas import tpu as pltpu
from jax.sharding import Mesh
from jax.sharding import PartitionSpec as P


SP = ("z", "x")
TP = ("y", "c")
TINY_NORM = 1e-06
TINY_VAR = 1e-05
CHUNK = 128
F32 = jnp.float32
BF16 = jnp.bfloat16


def whole():
    return pl.BlockSpec(memory_space=pltpu.VMEM)


def hbm():
    return pl.BlockSpec(memory_space=pltpu.HBM)


def anywhere():
    return pl.BlockSpec(memory_space=pl.ANY)


def home(array):
    return pltpu.with_memory_space_constraint(array, pltpu.HBM)


def fetch(sems, *pairs):
    copies = [pltpu.make_async_copy(a, b, sems.at[n]) for n, (a, b) in enumerate(pairs)]
    for one in copies:
        one.start()
    return copies


def scalars():
    return pl.BlockSpec(memory_space=pltpu.SMEM)


def params(mib):
    return pltpu.CompilerParams(vmem_limit_bytes=min(mib * 1024 * 1024, 67043328))


def cost(flops, bytes_accessed):
    return pl.CostEstimate(flops=flops, bytes_accessed=bytes_accessed, transcendentals=0)


def dot(a, b):
    return jnp.dot(a, b, preferred_element_type=F32)


def dot_nt(a, b):
    return lax.dot_general(a, b, (((1,), (1,)), ((), ())), preferred_element_type=F32)


def dot_tn(a, b):
    return lax.dot_general(a, b, (((0,), (0,)), ((), ())), preferred_element_type=F32)


def low(a):
    return a.astype(BF16)


def split_two(a):
    high = a.astype(BF16)
    return high, (a - high.astype(F32)).astype(BF16)


def split_three(a):
    high = a.astype(BF16)
    rest = a - high.astype(F32)
    middle = rest.astype(BF16)
    return high, middle, (rest - middle.astype(F32)).astype(BF16)


def dot_fine(a, b):
    a_high, a_low = split_two(a)
    b_high, b_low = split_two(b)
    return dot(a_high, b_high) + (dot(a_high, b_low) + dot(a_low, b_high))


def project_kernel(width_all, head_size, block_ref, rate_ref, *refs):
    own, sw, r1, sr1, l1, sl1, fa, sfa, fb, sfb = refs[:10]
    sides = refs[10:18]
    q_ref, k_ref, v_ref, bl_ref, dg_hbm, gu_hbm, cg_hbm = refs[18:25]
    gathered, weights, dg_ref, gu_ref, cg_ref, sems, out_sems = refs[25:]
    rows, piece_width = own.shape[0], own.shape[1]
    half = rows // 2
    places = [slice(0, half), slice(half, rows)]

    def columns(slot):
        return pl.ds(pl.multiple_of(block_ref[slot] * piece_width, piece_width), piece_width)

    moves = [[], []]
    for n, here in enumerate(places):
        for slot, ref in enumerate((own, sw, r1, sr1, l1, sl1)):
            moves[n].append((ref.at[here, :], gathered.at[here, columns(slot)]))
        for slot, ref in enumerate(((fa, sfa), (fb, sfb))[n]):
            moves[n].append((ref, gathered.at[here, columns(6 + slot)]))
    parts = [
        (ref, weights.at[n // 2, :, pl.ds(n % 2 * 128, 128)]) for n, ref in enumerate(sides)
    ]
    first = fetch(sems, *moves[0])
    loads = fetch(sems.at[pl.ds(16, 2)], *parts[:2])
    second = fetch(sems.at[pl.ds(8, 8)], *moves[1])
    loads += fetch(sems.at[pl.ds(18, 6)], *parts[2:])

    def unit_rows(raw):
        wide = low(raw).astype(F32)
        return wide * lax.rsqrt(jnp.sum(wide * wide, axis=-1, keepdims=True) + TINY_NORM)

    def factor_of(n, pieces):
        for one in pieces:
            one.wait()
        wide = gathered[places[n], :].astype(F32)
        squares = jnp.sum(wide * wide, axis=1, keepdims=True)
        return lax.rsqrt(squares / width_all + TINY_NORM)

    def pair(n, here, factor):
        both = dot(gathered[here, :], weights[n]) * factor
        return both[:, :128], both[:, 128:]

    factors = []
    for n, here in enumerate(places):
        factor = factor_of(n, second if n else first[:8])
        factors.append(factor)
        if n == 0:
            loads[0].wait()
            loads[1].wait()
        gv, gg = pair(0, here, factor)
        gu_ref[here, :] = low(low(gv).astype(F32) * jax.nn.sigmoid(low(gg).astype(F32)))
    stores = fetch(out_sems, (gu_ref, gu_hbm))
    for one in loads[2 : 4]:
        one.wait()
    for here, factor in zip(places, factors):
        dg, cg = pair(1, here, factor)
        dg_ref[here, :] = low(dg)
        cg_ref[here, :] = low(cg)
    stores += fetch(out_sems.at[pl.ds(1, 2)], (dg_ref, dg_hbm), (cg_ref, cg_hbm))
    for one in loads[4 : 6]:
        one.wait()
    for here, factor in zip(places, factors):
        q, k = pair(2, here, factor)
        q_ref[here, :] = low(unit_rows(q) * head_size ** (-0.5))
        k_ref[here, :] = low(unit_rows(k))
    for one in loads[6 : 8]:
        one.wait()
    for here, factor in zip(places, factors):
        v, bl = pair(3, here, factor)
        v_ref[here, :] = low(v)
        lane = lax.broadcasted_iota(jnp.int32, bl.shape, 1)
        bl_ref[here, :] = jnp.where(
            lane == 0, jax.nn.sigmoid(bl), -rate_ref[0] * jax.nn.softplus(bl)
        )
    for one in stores:
        one.wait()


def project(pieces, weights, blocks, rate, width_all, head_size):
    rows = pieces[0].shape[0]
    kinds = [BF16] * 3 + [F32] + [BF16] * 3
    return pl.pallas_call(
        functools.partial(project_kernel, width_all, head_size),
        in_specs=[scalars(), scalars()] + [anywhere()] * 18,
        out_specs=[whole()] * 4 + [hbm()] * 3,
        out_shape=[pltpu.VMEM((rows, 128), kind) for kind in kinds[:4]]
        + [pltpu.HBM((rows, 128), kind) for kind in kinds[4:]],
        scratch_shapes=[
            pltpu.VMEM((rows, width_all), BF16),
            pltpu.VMEM((4, width_all, 256), BF16),
        ]
        + [pltpu.VMEM((rows, 128), BF16)] * 3
        + [pltpu.SemaphoreType.DMA((24,)), pltpu.SemaphoreType.DMA((3,))],
        compiler_params=params(28),
        cost_estimate=cost(2 * rows * width_all * 1024, 12 << 20),
        name="project",
    )(blocks, rate, home(pieces[0]), *pieces[1:], *map(home, weights))


def write_state(ref, state):
    total, lost, made = state
    size = lost.shape[0]
    ref[0:size, 0:size] = low(lost)
    ref[0:size, size:] = low(made)
    row = lax.broadcasted_iota(jnp.int32, (16, 2 * size), 0)
    high, middle, rest = split_three(jnp.broadcast_to(total, (16, 2 * size)))
    packed = jnp.where(
        row == 0,
        high.astype(F32),
        jnp.where(row == 1, middle.astype(F32), rest.astype(F32)),
    )
    ref[size : size + 16, :] = low(packed)


def read_state(ref):
    size = ref.shape[1] // 2
    packed = ref[size : size + 16, 0:128].astype(F32)
    total = packed[0:1, 0:1] + packed[1:2, 0:1] + packed[2:3, 0:1]
    return (total, ref[0:size, 0:size].astype(F32), ref[0:size, size:].astype(F32))


def compose(later, earlier):
    total2, lost2, made2 = later
    total1, lost1, made1 = earlier
    size = lost1.shape[0]
    both = dot(low(lost2), low(jnp.concatenate([lost1, made1], axis=1)))
    lost = total2 * lost1 + total1 * lost2 - both[:, :size]
    made = total2 * made1 - both[:, size:] + made2
    return (total1 * total2, lost, made)


def delta_kernel(
    q_ref, k_ref, v_ref, bl_ref, coef_p_hbm, coef_q_hbm, state_ref, coef_p_ref, coef_q_ref, sems
):
    rows, size = q_ref.shape
    chunks = rows // CHUNK
    row = lax.broadcasted_iota(jnp.int32, (CHUNK, CHUNK), 0)
    column = lax.broadcasted_iota(jnp.int32, (CHUNK, CHUNK), 1)
    causal = row >= column
    strict = row > column
    ones = jnp.where(causal, 1.0, 0.0).astype(BF16)
    lowers, inverses, scores, grown, tails = [], [], [], [], []
    betas = []
    for n in range(chunks):
        here = slice(n * CHUNK, (n + 1) * CHUNK)
        both = bl_ref[here, :]
        beta = both[:, 0:1]
        high, middle, rest = split_three(both)
        sums = dot(ones, high) + (dot(ones, middle) + dot(ones, rest))
        log_sum = jnp.broadcast_to(sums[:, 1:2], (CHUNK, CHUNK))
        damping = jnp.where(causal, jnp.exp(jnp.minimum(log_sum - log_sum.T, 0.0)), 0.0)
        k = k_ref[here, :]
        lower = jnp.where(strict, dot_nt(k, k) * damping, 0.0) * beta
        scores.append(low(dot_nt(q_ref[here, :], k) * damping))
        lowers.append(lower)
        betas.append(beta)
        grown.append(log_sum)
        tails.append(log_sum[CHUNK - 1 : CHUNK, :])
        below = ((row & 1) == 1) & (column == row - 1)
        inverses.append(jnp.where(row == column, 1.0, 0.0) - jnp.where(below, lower, 0.0))
    level = 2
    while level < CHUNK:
        shift = level.bit_length() - 1
        part = row >> shift
        below = ((part & 1) == 1) & ((column >> shift) == part - 1)
        multiply = dot_fine if level >= 16 else (lambda a, b: dot(low(a), low(b)))
        moved = [
            multiply(inverse, jnp.where(below, lower, 0.0))
            for inverse, lower in zip(inverses, lowers)
        ]
        inverses = [
            inverse - multiply(middle, inverse) for inverse, middle in zip(inverses, moved)
        ]
        level *= 2
    queries, starts, losts, mades = [], [], [], []
    for n in range(chunks):
        here = slice(n * CHUNK, (n + 1) * CHUNK)
        k = k_ref[here, :].astype(F32)
        grow = jnp.exp(grown[n])
        right = jnp.concatenate(
            [v_ref[here, :].astype(F32) * betas[n], k * (betas[n] * grow)], axis=1
        )
        solved = low(dot(low(inverses[n]), low(right)))
        seen = dot(scores[n], solved)
        starts.append(seen[:, :size])
        queries.append(low(q_ref[here, :].astype(F32) * grow - seen[:, size:]))
        weighted = low(k * jnp.exp(tails[n] - grown[n]))
        written = dot_tn(weighted, solved)
        mades.append(written[:, :size])
        losts.append(low(written[:, size:]))
    carried = jnp.where(row == column, 1.0, 0.0)
    made = jnp.zeros((CHUNK, size), F32)
    log_total = jnp.zeros((1, CHUNK), F32)
    stores = []
    for n in range(chunks):
        here = slice(n * CHUNK, (n + 1) * CHUNK)
        rounded = low(jnp.concatenate([carried, made], axis=1))
        seen = dot(queries[n], rounded)
        coef_p_ref[here, :] = low(seen[:, :size])
        coef_q_ref[here, :] = seen[:, size:] + starts[n]
        stores += fetch(
            sems.at[n],
            (coef_p_ref.at[here, :], coef_p_hbm.at[here, :]),
            (coef_q_ref.at[here, :], coef_q_hbm.at[here, :]),
        )
        moved = dot(losts[n], rounded)
        keep = jnp.exp(tails[n])
        carried = carried * keep - moved[:, :size]
        made = made * keep - moved[:, size:] + mades[n]
        log_total = log_total + tails[n]
    total = jnp.exp(log_total)[:, 0:1]
    lost = jnp.where(row == column, total, 0.0) - carried
    write_state(state_ref, (total, lost, made))
    for one in stores:
        one.wait()


def delta(q, k, v, bl):
    rows, size = q.shape
    return pl.pallas_call(
        delta_kernel,
        in_specs=[whole()] * 4,
        out_specs=[hbm(), hbm(), whole()],
        out_shape=[
            pltpu.HBM((rows, size), BF16),
            pltpu.HBM((rows, size), F32),
            pltpu.VMEM((size + 16, 2 * size), BF16),
        ],
        scratch_shapes=[
            pltpu.VMEM((rows, size), BF16),
            pltpu.VMEM((rows, size), F32),
            pltpu.SemaphoreType.DMA((rows // CHUNK, 2)),
        ],
        compiler_params=params(16),
        cost_estimate=cost(2 * rows * size * size * 60, 3 << 20),
        name="delta",
    )(q, k, v, bl)


def along_kernel(place_ref, p0, p1, p2, p3, before_hbm, total_ref, held, kept, sems, out_sem):
    me = place_ref[0]
    pieces = ((0, p0), (2, p1), (3, p2), (1, p3))
    for one in fetch(sems, *((piece, held.at[(me - j + 4) & 3]) for j, piece in pieces)):
        one.wait()
    size = p0.shape[1] // 2
    nothing = (jnp.ones((1, 1), F32), jnp.zeros((size, size), F32), jnp.zeros((size, size), F32))
    before = nothing
    so_far = read_state(held.at[0])
    for m in range(1, 4):
        before = tuple(jnp.where(me == m, a, b) for a, b in zip(so_far, before))
        so_far = compose(read_state(held.at[m]), so_far)
    write_state(kept, before)
    (store,) = fetch(out_sem, (kept, before_hbm))
    write_state(total_ref, so_far)
    store.wait()


def along(place, state, *others):
    return pl.pallas_call(
        along_kernel,
        in_specs=[scalars()] + [anywhere()] * 4,
        out_specs=[hbm(), whole()],
        out_shape=[pltpu.HBM(state.shape, BF16), pltpu.VMEM(state.shape, BF16)],
        scratch_shapes=[
            pltpu.VMEM((4,) + state.shape, BF16),
            pltpu.VMEM(state.shape, BF16),
            pltpu.SemaphoreType.DMA((4,)),
            pltpu.SemaphoreType.DMA((1,)),
        ],
        compiler_params=params(4),
        cost_estimate=cost(16 << 20, 1 << 18),
        name="along",
    )(place[None].astype(jnp.int32), state, *others)


def cyclic(block, axis, distance):
    count = lax.axis_size(axis)
    return lax.ppermute(block, axis, [(i, (i + distance) % count) for i in range(count)])


def shifted(block, axis, distance):
    devices = range(lax.axis_size(axis))
    return lax.ppermute(block, axis, [(i, i + distance) for i in devices if i + distance in devices])


def swapped(block):
    return lax.ppermute(block, "c", [(0, 1), (1, 0)])


def finish_kernel(
    coef_p_hbm, coef_q_hbm, dg_hbm, gain_ref, reach_any, far_any, before_hbm, out_hbm, *scratch
):
    coef_p_ref, coef_q_ref, dg_ref, reach_ref, far_ref, before_ref, out_ref, sems, out_sems = scratch
    loads = fetch(
        sems,
        (reach_any, reach_ref),
        (far_any, far_ref),
        (before_hbm, before_ref),
        (coef_p_hbm, coef_p_ref),
        (coef_q_hbm, coef_q_ref),
        (dg_hbm, dg_ref),
    )
    for one in loads[:3]:
        one.wait()
    total, lost, made = read_state(reach_ref)
    state = total * far_ref[...].astype(F32) - dot(low(lost), far_ref[...]) + made
    total, lost, made = read_state(before_ref)
    state = low(total * state - dot(low(lost), low(state)) + made)
    for one in loads[3:]:
        one.wait()
    stores = []
    step = out_ref.shape[0] // 4
    for n in range(4):
        here = slice(n * step, (n + 1) * step)
        result = coef_q_ref[here, :] + dot(coef_p_ref[here, :], state)
        mean = jnp.sum(result * result, axis=-1, keepdims=True) * (1.0 / result.shape[1])
        result = result * lax.rsqrt(mean + TINY_NORM) * gain_ref[...]
        out_ref[here, :] = low(result * jax.nn.silu(dg_ref[here, :].astype(F32)))
        stores += fetch(out_sems.at[pl.ds(n, 1)], (out_ref.at[here, :], out_hbm.at[here, :]))
    for one in stores:
        one.wait()


def finish(coef_p, coef_q, dg, gain, reach, far, before):
    coef_p, coef_q, dg, before, reach = map(home, (coef_p, coef_q, dg, before, reach))
    args = (coef_p, coef_q, dg, gain, reach, far, before)
    copied = (coef_p, coef_q, dg, reach, far, before, dg)
    return pl.pallas_call(
        finish_kernel,
        in_specs=[hbm(), hbm(), hbm(), whole(), anywhere(), anywhere(), hbm()],
        out_specs=hbm(),
        out_shape=pltpu.HBM(dg.shape, BF16),
        scratch_shapes=[pltpu.VMEM(a.shape, a.dtype) for a in copied]
        + [pltpu.SemaphoreType.DMA((6,)), pltpu.SemaphoreType.DMA((4,))],
        compiler_params=params(8),
        cost_estimate=cost(64 << 20, 2 << 20),
        name="finish",
    )(*args)


def conv_kernel(gu_hbm, before_any, taps_ref, cg_hbm, out_hbm, gu_ref, before_ref, padded, out_ref, sems, out_sems):
    rows, size = gu_ref.shape
    head = before_ref.shape[0]
    count = taps_ref.shape[0]
    gate = pltpu.make_async_copy(cg_hbm, out_ref.at[:, pl.ds(size, size)], sems.at[2])
    gate.start()
    for one in fetch(sems, (gu_hbm, gu_ref), (before_any, before_ref)):
        one.wait()
    padded[0:head, :] = before_ref[...].astype(F32)
    padded[head:, :] = gu_ref[...].astype(F32)
    taps = taps_ref[...].astype(F32)
    step = 64
    skip = head - (count - 1)
    gate.wait()
    stores = []
    for n, base in enumerate(range(0, rows, step)):
        total = jnp.zeros((step, size), F32)
        for j in range(count):
            total = total + padded[base + skip + j : base + skip + j + step, :] * taps[j : j + 1, :]
        here = slice(base, base + step)
        out_ref[here, 0:size] = low(total)
        stores += fetch(out_sems.at[pl.ds(n, 1)], (out_ref.at[here, :], out_hbm.at[here, :]))
    for one in stores:
        one.wait()


def conv(gu, before, taps, cg):
    rows, size = gu.shape
    return pl.pallas_call(
        conv_kernel,
        in_specs=[hbm(), anywhere(), whole(), hbm()],
        out_specs=hbm(),
        out_shape=pltpu.HBM((rows, 2 * size), BF16),
        scratch_shapes=[
            pltpu.VMEM(gu.shape, BF16),
            pltpu.VMEM(before.shape, BF16),
            pltpu.VMEM((rows + before.shape[0], size), F32),
            pltpu.VMEM((rows, 2 * size), BF16),
            pltpu.SemaphoreType.DMA((3,)),
            pltpu.SemaphoreType.DMA((rows // 64,)),
        ],
        compiler_params=params(8),
        cost_estimate=cost(256 << 20, 1 << 20),
        name="conv",
    )(home(gu), before, taps, home(cg))


def conv_out_kernel(block_ref, got_hbm, *refs):
    sources, out_hbm = refs[:8], refs[8]
    got_ref, weights, mixed, out_ref, sems, out_sems = refs[9:]
    groups, rows, size = mixed.shape
    (load,) = fetch(sems.at[pl.ds(8, 1)], (got_hbm, got_ref))
    loads = fetch(
        sems,
        *(
            (ref.at[pl.ds(0 if ref.shape[0] == size + 16 else size, size + 16), :], weights.at[slot])
            for slot, ref in enumerate(sources)
        ),
    )
    load.wait()
    total = jnp.zeros((rows, 1), F32)
    total_square = jnp.zeros((rows, 1), F32)
    for g in range(groups):
        part = got_ref[g, :, 0:size].astype(F32)
        total = total + jnp.sum(part, axis=1, keepdims=True)
        total_square = total_square + jnp.sum(part * part, axis=1, keepdims=True)
    scale = 1.0 / (groups * size)
    center = total * scale
    variance = jnp.maximum(total_square * scale - center * center, 0.0)
    factor = lax.rsqrt(variance + TINY_VAR)
    for one in loads:
        one.wait()
    for slot in range(groups):
        g = block_ref[slot]
        extra = weights[slot, size : size + 16, :].astype(F32)
        gain = extra[0:1, 0:size] + extra[1:2, 0:size] + extra[2:3, 0:size]
        shift = extra[3:4, 0:size] + extra[4:5, 0:size] + extra[5:6, 0:size]
        normed = (got_ref[g, :, 0:size].astype(F32) - center) * factor * gain + shift
        gate = got_ref[g, :, size:].astype(F32)
        mixed[slot] = low(jax.nn.silu(normed) * jax.nn.silu(gate))
    width = out_ref.shape[1]
    stores = []
    for n, base in enumerate(range(0, width, 512)):
        acc = jnp.zeros((rows, 512), F32)
        for slot in range(groups):
            acc = acc + dot(mixed[slot], weights[slot, 0:size, base : base + 512])
        here = slice(base, base + 512)
        out_ref[:, here] = acc
        stores += fetch(out_sems.at[pl.ds(n, 1)], (out_ref.at[:, here], out_hbm.at[:, here]))
    for one in stores:
        one.wait()


def conv_out(blocks, got, *sources):
    groups, rows, both = got.shape
    size, width = both // 2, sources[0].shape[1]
    return pl.pallas_call(
        conv_out_kernel,
        in_specs=[scalars()] + [anywhere()] * 9,
        out_specs=hbm(),
        out_shape=pltpu.HBM((rows, width), F32),
        scratch_shapes=[
            pltpu.VMEM(got.shape, BF16),
            pltpu.VMEM((groups, size + 16, width), BF16),
            pltpu.VMEM((groups, rows, size), BF16),
            pltpu.VMEM((rows, width), F32),
            pltpu.SemaphoreType.DMA((9,)),
            pltpu.SemaphoreType.DMA((4,)),
        ],
        compiler_params=params(12),
        cost_estimate=cost(2 * rows * 1024 * width, 6 << 20),
        name="conv_out",
    )(blocks, got, *sources)


def delta_out_kernel(block_ref, got_hbm, conv_hbm, *refs):
    sources, out_ref = refs[:8], refs[8]
    got_ref, weights, conv_ref, sems = refs[9:]
    size = got_ref.shape[1]
    loads = fetch(
        sems,
        (got_hbm, got_ref),
        *((ref.at[pl.ds(0, size), :], weights.at[slot]) for slot, ref in enumerate(sources)),
        (conv_hbm, conv_ref),
    )
    for one in loads:
        one.wait()
    width = out_ref.shape[1]
    for base in range(0, width, 512):
        acc = conv_ref[:, base : base + 512]
        for slot in range(len(sources)):
            acc = acc + dot(got_ref[block_ref[slot]], weights[slot, :, base : base + 512])
        out_ref[:, base : base + 512] = low(acc)


def delta_out(blocks, got, conv_part, *sources):
    groups, rows, size = got.shape
    width = conv_part.shape[1]
    return pl.pallas_call(
        delta_out_kernel,
        in_specs=[scalars()] + [anywhere()] * 10,
        out_specs=whole(),
        out_shape=jax.ShapeDtypeStruct((rows, width), BF16),
        scratch_shapes=[
            pltpu.VMEM(got.shape, BF16),
            pltpu.VMEM((groups, size, width), BF16),
            pltpu.VMEM(conv_part.shape, F32),
            pltpu.SemaphoreType.DMA((10,)),
        ],
        compiler_params=params(12),
        cost_estimate=cost(2 * rows * 1024 * width, 6 << 20),
        name="delta_out",
    )(blocks, got, home(conv_part), *sources)


def local(
    tokens,
    w_query,
    w_key,
    w_value,
    w_delta_gate,
    w_glu_value,
    w_glu_gate,
    w_conv_gate,
    w_beta,
    w_decay,
    decay_log,
    head_gain,
    conv_taps,
    ln_gain,
    ln_shift,
    out_delta,
    out_conv,
):
    rows = tokens.shape[0]
    half = rows // 2
    size = w_query.shape[1]
    y, core = lax.axis_index("y"), lax.axis_index("c")
    x, z = lax.axis_index("x"), lax.axis_index("z")
    count_y = lax.axis_size("y")
    head = y * 2 + core
    chips = [y, (y - 1) % count_y, (y + 1) % count_y, (y + 2) % count_y]
    blocks = jnp.stack([chip * 2 + side for chip in chips for side in (core, 1 - core)])
    blocks = blocks.astype(jnp.int32)

    beta_decay = jnp.concatenate(
        [
            lax.dynamic_slice_in_dim(w_beta, head, 1, 1),
            lax.dynamic_slice_in_dim(w_decay, head, 1, 1),
            jnp.zeros((w_beta.shape[0], 126), BF16),
        ],
        axis=1,
    )
    weights = (
        w_glu_value,
        w_glu_gate,
        w_delta_gate,
        w_conv_gate,
        w_query,
        w_key,
        w_value,
        beta_decay,
    )
    rate = jnp.exp(lax.dynamic_slice_in_dim(decay_log, head, 1, 0))

    def three(vector):
        high = lax.reduce_precision(vector, 8, 7)
        rest = vector - high
        middle = lax.reduce_precision(rest, 8, 7)
        return [high, middle, rest - middle]

    extra = jnp.stack(three(ln_gain) + three(ln_shift)).astype(BF16)
    extra = jnp.pad(extra, ((0, 10), (0, out_conv.shape[1] - extra.shape[1])))
    last = jnp.concatenate([out_delta, out_conv, extra], axis=0)

    own = tokens
    r1, l1 = cyclic(own, "y", 1), cyclic(own, "y", -1)
    sw = swapped(own)
    r1, l1, beta_decay, last = lax.optimization_barrier((r1, l1, beta_decay, last))
    weights = weights[:7] + (beta_decay,)
    fa, fb = cyclic(r1[:half], "y", 1), cyclic(l1[half:], "y", -1)
    sr1, sl1 = swapped(r1), swapped(l1)
    sfa, sfb = swapped(fa), swapped(fb)
    pieces = [own, sw, r1, sr1, l1, sl1, fa, sfa, fb, sfb]
    wr, wl = cyclic(last, "y", 1), cyclic(last, "y", -1)
    q, k, v, bl, dg, gu, cg = project(pieces, weights, blocks, rate, 2048, size)

    coef_p, coef_q, state = delta(q, k, v, bl)


    before, total = along(x, state, *(cyclic(state, "x", j) for j in (2, 3, 1)))
    route = lambda j: [(h + i, h + (i + j) % 4) for h in (0, 4) for i in range(4)]
    around = []
    for j in (2, 3, 1):
        around.append(lax.ppermute(total, "z", route(j)))
    before_z, total_z = along(z % 4, total, *around)
    far = shifted(total_z[:size, size:], "z", 4)

    ws = swapped(last)
    wfa, wfb = cyclic(wr[:size], "y", 1), cyclic(wl[size:], "y", -1)
    wsr, wsl = swapped(wr), swapped(wl)
    wsfa, wsfb = swapped(wfa), swapped(wfb)
    near = [last, ws, wr, wsr, wl, wsl]
    delta_weights = near + [wfa, wsfa]
    conv_weights = near + [wfb, wsfb]

    halo = lax.ppermute(gu[rows - 32 :], SP, [(i, i + 1) for i in range(31)])
    filtered = conv(gu, halo, conv_taps, cg)
    groups = 8
    got = lax.all_to_all(filtered.reshape(groups, rows // groups, 2 * size), TP, 0, 0, tiled=True)
    conv_part = conv_out(blocks, got, *conv_weights)

    mixed = finish(coef_p, coef_q, dg, head_gain[None, :], before_z, far, before)
    mixed = lax.all_to_all(mixed.reshape(groups, rows // groups, size), TP, 0, 0, tiled=True)
    return delta_out(blocks, mixed, conv_part, *delta_weights)


def solution(mesh):
    finer = Mesh(mesh.devices.reshape(8, 4, 4, 2), ("z", "x", "y", "c"))
    placed = (
        P(SP, TP),
        P(None, TP),
        P(None, TP),
        P(None, TP),
        P(None, TP),
        P(None, TP),
        P(None, TP),
        P(None, TP),
        P(),
        P(),
        P(),
        P(),
        P(None, TP),
        P(TP),
        P(TP),
        P(TP, None),
        P(TP, None),
    )
    return jax.shard_map(
        local, mesh=finer, in_specs=placed, out_specs=P(SP + TP, None), check_vma=False
    )
```

```python
import functools

import jax
import jax.numpy as jnp
from jax import lax
from jax.experimental import pallas as pl
from jax.experimental.pallas import tpu as pltpu
from jax.sharding import Mesh
from jax.sharding import PartitionSpec as P


SP = ("z", "x")
TP = ("y", "c")
TINY_NORM = 1e-06
TINY_VAR = 1e-05
CHUNK = 128
F32 = jnp.float32
BF16 = jnp.bfloat16


def whole():
    return pl.BlockSpec(memory_space=pltpu.VMEM)


def hbm():
    return pl.BlockSpec(memory_space=pltpu.HBM)


def anywhere():
    return pl.BlockSpec(memory_space=pl.ANY)


def home(array):
    return pltpu.with_memory_space_constraint(array, pltpu.HBM)


def fetch(sems, *pairs):
    copies = [pltpu.make_async_copy(a, b, sems.at[n]) for n, (a, b) in enumerate(pairs)]
    for one in copies:
        one.start()
    return copies


def scalars():
    return pl.BlockSpec(memory_space=pltpu.SMEM)


def params(mib):
    return pltpu.CompilerParams(vmem_limit_bytes=min(mib * 1024 * 1024, 67043328))


def cost(flops, bytes_accessed):
    return pl.CostEstimate(flops=flops, bytes_accessed=bytes_accessed, transcendentals=0)


def dot(a, b):
    return jnp.dot(a, b, preferred_element_type=F32)


def dot_nt(a, b):
    return lax.dot_general(a, b, (((1,), (1,)), ((), ())), preferred_element_type=F32)


def dot_tn(a, b):
    return lax.dot_general(a, b, (((0,), (0,)), ((), ())), preferred_element_type=F32)


def low(a):
    return a.astype(BF16)


def split_two(a):
    high = a.astype(BF16)
    return high, (a - high.astype(F32)).astype(BF16)


def split_three(a):
    high = a.astype(BF16)
    rest = a - high.astype(F32)
    middle = rest.astype(BF16)
    return high, middle, (rest - middle.astype(F32)).astype(BF16)


def dot_fine(a, b):
    a_high, a_low = split_two(a)
    b_high, b_low = split_two(b)
    return dot(a_high, b_high) + (dot(a_high, b_low) + dot(a_low, b_high))


def project_kernel(width_all, head_size, block_ref, rate_ref, *refs):
    own, sw, r1, sr1, l1, sl1, fa, sfa, fb, sfb = refs[:10]
    sides = refs[10:18]
    q_ref, k_ref, v_ref, bl_ref, dg_hbm, gu_hbm, cg_hbm = refs[18:25]
    gathered, weights, dg_ref, gu_ref, cg_ref, sems, out_sems = refs[25:]
    rows, piece_width = own.shape[0], own.shape[1]
    half = rows // 2
    places = [slice(0, half), slice(half, rows)]

    def columns(slot):
        return pl.ds(pl.multiple_of(block_ref[slot] * piece_width, piece_width), piece_width)

    moves = [[], []]
    for n, here in enumerate(places):
        for slot, ref in enumerate((own, sw, r1, sr1, l1, sl1)):
            moves[n].append((ref.at[here, :], gathered.at[here, columns(slot)]))
        for slot, ref in enumerate(((fa, sfa), (fb, sfb))[n]):
            moves[n].append((ref, gathered.at[here, columns(6 + slot)]))
    parts = [
        (ref, weights.at[n // 2, :, pl.ds(n % 2 * 128, 128)]) for n, ref in enumerate(sides)
    ]
    first = fetch(sems, *moves[0])
    loads = fetch(sems.at[pl.ds(16, 2)], *parts[:2])
    second = fetch(sems.at[pl.ds(8, 8)], *moves[1])
    loads += fetch(sems.at[pl.ds(18, 6)], *parts[2:])

    def unit_rows(raw):
        wide = low(raw).astype(F32)
        return wide * lax.rsqrt(jnp.sum(wide * wide, axis=-1, keepdims=True) + TINY_NORM)

    def factor_of(n, pieces):
        for one in pieces:
            one.wait()
        wide = gathered[places[n], :].astype(F32)
        squares = jnp.sum(wide * wide, axis=1, keepdims=True)
        return lax.rsqrt(squares / width_all + TINY_NORM)

    def pair(n, here, factor):
        both = dot(gathered[here, :], weights[n]) * factor
        return both[:, :128], both[:, 128:]

    factors = []
    for n, here in enumerate(places):
        factor = factor_of(n, second if n else first[:8])
        factors.append(factor)
        if n == 0:
            loads[0].wait()
            loads[1].wait()
        gv, gg = pair(0, here, factor)
        gu_ref[here, :] = low(low(gv).astype(F32) * jax.nn.sigmoid(low(gg).astype(F32)))
    stores = fetch(out_sems, (gu_ref, gu_hbm))
    for one in loads[2 : 4]:
        one.wait()
    for here, factor in zip(places, factors):
        dg, cg = pair(1, here, factor)
        dg_ref[here, :] = low(dg)
        cg_ref[here, :] = low(cg)
    stores += fetch(out_sems.at[pl.ds(1, 2)], (dg_ref, dg_hbm), (cg_ref, cg_hbm))
    for one in loads[4 : 6]:
        one.wait()
    for here, factor in zip(places, factors):
        q, k = pair(2, here, factor)
        q_ref[here, :] = low(unit_rows(q) * head_size ** (-0.5))
        k_ref[here, :] = low(unit_rows(k))
    for one in loads[6 : 8]:
        one.wait()
    for here, factor in zip(places, factors):
        v, bl = pair(3, here, factor)
        v_ref[here, :] = low(v)
        lane = lax.broadcasted_iota(jnp.int32, bl.shape, 1)
        bl_ref[here, :] = jnp.where(
            lane == 0, jax.nn.sigmoid(bl), -rate_ref[0] * jax.nn.softplus(bl)
        )
    for one in stores:
        one.wait()


def project(pieces, weights, blocks, rate, width_all, head_size):
    rows = pieces[0].shape[0]
    kinds = [BF16] * 3 + [F32] + [BF16] * 3
    return pl.pallas_call(
        functools.partial(project_kernel, width_all, head_size),
        in_specs=[scalars(), scalars()] + [anywhere()] * 18,
        out_specs=[whole()] * 4 + [hbm()] * 3,
        out_shape=[pltpu.VMEM((rows, 128), kind) for kind in kinds[:4]]
        + [pltpu.HBM((rows, 128), kind) for kind in kinds[4:]],
        scratch_shapes=[
            pltpu.VMEM((rows, width_all), BF16),
            pltpu.VMEM((4, width_all, 256), BF16),
        ]
        + [pltpu.VMEM((rows, 128), BF16)] * 3
        + [pltpu.SemaphoreType.DMA((24,)), pltpu.SemaphoreType.DMA((3,))],
        compiler_params=params(28),
        cost_estimate=cost(2 * rows * width_all * 1024, 12 << 20),
        name="project",
    )(blocks, rate, home(pieces[0]), *pieces[1:], *map(home, weights))


def write_state(ref, state):
    total, lost, made = state
    size = lost.shape[0]
    ref[0:size, 0:size] = low(lost)
    ref[0:size, size:] = low(made)
    row = lax.broadcasted_iota(jnp.int32, (16, 2 * size), 0)
    high, middle, rest = split_three(jnp.broadcast_to(total, (16, 2 * size)))
    packed = jnp.where(
        row == 0,
        high.astype(F32),
        jnp.where(row == 1, middle.astype(F32), rest.astype(F32)),
    )
    ref[size : size + 16, :] = low(packed)


def read_state(ref):
    size = ref.shape[1] // 2
    packed = ref[size : size + 16, 0:128].astype(F32)
    total = packed[0:1, 0:1] + packed[1:2, 0:1] + packed[2:3, 0:1]
    return (total, ref[0:size, 0:size].astype(F32), ref[0:size, size:].astype(F32))


def compose(later, earlier):
    total2, lost2, made2 = later
    total1, lost1, made1 = earlier
    size = lost1.shape[0]
    both = dot(low(lost2), low(jnp.concatenate([lost1, made1], axis=1)))
    lost = total2 * lost1 + total1 * lost2 - both[:, :size]
    made = total2 * made1 - both[:, size:] + made2
    return (total1 * total2, lost, made)


def delta_kernel(
    q_ref, k_ref, v_ref, bl_ref, coef_p_hbm, coef_q_hbm, state_ref, coef_p_ref, coef_q_ref, sems
):
    rows, size = q_ref.shape
    chunks = rows // CHUNK
    row = lax.broadcasted_iota(jnp.int32, (CHUNK, CHUNK), 0)
    column = lax.broadcasted_iota(jnp.int32, (CHUNK, CHUNK), 1)
    causal = row >= column
    strict = row > column
    ones = jnp.where(causal, 1.0, 0.0).astype(BF16)
    lowers, inverses, scores, grown, tails = [], [], [], [], []
    betas = []
    for n in range(chunks):
        here = slice(n * CHUNK, (n + 1) * CHUNK)
        both = bl_ref[here, :]
        beta = both[:, 0:1]
        high, middle, rest = split_three(both)
        sums = dot(ones, high) + (dot(ones, middle) + dot(ones, rest))
        log_sum = jnp.broadcast_to(sums[:, 1:2], (CHUNK, CHUNK))
        damping = jnp.where(causal, jnp.exp(jnp.minimum(log_sum - log_sum.T, 0.0)), 0.0)
        k = k_ref[here, :]
        lower = jnp.where(strict, dot_nt(k, k) * damping, 0.0) * beta
        scores.append(low(dot_nt(q_ref[here, :], k) * damping))
        lowers.append(lower)
        betas.append(beta)
        grown.append(log_sum)
        tails.append(log_sum[CHUNK - 1 : CHUNK, :])
        below = ((row & 1) == 1) & (column == row - 1)
        inverses.append(jnp.where(row == column, 1.0, 0.0) - jnp.where(below, lower, 0.0))
    level = 2
    while level < CHUNK:
        shift = level.bit_length() - 1
        part = row >> shift
        below = ((part & 1) == 1) & ((column >> shift) == part - 1)
        multiply = dot_fine if level >= 16 else (lambda a, b: dot(low(a), low(b)))
        moved = [
            multiply(inverse, jnp.where(below, lower, 0.0))
            for inverse, lower in zip(inverses, lowers)
        ]
        inverses = [
            inverse - multiply(middle, inverse) for inverse, middle in zip(inverses, moved)
        ]
        level *= 2
    queries, starts, losts, mades = [], [], [], []
    for n in range(chunks):
        here = slice(n * CHUNK, (n + 1) * CHUNK)
        k = k_ref[here, :].astype(F32)
        grow = jnp.exp(grown[n])
        right = jnp.concatenate(
            [v_ref[here, :].astype(F32) * betas[n], k * (betas[n] * grow)], axis=1
        )
        solved = low(dot(low(inverses[n]), low(right)))
        seen = dot(scores[n], solved)
        starts.append(seen[:, :size])
        queries.append(low(q_ref[here, :].astype(F32) * grow - seen[:, size:]))
        weighted = low(k * jnp.exp(tails[n] - grown[n]))
        written = dot_tn(weighted, solved)
        mades.append(written[:, :size])
        losts.append(low(written[:, size:]))
    carried = jnp.where(row == column, 1.0, 0.0)
    made = jnp.zeros((CHUNK, size), F32)
    log_total = jnp.zeros((1, CHUNK), F32)
    stores = []
    for n in range(chunks):
        here = slice(n * CHUNK, (n + 1) * CHUNK)
        rounded = low(jnp.concatenate([carried, made], axis=1))
        seen = dot(queries[n], rounded)
        coef_p_ref[here, :] = low(seen[:, :size])
        coef_q_ref[here, :] = seen[:, size:] + starts[n]
        stores += fetch(
            sems.at[n],
            (coef_p_ref.at[here, :], coef_p_hbm.at[here, :]),
            (coef_q_ref.at[here, :], coef_q_hbm.at[here, :]),
        )
        moved = dot(losts[n], rounded)
        keep = jnp.exp(tails[n])
        carried = carried * keep - moved[:, :size]
        made = made * keep - moved[:, size:] + mades[n]
        log_total = log_total + tails[n]
    total = jnp.exp(log_total)[:, 0:1]
    lost = jnp.where(row == column, total, 0.0) - carried
    write_state(state_ref, (total, lost, made))
    for one in stores:
        one.wait()


def delta(q, k, v, bl):
    rows, size = q.shape
    return pl.pallas_call(
        delta_kernel,
        in_specs=[whole()] * 4,
        out_specs=[hbm(), hbm(), whole()],
        out_shape=[
            pltpu.HBM((rows, size), BF16),
            pltpu.HBM((rows, size), F32),
            pltpu.VMEM((size + 16, 2 * size), BF16),
        ],
        scratch_shapes=[
            pltpu.VMEM((rows, size), BF16),
            pltpu.VMEM((rows, size), F32),
            pltpu.SemaphoreType.DMA((rows // CHUNK, 2)),
        ],
        compiler_params=params(16),
        cost_estimate=cost(2 * rows * size * size * 60, 3 << 20),
        name="delta",
    )(q, k, v, bl)


def along_kernel(place_ref, p0, p1, p2, p3, before_hbm, total_ref, held, kept, out_sem):
    me = place_ref[0]
    for j, piece in ((0, p0), (2, p1), (3, p2), (1, p3)):
        held[(me - j + 4) & 3] = piece[...]
    size = p0.shape[1] // 2
    nothing = (jnp.ones((1, 1), F32), jnp.zeros((size, size), F32), jnp.zeros((size, size), F32))
    before = nothing
    so_far = read_state(held.at[0])
    for m in range(1, 4):
        before = tuple(jnp.where(me == m, a, b) for a, b in zip(so_far, before))
        so_far = compose(read_state(held.at[m]), so_far)
    write_state(kept, before)
    (store,) = fetch(out_sem, (kept, before_hbm))
    write_state(total_ref, so_far)
    store.wait()


def along(place, state, *others):
    return pl.pallas_call(
        along_kernel,
        in_specs=[scalars()] + [whole()] * 4,
        out_specs=[hbm(), whole()],
        out_shape=[pltpu.HBM(state.shape, BF16), pltpu.VMEM(state.shape, BF16)],
        scratch_shapes=[
            pltpu.VMEM((4,) + state.shape, BF16),
            pltpu.VMEM(state.shape, BF16),
            pltpu.SemaphoreType.DMA((1,)),
        ],
        compiler_params=params(4),
        cost_estimate=cost(16 << 20, 1 << 18),
        name="along",
    )(place[None].astype(jnp.int32), state, *others)


def cyclic(block, axis, distance):
    count = lax.axis_size(axis)
    return lax.ppermute(block, axis, [(i, (i + distance) % count) for i in range(count)])


def shifted(block, axis, distance):
    devices = range(lax.axis_size(axis))
    return lax.ppermute(block, axis, [(i, i + distance) for i in devices if i + distance in devices])


def swapped(block):
    return lax.ppermute(block, "c", [(0, 1), (1, 0)])


def finish_kernel(
    coef_p_hbm, coef_q_hbm, dg_hbm, gain_ref, reach_any, far_any, before_hbm, out_hbm, *scratch
):
    coef_p_ref, coef_q_ref, dg_ref, reach_ref, far_ref, before_ref, out_ref, sems, out_sems = scratch
    loads = fetch(
        sems,
        (reach_any, reach_ref),
        (far_any, far_ref),
        (before_hbm, before_ref),
        (coef_p_hbm, coef_p_ref),
        (coef_q_hbm, coef_q_ref),
        (dg_hbm, dg_ref),
    )
    for one in loads[:3]:
        one.wait()
    total, lost, made = read_state(reach_ref)
    state = total * far_ref[...].astype(F32) - dot(low(lost), far_ref[...]) + made
    total, lost, made = read_state(before_ref)
    state = low(total * state - dot(low(lost), low(state)) + made)
    for one in loads[3:]:
        one.wait()
    stores = []
    step = out_ref.shape[0] // 4
    for n in range(4):
        here = slice(n * step, (n + 1) * step)
        result = coef_q_ref[here, :] + dot(coef_p_ref[here, :], state)
        mean = jnp.sum(result * result, axis=-1, keepdims=True) * (1.0 / result.shape[1])
        result = result * lax.rsqrt(mean + TINY_NORM) * gain_ref[...]
        out_ref[here, :] = low(result * jax.nn.silu(dg_ref[here, :].astype(F32)))
        stores += fetch(out_sems.at[pl.ds(n, 1)], (out_ref.at[here, :], out_hbm.at[here, :]))
    for one in stores:
        one.wait()


def finish(coef_p, coef_q, dg, gain, reach, far, before):
    coef_p, coef_q, dg, before, reach = map(home, (coef_p, coef_q, dg, before, reach))
    args = (coef_p, coef_q, dg, gain, reach, far, before)
    copied = (coef_p, coef_q, dg, reach, far, before, dg)
    return pl.pallas_call(
        finish_kernel,
        in_specs=[hbm(), hbm(), hbm(), whole(), anywhere(), anywhere(), hbm()],
        out_specs=hbm(),
        out_shape=pltpu.HBM(dg.shape, BF16),
        scratch_shapes=[pltpu.VMEM(a.shape, a.dtype) for a in copied]
        + [pltpu.SemaphoreType.DMA((6,)), pltpu.SemaphoreType.DMA((4,))],
        compiler_params=params(8),
        cost_estimate=cost(64 << 20, 2 << 20),
        name="finish",
    )(*args)


def conv_kernel(gu_hbm, before_any, taps_ref, cg_hbm, out_hbm, gu_ref, before_ref, padded, out_ref, sems, out_sems):
    rows, size = gu_ref.shape
    head = before_ref.shape[0]
    count = taps_ref.shape[0]
    gate = pltpu.make_async_copy(cg_hbm, out_ref.at[:, pl.ds(size, size)], sems.at[2])
    gate.start()
    for one in fetch(sems, (gu_hbm, gu_ref), (before_any, before_ref)):
        one.wait()
    padded[0:head, :] = before_ref[...].astype(F32)
    padded[head:, :] = gu_ref[...].astype(F32)
    taps = taps_ref[...].astype(F32)
    step = 64
    skip = head - (count - 1)
    gate.wait()
    stores = []
    for n, base in enumerate(range(0, rows, step)):
        total = jnp.zeros((step, size), F32)
        for j in range(count):
            total = total + padded[base + skip + j : base + skip + j + step, :] * taps[j : j + 1, :]
        here = slice(base, base + step)
        out_ref[here, 0:size] = low(total)
        stores += fetch(out_sems.at[pl.ds(n, 1)], (out_ref.at[here, :], out_hbm.at[here, :]))
    for one in stores:
        one.wait()


def conv(gu, before, taps, cg):
    rows, size = gu.shape
    return pl.pallas_call(
        conv_kernel,
        in_specs=[hbm(), anywhere(), whole(), hbm()],
        out_specs=hbm(),
        out_shape=pltpu.HBM((rows, 2 * size), BF16),
        scratch_shapes=[
            pltpu.VMEM(gu.shape, BF16),
            pltpu.VMEM(before.shape, BF16),
            pltpu.VMEM((rows + before.shape[0], size), F32),
            pltpu.VMEM((rows, 2 * size), BF16),
            pltpu.SemaphoreType.DMA((3,)),
            pltpu.SemaphoreType.DMA((rows // 64,)),
        ],
        compiler_params=params(8),
        cost_estimate=cost(256 << 20, 1 << 20),
        name="conv",
    )(home(gu), before, taps, home(cg))


def add_slots(out_ref, slots, left, weights, start):
    width = out_ref.shape[1]
    size = weights.shape[1] - weights.shape[1] % 128
    for base in range(0, width, 512):
        here = slice(base, base + 512)
        acc = jnp.zeros((out_ref.shape[0], 512), F32) if start is None else start[:, here]
        for slot in slots:
            acc = acc + dot(left(slot), weights[slot, 0:size, here])
        out_ref[:, here] = acc.astype(out_ref.dtype)


def conv_out_kernel(block_ref, got_hbm, *refs):
    sources, out_hbm = refs[:8], refs[8]
    got_ref, weights, mixed, out_ref, sems, out_sems = refs[9:]
    groups, rows, size = mixed.shape
    (load,) = fetch(sems.at[pl.ds(8, 1)], (got_hbm, got_ref))
    loads = fetch(
        sems,
        *(
            (ref.at[pl.ds(0 if ref.shape[0] == size + 16 else size, size + 16), :], weights.at[slot])
            for slot, ref in enumerate(sources)
        ),
    )
    load.wait()
    total = jnp.zeros((rows, size), F32)
    total_square = jnp.zeros((rows, size), F32)
    for g in range(groups):
        part = got_ref[g, :, 0:size].astype(F32)
        total = total + part
        total_square = total_square + part * part
    scale = 1.0 / (groups * size)
    center = jnp.sum(total, axis=1, keepdims=True) * scale
    second = jnp.sum(total_square, axis=1, keepdims=True) * scale
    factor = lax.rsqrt(jnp.maximum(second - center * center, 0.0) + TINY_VAR)
    for half in range(2):
        slots = range(half * 4, half * 4 + 4)
        for slot in slots:
            loads[slot].wait()
            g = block_ref[slot]
            extra = weights[slot, size : size + 16, :].astype(F32)
            gain = extra[0:1, 0:size] + extra[1:2, 0:size] + extra[2:3, 0:size]
            shift = extra[3:4, 0:size] + extra[4:5, 0:size] + extra[5:6, 0:size]
            normed = (got_ref[g, :, 0:size].astype(F32) - center) * factor * gain + shift
            gate = got_ref[g, :, size:].astype(F32)
            mixed[slot] = low(jax.nn.silu(normed) * jax.nn.silu(gate))
        add_slots(
            out_ref, slots, lambda slot: mixed[slot], weights, out_ref if half else None
        )
    (store,) = fetch(out_sems, (out_ref, out_hbm))
    store.wait()


def conv_out(blocks, got, *sources):
    groups, rows, both = got.shape
    size, width = both // 2, sources[0].shape[1]
    return pl.pallas_call(
        conv_out_kernel,
        in_specs=[scalars()] + [anywhere()] * 9,
        out_specs=hbm(),
        out_shape=pltpu.HBM((rows, width), F32),
        scratch_shapes=[
            pltpu.VMEM(got.shape, BF16),
            pltpu.VMEM((groups, size + 16, width), BF16),
            pltpu.VMEM((groups, rows, size), BF16),
            pltpu.VMEM((rows, width), F32),
            pltpu.SemaphoreType.DMA((9,)),
            pltpu.SemaphoreType.DMA((1,)),
        ],
        compiler_params=params(12),
        cost_estimate=cost(2 * rows * 1024 * width, 6 << 20),
        name="conv_out",
    )(blocks, got, *sources)


def delta_out_kernel(block_ref, got_hbm, conv_hbm, *refs):
    sources, out_ref = refs[:8], refs[8]
    got_ref, weights, conv_ref, sems = refs[9:]
    size = got_ref.shape[1]
    loads = fetch(
        sems,
        (got_hbm, got_ref),
        (conv_hbm, conv_ref),
        *((ref.at[pl.ds(0, size), :], weights.at[slot]) for slot, ref in enumerate(sources)),
    )
    loads[0].wait()
    loads[1].wait()
    for half in range(2):
        slots = range(half * 4, half * 4 + 4)
        for slot in slots:
            loads[2 + slot].wait()
        add_slots(
            out_ref if half else conv_ref,
            slots,
            lambda slot: got_ref[block_ref[slot]],
            weights,
            conv_ref,
        )


def delta_out(blocks, got, conv_part, *sources):
    groups, rows, size = got.shape
    width = conv_part.shape[1]
    return pl.pallas_call(
        delta_out_kernel,
        in_specs=[scalars()] + [anywhere()] * 10,
        out_specs=whole(),
        out_shape=jax.ShapeDtypeStruct((rows, width), BF16),
        scratch_shapes=[
            pltpu.VMEM(got.shape, BF16),
            pltpu.VMEM((groups, size, width), BF16),
            pltpu.VMEM(conv_part.shape, F32),
            pltpu.SemaphoreType.DMA((10,)),
        ],
        compiler_params=params(12),
        cost_estimate=cost(2 * rows * 1024 * width, 6 << 20),
        name="delta_out",
    )(blocks, got, home(conv_part), *sources)


def local(
    tokens,
    w_query,
    w_key,
    w_value,
    w_delta_gate,
    w_glu_value,
    w_glu_gate,
    w_conv_gate,
    w_beta,
    w_decay,
    decay_log,
    head_gain,
    conv_taps,
    ln_gain,
    ln_shift,
    out_delta,
    out_conv,
):
    rows = tokens.shape[0]
    half = rows // 2
    size = w_query.shape[1]
    y, core = lax.axis_index("y"), lax.axis_index("c")
    x, z = lax.axis_index("x"), lax.axis_index("z")
    count_y = lax.axis_size("y")
    head = y * 2 + core
    chips = [y, (y - 1) % count_y, (y + 1) % count_y, (y + 2) % count_y]
    blocks = jnp.stack([chip * 2 + side for chip in chips for side in (core, 1 - core)])
    blocks = blocks.astype(jnp.int32)

    beta_decay = jnp.concatenate(
        [
            lax.dynamic_slice_in_dim(w_beta, head, 1, 1),
            lax.dynamic_slice_in_dim(w_decay, head, 1, 1),
            jnp.zeros((w_beta.shape[0], 126), BF16),
        ],
        axis=1,
    )
    weights = (
        w_glu_value,
        w_glu_gate,
        w_delta_gate,
        w_conv_gate,
        w_query,
        w_key,
        w_value,
        beta_decay,
    )
    rate = jnp.exp(lax.dynamic_slice_in_dim(decay_log, head, 1, 0))

    def three(vector):
        high = lax.reduce_precision(vector, 8, 7)
        rest = vector - high
        middle = lax.reduce_precision(rest, 8, 7)
        return [high, middle, rest - middle]

    extra = jnp.stack(three(ln_gain) + three(ln_shift)).astype(BF16)
    extra = jnp.pad(extra, ((0, 10), (0, out_conv.shape[1] - extra.shape[1])))
    last = jnp.concatenate([out_delta, out_conv, extra], axis=0)

    own = tokens
    r1, l1 = cyclic(own, "y", 1), cyclic(own, "y", -1)
    sw = swapped(own)
    r1, l1, beta_decay, last = lax.optimization_barrier((r1, l1, beta_decay, last))
    weights = weights[:7] + (beta_decay,)
    fa, fb = cyclic(r1[:half], "y", 1), cyclic(l1[half:], "y", -1)
    sr1, sl1 = swapped(r1), swapped(l1)
    sfa, sfb = swapped(fa), swapped(fb)
    pieces = [own, sw, r1, sr1, l1, sl1, fa, sfa, fb, sfb]
    wr, wl = cyclic(last, "y", 1), cyclic(last, "y", -1)
    q, k, v, bl, dg, gu, cg = project(pieces, weights, blocks, rate, 2048, size)

    coef_p, coef_q, state = delta(q, k, v, bl)


    before, total = along(x, state, *(cyclic(state, "x", j) for j in (2, 3, 1)))
    route = lambda j: [(h + i, h + (i + j) % 4) for h in (0, 4) for i in range(4)]
    around = []
    for j in (2, 3, 1):
        around.append(lax.ppermute(total, "z", route(j)))
    before_z, total_z = along(z % 4, total, *around)
    far = shifted(total_z[:size, size:], "z", 4)

    ws = swapped(last)
    wr_top, wl_rest = wr[:size], wl[size:]
    wfa, wfb = cyclic(wr_top, "y", 1), cyclic(wl_rest, "y", -1)
    wsr, wsl = swapped(wr), swapped(wl)
    wsfa, wsfb = swapped(wfa), swapped(wfb)
    near = [last, ws, wr, wsr, wl, wsl]
    delta_weights = near + [wfa, wsfa]
    conv_weights = near + [wfb, wsfb]

    halo = lax.ppermute(gu[rows - 32 :], SP, [(i, i + 1) for i in range(31)])
    filtered = conv(gu, halo, conv_taps, cg)
    groups = 8
    got = lax.all_to_all(filtered.reshape(groups, rows // groups, 2 * size), TP, 0, 0, tiled=True)
    conv_part = conv_out(blocks, got, *conv_weights)

    mixed = finish(coef_p, coef_q, dg, head_gain[None, :], before_z, far, before)
    mixed = lax.all_to_all(mixed.reshape(groups, rows // groups, size), TP, 0, 0, tiled=True)
    return delta_out(blocks, mixed, conv_part, *delta_weights)


def solution(mesh):
    finer = Mesh(mesh.devices.reshape(8, 4, 4, 2), ("z", "x", "y", "c"))
    placed = (
        P(SP, TP),
        P(None, TP),
        P(None, TP),
        P(None, TP),
        P(None, TP),
        P(None, TP),
        P(None, TP),
        P(None, TP),
        P(),
        P(),
        P(),
        P(),
        P(None, TP),
        P(TP),
        P(TP),
        P(TP, None),
        P(TP, None),
    )
    return jax.shard_map(
        local, mesh=finer, in_specs=placed, out_specs=P(SP + TP, None), check_vma=False
    )
```

```python
import functools

import jax
import jax.numpy as jnp
from jax import lax
from jax.experimental import pallas as pl
from jax.experimental.pallas import tpu as pltpu
from jax.sharding import Mesh
from jax.sharding import PartitionSpec as P


SP = ("z", "x")
TP = ("y", "c")
TINY_NORM = 1e-06
TINY_VAR = 1e-05
CHUNK = 128
STEPS = (0, 1, -1, 2)
GOES_TO = (0, 1, 4, 5, 2, 3, 6, 7)
F32 = jnp.float32
BF16 = jnp.bfloat16


def whole():
    return pl.BlockSpec(memory_space=pltpu.VMEM)


def hbm():
    return pl.BlockSpec(memory_space=pltpu.HBM)


def anywhere():
    return pl.BlockSpec(memory_space=pl.ANY)


def home(array):
    return pltpu.with_memory_space_constraint(array, pltpu.HBM)


def near_core(array):
    return pltpu.with_memory_space_constraint(array, pltpu.VMEM)


def fetch(sems, *pairs):
    copies = [pltpu.make_async_copy(a, b, sems.at[n]) for n, (a, b) in enumerate(pairs)]
    for one in copies:
        one.start()
    return copies


def scalars():
    return pl.BlockSpec(memory_space=pltpu.SMEM)


def params(mib):
    return pltpu.CompilerParams(vmem_limit_bytes=min(mib * 1024 * 1024, 67043328))


def cost(flops, bytes_accessed):
    return pl.CostEstimate(flops=flops, bytes_accessed=bytes_accessed, transcendentals=0)


def dot(a, b):
    return jnp.dot(a, b, preferred_element_type=F32)


def dot_nt(a, b):
    return lax.dot_general(a, b, (((1,), (1,)), ((), ())), preferred_element_type=F32)


def dot_tn(a, b):
    return lax.dot_general(a, b, (((0,), (0,)), ((), ())), preferred_element_type=F32)


def low(a):
    return a.astype(BF16)


def split_two(a):
    high = a.astype(BF16)
    return high, (a - high.astype(F32)).astype(BF16)


def split_three(a):
    high = a.astype(BF16)
    rest = a - high.astype(F32)
    middle = rest.astype(BF16)
    return high, middle, (rest - middle.astype(F32)).astype(BF16)


def dot_fine(a, b):
    a_high, a_low = split_two(a)
    b_high, b_low = split_two(b)
    return dot(a_high, b_high) + (dot(a_high, b_low) + dot(a_low, b_high))


def project_kernel(width_all, head_size, block_ref, rate_ref, *refs):
    own, sw, r1, sr1, l1, sl1, fa, sfa, fb, sfb = refs[:10]
    sides = refs[10:18]
    q_ref, k_ref, v_ref, bl_ref, dg_hbm, gu_hbm, cg_hbm = refs[18:25]
    gathered, weights, factors, dg_ref, gu_ref, cg_ref, sems, out_sems = refs[25:]
    rows, piece_width = own.shape[0], own.shape[1]
    half = rows // 2
    places = [slice(0, half), slice(half, rows)]

    def columns(slot):
        return pl.ds(pl.multiple_of(block_ref[slot] * piece_width, piece_width), piece_width)

    moves = [[], []]
    for n, here in enumerate(places):
        for slot, ref in enumerate((own, sw, r1, sr1, l1, sl1)):
            moves[n].append((ref.at[here, :], gathered.at[here, columns(slot)]))
        for slot, ref in enumerate(((fa, sfa), (fb, sfb))[n]):
            moves[n].append((ref, gathered.at[here, columns(6 + slot)]))
    parts = [
        (ref, weights.at[n // 2, :, pl.ds(n % 2 * 128, 128)]) for n, ref in enumerate(sides)
    ]
    first = fetch(sems, *moves[0])
    loads = fetch(sems.at[pl.ds(16, 2)], *parts[:2])
    second = fetch(sems.at[pl.ds(8, 8)], *moves[1])
    loads += fetch(sems.at[pl.ds(18, 6)], *parts[2:])

    def unit_rows(raw):
        wide = low(raw).astype(F32)
        return wide * lax.rsqrt(jnp.sum(wide * wide, axis=-1, keepdims=True) + TINY_NORM)

    def pair(n, here):
        both = dot(gathered[here, :], weights[n]) * factors[here, :]
        return both[:, :128], both[:, 128:]

    def each_half(body):
        def step(n, carry):
            body(n, pl.ds(pl.multiple_of(n * half, half), half))
            return carry

        lax.fori_loop(0, 2, step, 0)

    def gated(n, here):
        for which, pieces in enumerate((first + loads[:2], second)):

            @pl.when(n == which)
            def _():
                for one in pieces:
                    one.wait()

        wide = gathered[here, :].astype(F32)
        squares = jnp.sum(wide * wide, axis=1, keepdims=True)
        factors[here, :] = lax.rsqrt(squares / width_all + TINY_NORM)
        gv, gg = pair(0, here)
        gu_ref[here, :] = low(low(gv).astype(F32) * jax.nn.sigmoid(low(gg).astype(F32)))

    def gates(n, here):
        dg, cg = pair(1, here)
        dg_ref[here, :] = low(dg)
        cg_ref[here, :] = low(cg)

    def queries(n, here):
        q, k = pair(2, here)
        q_ref[here, :] = low(unit_rows(q) * head_size ** (-0.5))
        k_ref[here, :] = low(unit_rows(k))

    def rest_of(n, here):
        v, bl = pair(3, here)
        v_ref[here, :] = low(v)
        lane = lax.broadcasted_iota(jnp.int32, bl.shape, 1)
        bl_ref[here, :] = jnp.where(
            lane == 0, jax.nn.sigmoid(bl), -rate_ref[0] * jax.nn.softplus(bl)
        )

    each_half(gated)
    stores = fetch(out_sems, (gu_ref, gu_hbm))
    for n, body in enumerate((gates, queries, rest_of)):
        for one in loads[2 * n + 2 : 2 * n + 4]:
            one.wait()
        each_half(body)
        if n == 0:
            stores += fetch(out_sems.at[pl.ds(1, 2)], (dg_ref, dg_hbm), (cg_ref, cg_hbm))
    for one in stores:
        one.wait()


def project(pieces, weights, blocks, rate, width_all, head_size):
    rows = pieces[0].shape[0]
    kinds = [BF16] * 3 + [F32] + [BF16] * 3
    return pl.pallas_call(
        functools.partial(project_kernel, width_all, head_size),
        in_specs=[scalars(), scalars()] + [anywhere()] * 18,
        out_specs=[whole()] * 4 + [hbm()] * 3,
        out_shape=[pltpu.VMEM((rows, 128), kind) for kind in kinds[:4]]
        + [pltpu.HBM((rows, 128), kind) for kind in kinds[4:]],
        scratch_shapes=[
            pltpu.VMEM((rows, width_all), BF16),
            pltpu.VMEM((4, width_all, 256), BF16),
            pltpu.VMEM((rows, 1), F32),
        ]
        + [pltpu.VMEM((rows, 128), BF16)] * 3
        + [pltpu.SemaphoreType.DMA((24,)), pltpu.SemaphoreType.DMA((3,))],
        compiler_params=params(28),
        cost_estimate=cost(2 * rows * width_all * 1024, 12 << 20),
        name="project",
    )(blocks, rate, home(pieces[0]), *pieces[1:], *map(home, weights))


def write_state(ref, state):
    total, lost, made = state
    size = lost.shape[0]
    ref[0:size, 0:size] = low(lost)
    ref[0:size, size:] = low(made)
    row = lax.broadcasted_iota(jnp.int32, (16, 2 * size), 0)
    high, middle, rest = split_three(jnp.broadcast_to(total, (16, 2 * size)))
    packed = jnp.where(
        row == 0,
        high.astype(F32),
        jnp.where(row == 1, middle.astype(F32), rest.astype(F32)),
    )
    ref[size : size + 16, :] = low(packed)


def read_state(ref):
    size = ref.shape[1] // 2
    packed = ref[size : size + 16, 0:128].astype(F32)
    total = packed[0:1, 0:1] + packed[1:2, 0:1] + packed[2:3, 0:1]
    return (total, ref[0:size, 0:size].astype(F32), ref[0:size, size:].astype(F32))


def compose(later, earlier):
    total2, lost2, made2 = later
    total1, lost1, made1 = earlier
    size = lost1.shape[0]
    both = dot(low(lost2), low(jnp.concatenate([lost1, made1], axis=1)))
    lost = total2 * lost1 + total1 * lost2 - both[:, :size]
    made = total2 * made1 - both[:, size:] + made2
    return (total1 * total2, lost, made)


def delta_kernel(
    q_ref, k_ref, v_ref, bl_ref, coef_p_hbm, coef_q_hbm, state_ref, coef_p_ref, coef_q_ref, sems
):
    rows, size = q_ref.shape
    chunks = rows // CHUNK
    row = lax.broadcasted_iota(jnp.int32, (CHUNK, CHUNK), 0)
    column = lax.broadcasted_iota(jnp.int32, (CHUNK, CHUNK), 1)
    causal = row >= column
    strict = row > column
    ones = jnp.where(causal, 1.0, 0.0).astype(BF16)
    lowers, inverses, scores, grown, tails = [], [], [], [], []
    betas = []
    for n in range(chunks):
        here = slice(n * CHUNK, (n + 1) * CHUNK)
        both = bl_ref[here, :]
        beta = both[:, 0:1]
        high, middle, rest = split_three(both)
        sums = dot(ones, high) + (dot(ones, middle) + dot(ones, rest))
        log_sum = jnp.broadcast_to(sums[:, 1:2], (CHUNK, CHUNK))
        damping = jnp.where(causal, jnp.exp(jnp.minimum(log_sum - log_sum.T, 0.0)), 0.0)
        k = k_ref[here, :]
        lower = jnp.where(strict, dot_nt(k, k) * damping, 0.0) * beta
        scores.append(low(dot_nt(q_ref[here, :], k) * damping))
        lowers.append(lower)
        betas.append(beta)
        grown.append(log_sum)
        tails.append(log_sum[CHUNK - 1 : CHUNK, :])
        below = ((row & 1) == 1) & (column == row - 1)
        inverses.append(jnp.where(row == column, 1.0, 0.0) - jnp.where(below, lower, 0.0))
    level = 2
    while level < CHUNK:
        shift = level.bit_length() - 1
        part = row >> shift
        below = ((part & 1) == 1) & ((column >> shift) == part - 1)
        multiply = dot_fine if level >= 16 else (lambda a, b: dot(low(a), low(b)))
        moved = [
            multiply(inverse, jnp.where(below, lower, 0.0))
            for inverse, lower in zip(inverses, lowers)
        ]
        inverses = [
            inverse - multiply(middle, inverse) for inverse, middle in zip(inverses, moved)
        ]
        level *= 2
    queries, starts, losts, mades = [], [], [], []
    for n in range(chunks):
        here = slice(n * CHUNK, (n + 1) * CHUNK)
        k = k_ref[here, :].astype(F32)
        grow = jnp.exp(grown[n])
        right = jnp.concatenate(
            [v_ref[here, :].astype(F32) * betas[n], k * (betas[n] * grow)], axis=1
        )
        solved = low(dot(low(inverses[n]), low(right)))
        seen = dot(scores[n], solved)
        starts.append(seen[:, :size])
        queries.append(low(q_ref[here, :].astype(F32) * grow - seen[:, size:]))
        weighted = low(k * jnp.exp(tails[n] - grown[n]))
        written = dot_tn(weighted, solved)
        mades.append(written[:, :size])
        losts.append(low(written[:, size:]))
    carried = jnp.where(row == column, 1.0, 0.0)
    made = jnp.zeros((CHUNK, size), F32)
    log_total = jnp.zeros((1, CHUNK), F32)
    stores = []
    for n in range(chunks):
        here = slice(n * CHUNK, (n + 1) * CHUNK)
        rounded = low(jnp.concatenate([carried, made], axis=1))
        seen = dot(queries[n], rounded)
        coef_p_ref[here, :] = low(seen[:, :size])
        coef_q_ref[here, :] = seen[:, size:] + starts[n]
        stores += fetch(
            sems.at[n],
            (coef_p_ref.at[here, :], coef_p_hbm.at[here, :]),
            (coef_q_ref.at[here, :], coef_q_hbm.at[here, :]),
        )
        moved = dot(losts[n], rounded)
        keep = jnp.exp(tails[n])
        carried = carried * keep - moved[:, :size]
        made = made * keep - moved[:, size:] + mades[n]
        log_total = log_total + tails[n]
    total = jnp.exp(log_total)[:, 0:1]
    lost = jnp.where(row == column, total, 0.0) - carried
    write_state(state_ref, (total, lost, made))
    for one in stores:
        one.wait()


def delta(q, k, v, bl):
    rows, size = q.shape
    return pl.pallas_call(
        delta_kernel,
        in_specs=[whole()] * 4,
        out_specs=[hbm(), hbm(), whole()],
        out_shape=[
            pltpu.HBM((rows, size), BF16),
            pltpu.HBM((rows, size), F32),
            pltpu.VMEM((size + 16, 2 * size), BF16),
        ],
        scratch_shapes=[
            pltpu.VMEM((rows, size), BF16),
            pltpu.VMEM((rows, size), F32),
            pltpu.SemaphoreType.DMA((rows // CHUNK, 2)),
        ],
        compiler_params=params(16),
        cost_estimate=cost(2 * rows * size * size * 60, 3 << 20),
        name="delta",
    )(q, k, v, bl)


def along_kernel(which, place_ref, p0, p1, p2, p3, before_ref, total_ref, held):
    me = place_ref[which]
    for j, piece in ((0, p0), (2, p1), (3, p2), (1, p3)):
        held[(me - j + 4) & 3] = piece[...]
    size = p0.shape[1] // 2
    nothing = (jnp.ones((1, 1), F32), jnp.zeros((size, size), F32), jnp.zeros((size, size), F32))
    before = nothing
    so_far = read_state(held.at[0])
    for m in range(1, 4):
        before = tuple(jnp.where(me == m, a, b) for a, b in zip(so_far, before))
        so_far = compose(read_state(held.at[m]), so_far)
    write_state(before_ref, before)
    write_state(total_ref, so_far)


def along(which, places, state, *others):
    return pl.pallas_call(
        functools.partial(along_kernel, which),
        in_specs=[scalars()] + [whole()] * 4,
        out_specs=[whole(), whole()],
        out_shape=[
            jax.ShapeDtypeStruct(state.shape, BF16),
            pltpu.VMEM(state.shape, BF16),
        ],
        scratch_shapes=[pltpu.VMEM((4,) + state.shape, BF16)],
        compiler_params=params(4),
        cost_estimate=cost(16 << 20, 1 << 18),
        name="along",
    )(places, *map(near_core, (state,) + others))


def cyclic(block, axis, distance):
    count = lax.axis_size(axis)
    return lax.ppermute(block, axis, [(i, (i + distance) % count) for i in range(count)])


def shifted(block, axis, distance):
    devices = range(lax.axis_size(axis))
    return lax.ppermute(block, axis, [(i, i + distance) for i in devices if i + distance in devices])


def swapped(block):
    return lax.ppermute(block, "c", [(0, 1), (1, 0)])


def exchanged(parts):
    got = [parts[0]]
    for slot in range(1, 8):
        step, side = STEPS[slot // 2], slot % 2
        route = [(y * 2 + c, (y + step) % 4 * 2 + (c ^ side)) for y in range(4) for c in range(2)]
        got.append(lax.ppermute(parts[slot], TP, route))
    return got


def finish_kernel(
    block_ref, coef_p_hbm, coef_q_hbm, dg_hbm, gain_ref, reach_any, far_any, before_hbm, *rest
):
    outs, scratch = rest[:8], rest[8:]
    coef_p_ref, coef_q_ref, dg_ref, reach_ref, far_ref, before_ref, out_ref, sems, out_sems = scratch
    loads = fetch(
        sems,
        (reach_any, reach_ref),
        (far_any, far_ref),
        (before_hbm, before_ref),
        (coef_p_hbm, coef_p_ref),
        (coef_q_hbm, coef_q_ref),
        (dg_hbm, dg_ref),
    )
    for one in loads[:3]:
        one.wait()
    total, lost, made = read_state(reach_ref)
    state = total * far_ref[...].astype(F32) - dot(low(lost), far_ref[...]) + made
    total, lost, made = read_state(before_ref)
    state = low(total * state - dot(low(lost), low(state)) + made)
    for one in loads[3:]:
        one.wait()
    stores = []
    step = out_ref.shape[1]
    for slot in range(8):
        here = pl.ds(pl.multiple_of(block_ref[GOES_TO[slot]] * step, step), step)
        result = coef_q_ref[here, :] + dot(coef_p_ref[here, :], state)
        mean = jnp.sum(result * result, axis=-1, keepdims=True) * (1.0 / result.shape[1])
        result = result * lax.rsqrt(mean + TINY_NORM) * gain_ref[...]
        out_ref[slot] = low(result * jax.nn.silu(dg_ref[here, :].astype(F32)))
        stores += fetch(out_sems.at[pl.ds(slot, 1)], (out_ref.at[slot], outs[slot]))
    for one in stores:
        one.wait()


def finish(blocks, coef_p, coef_q, dg, gain, reach, far, before):
    coef_p, coef_q, dg = map(home, (coef_p, coef_q, dg))
    rows, size = dg.shape
    args = (coef_p, coef_q, dg, gain, reach, far, before)
    copied = (coef_p, coef_q, dg, reach, far, before)
    return pl.pallas_call(
        finish_kernel,
        in_specs=[scalars(), hbm(), hbm(), hbm(), whole(), anywhere(), anywhere(), anywhere()],
        out_specs=[hbm()] * 8,
        out_shape=[pltpu.HBM((rows // 8, size), BF16)] * 8,
        scratch_shapes=[pltpu.VMEM(a.shape, a.dtype) for a in copied]
        + [pltpu.VMEM((8, rows // 8, size), BF16)]
        + [pltpu.SemaphoreType.DMA((6,)), pltpu.SemaphoreType.DMA((8,))],
        compiler_params=params(8),
        cost_estimate=cost(64 << 20, 2 << 20),
        name="finish",
    )(blocks, *args)


def conv_kernel(block_ref, gu_hbm, before_any, taps_ref, cg_hbm, *rest):
    outs = rest[:8]
    gu_ref, before_ref, padded, out_ref, sems, out_sems = rest[8:]
    rows, size = gu_ref.shape
    head = before_ref.shape[0]
    count = taps_ref.shape[0]
    gate = pltpu.make_async_copy(cg_hbm, out_ref.at[:, pl.ds(size, size)], sems.at[2])
    gate.start()
    for one in fetch(sems, (gu_hbm, gu_ref), (before_any, before_ref)):
        one.wait()
    padded[0:head, :] = before_ref[...].astype(F32)
    padded[head:, :] = gu_ref[...].astype(F32)
    taps = taps_ref[...].astype(F32)
    step = 64
    skip = head - (count - 1)

    def block(n, carry):
        base = pl.multiple_of(n * step, step)
        total = jnp.zeros((step, size), F32)
        for j in range(count):
            total = total + padded[pl.ds(base + skip + j, step), :] * taps[j : j + 1, :]
        out_ref[pl.ds(base, step), 0:size] = low(total)
        return carry

    lax.fori_loop(0, rows // step, block, 0)
    gate.wait()
    part = rows // 8
    pairs = []
    for slot in range(8):
        here = pl.ds(pl.multiple_of(block_ref[GOES_TO[slot]] * part, part), part)
        pairs.append((out_ref.at[here, :], outs[slot]))
    for one in fetch(out_sems, *pairs):
        one.wait()


def conv(blocks, gu, before, taps, cg):
    rows, size = gu.shape
    return pl.pallas_call(
        conv_kernel,
        in_specs=[scalars(), hbm(), anywhere(), whole(), hbm()],
        out_specs=[hbm()] * 8,
        out_shape=[pltpu.HBM((rows // 8, 2 * size), BF16)] * 8,
        scratch_shapes=[
            pltpu.VMEM(gu.shape, BF16),
            pltpu.VMEM(before.shape, BF16),
            pltpu.VMEM((rows + before.shape[0], size), F32),
            pltpu.VMEM((rows, 2 * size), BF16),
            pltpu.SemaphoreType.DMA((3,)),
            pltpu.SemaphoreType.DMA((8,)),
        ],
        compiler_params=params(8),
        cost_estimate=cost(256 << 20, 1 << 20),
        name="conv",
    )(blocks, home(gu), before, taps, home(cg))


def add_slots(out_ref, slots, left, weights, start):
    size = weights.shape[1] - weights.shape[1] % 128

    def step(n, carry):
        here = pl.ds(pl.multiple_of(n * 512, 512), 512)
        acc = jnp.zeros((out_ref.shape[0], 512), F32) if start is None else start[:, here]
        for slot in slots:
            acc = acc + dot(left(slot), weights[slot, 0:size, here])
        out_ref[:, here] = acc.astype(out_ref.dtype)
        return carry

    lax.fori_loop(0, out_ref.shape[1] // 512, step, 0)


def cut_kernel(right_any, left_any, top_hbm, rest_hbm, top, rest, sems):
    count = top.shape[0]
    inward = fetch(
        sems,
        (right_any.at[pl.ds(0, count), :], top),
        (left_any.at[pl.ds(count, rest.shape[0]), :], rest),
    )
    outward = []
    for n, pair in enumerate(((top, top_hbm), (rest, rest_hbm))):
        inward[n].wait()
        outward += fetch(sems.at[pl.ds(2 + n, 1)], pair)
    for one in outward:
        one.wait()


def cut(right, left, count):
    rows, width = right.shape
    shapes = [(count, width), (rows - count, width)]
    return pl.pallas_call(
        cut_kernel,
        in_specs=[anywhere()] * 2,
        out_specs=[hbm()] * 2,
        out_shape=[pltpu.HBM(shape, BF16) for shape in shapes],
        scratch_shapes=[pltpu.VMEM(shape, BF16) for shape in shapes]
        + [pltpu.SemaphoreType.DMA((4,))],
        compiler_params=params(4),
        cost_estimate=cost(1 << 20, 4 << 20),
        name="cut",
    )(right, left)


def conv_out_kernel(*refs):
    got, sources, out_hbm = refs[:8], refs[8:16], refs[16]
    got_ref, weights, mixed, out_ref, sems, out_sems = refs[17:]
    groups, rows, size = mixed.shape
    got_loads = fetch(
        sems.at[pl.ds(8, 8)], *((ref, got_ref.at[slot]) for slot, ref in enumerate(got))
    )
    loads = fetch(
        sems,
        *(
            (ref.at[pl.ds(0 if ref.shape[0] == size + 16 else size, size + 16), :], weights.at[slot])
            for slot, ref in enumerate(sources)
        ),
    )
    for one in got_loads:
        one.wait()
    total = jnp.zeros((rows, size), F32)
    total_square = jnp.zeros((rows, size), F32)
    for g in range(groups):
        part = got_ref[g, :, 0:size].astype(F32)
        total = total + part
        total_square = total_square + part * part
    scale = 1.0 / (groups * size)
    center = jnp.sum(total, axis=1, keepdims=True) * scale
    second = jnp.sum(total_square, axis=1, keepdims=True) * scale
    factor = lax.rsqrt(jnp.maximum(second - center * center, 0.0) + TINY_VAR)
    for half in range(2):
        slots = range(half * 4, half * 4 + 4)
        for slot in slots:
            loads[slot].wait()
            extra = weights[slot, size : size + 16, :].astype(F32)
            gain = extra[0:1, 0:size] + extra[1:2, 0:size] + extra[2:3, 0:size]
            shift = extra[3:4, 0:size] + extra[4:5, 0:size] + extra[5:6, 0:size]
            normed = (got_ref[slot, :, 0:size].astype(F32) - center) * factor * gain + shift
            gate = got_ref[slot, :, size:].astype(F32)
            mixed[slot] = low(jax.nn.silu(normed) * jax.nn.silu(gate))
        add_slots(
            out_ref, slots, lambda slot: mixed[slot], weights, out_ref if half else None
        )
    (store,) = fetch(out_sems, (out_ref, out_hbm))
    store.wait()


def conv_out(got, sources):
    groups = len(got)
    rows, both = got[0].shape
    size, width = both // 2, sources[0].shape[1]
    return pl.pallas_call(
        conv_out_kernel,
        in_specs=[anywhere()] * 16,
        out_specs=hbm(),
        out_shape=pltpu.HBM((rows, width), F32),
        scratch_shapes=[
            pltpu.VMEM((groups, rows, both), BF16),
            pltpu.VMEM((groups, size + 16, width), BF16),
            pltpu.VMEM((groups, rows, size), BF16),
            pltpu.VMEM((rows, width), F32),
            pltpu.SemaphoreType.DMA((16,)),
            pltpu.SemaphoreType.DMA((1,)),
        ],
        compiler_params=params(12),
        cost_estimate=cost(2 * rows * 1024 * width, 6 << 20),
        name="conv_out",
    )(*got, *sources)


def delta_out_kernel(conv_hbm, *refs):
    got, sources, out_ref = refs[:8], refs[8:16], refs[16]
    got_ref, weights, conv_ref, sems = refs[17:]
    size = got_ref.shape[1]
    loads = fetch(
        sems,
        (conv_hbm, conv_ref),
        *((ref, got_ref.at[slot]) for slot, ref in enumerate(got)),
        *((ref.at[pl.ds(0, size), :], weights.at[slot]) for slot, ref in enumerate(sources)),
    )
    for one in loads[:9]:
        one.wait()
    for half in range(2):
        slots = range(half * 4, half * 4 + 4)
        for slot in slots:
            loads[9 + slot].wait()
        add_slots(
            out_ref if half else conv_ref,
            slots,
            lambda slot: got_ref[slot],
            weights,
            conv_ref,
        )


def delta_out(got, conv_part, sources):
    groups = len(got)
    rows, size = got[0].shape
    width = conv_part.shape[1]
    return pl.pallas_call(
        delta_out_kernel,
        in_specs=[anywhere()] * 17,
        out_specs=whole(),
        out_shape=jax.ShapeDtypeStruct((rows, width), BF16),
        scratch_shapes=[
            pltpu.VMEM((groups, rows, size), BF16),
            pltpu.VMEM((groups, size, width), BF16),
            pltpu.VMEM(conv_part.shape, F32),
            pltpu.SemaphoreType.DMA((17,)),
        ],
        compiler_params=params(12),
        cost_estimate=cost(2 * rows * 1024 * width, 6 << 20),
        name="delta_out",
    )(home(conv_part), *got, *sources)


def local(
    tokens,
    w_query,
    w_key,
    w_value,
    w_delta_gate,
    w_glu_value,
    w_glu_gate,
    w_conv_gate,
    w_beta,
    w_decay,
    decay_log,
    head_gain,
    conv_taps,
    ln_gain,
    ln_shift,
    out_delta,
    out_conv,
):
    rows = tokens.shape[0]
    half = rows // 2
    size = w_query.shape[1]
    y, core = lax.axis_index("y"), lax.axis_index("c")
    x, z = lax.axis_index("x"), lax.axis_index("z")
    count_y = lax.axis_size("y")
    head = y * 2 + core
    chips = [y, (y - 1) % count_y, (y + 1) % count_y, (y + 2) % count_y]
    slots = [chip * 2 + side for chip in chips for side in (core, 1 - core)]
    blocks = jnp.stack(slots + [x, z % 4])
    blocks = blocks.astype(jnp.int32)

    beta_decay = jnp.concatenate(
        [
            lax.dynamic_slice_in_dim(w_beta, head, 1, 1),
            lax.dynamic_slice_in_dim(w_decay, head, 1, 1),
            jnp.zeros((w_beta.shape[0], 126), BF16),
        ],
        axis=1,
    )
    weights = (
        w_glu_value,
        w_glu_gate,
        w_delta_gate,
        w_conv_gate,
        w_query,
        w_key,
        w_value,
        beta_decay,
    )
    rate = jnp.exp(lax.dynamic_slice_in_dim(decay_log, head, 1, 0))

    def three(vector):
        high = lax.reduce_precision(vector, 8, 7)
        rest = vector - high
        middle = lax.reduce_precision(rest, 8, 7)
        return [high, middle, rest - middle]

    extra = jnp.stack(three(ln_gain) + three(ln_shift)).astype(BF16)
    extra = jnp.pad(extra, ((0, 10), (0, out_conv.shape[1] - extra.shape[1])))
    last = jnp.concatenate([out_delta, out_conv, extra], axis=0)

    own = tokens
    r1, l1 = cyclic(own, "y", 1), cyclic(own, "y", -1)
    sw = swapped(own)
    r1, l1, beta_decay, last = lax.optimization_barrier((r1, l1, beta_decay, last))
    weights = weights[:7] + (beta_decay,)
    fa, fb = cyclic(r1[:half], "y", 1), cyclic(l1[half:], "y", -1)
    sr1, sl1 = swapped(r1), swapped(l1)
    sfa, sfb = swapped(fa), swapped(fb)
    pieces = [own, sw, r1, sr1, l1, sl1, fa, sfa, fb, sfb]
    wr, wl = cyclic(last, "y", 1), cyclic(last, "y", -1)
    q, k, v, bl, dg, gu, cg = project(pieces, weights, blocks, rate, 2048, size)

    coef_p, coef_q, state = delta(q, k, v, bl)


    before, total = along(8, blocks, state, *(cyclic(state, "x", j) for j in (2, 3, 1)))
    route = lambda j: [(h + i, h + (i + j) % 4) for h in (0, 4) for i in range(4)]
    around = []
    for j in (2, 3, 1):
        around.append(lax.ppermute(total, "z", route(j)))
    before_z, total_z = along(9, blocks, total, *around)
    far = shifted(total_z[:size, size:], "z", 4)

    ws = swapped(last)
    wr_top, wl_rest = cut(wr, wl, size)
    wfa, wfb = cyclic(wr_top, "y", 1), cyclic(wl_rest, "y", -1)
    wsr, wsl = swapped(wr), swapped(wl)
    wsfa, wsfb = swapped(wfa), swapped(wfb)
    near = [last, ws, wr, wsr, wl, wsl]
    delta_weights = near + [wfa, wsfa]
    conv_weights = near + [wfb, wsfb]

    halo = lax.ppermute(gu[rows - 32 :], SP, [(i, i + 1) for i in range(31)])
    filtered = conv(blocks, gu, halo, conv_taps, cg)
    got = exchanged(filtered)
    conv_part = conv_out(got, conv_weights)

    mixed = finish(blocks, coef_p, coef_q, dg, head_gain[None, :], before_z, far, before)
    return delta_out(exchanged(mixed), conv_part, delta_weights)


def solution(mesh):
    finer = Mesh(mesh.devices.reshape(8, 4, 4, 2), ("z", "x", "y", "c"))
    placed = (
        P(SP, TP),
        P(None, TP),
        P(None, TP),
        P(None, TP),
        P(None, TP),
        P(None, TP),
        P(None, TP),
        P(None, TP),
        P(),
        P(),
        P(),
        P(),
        P(None, TP),
        P(TP),
        P(TP),
        P(TP, None),
        P(TP, None),
    )
    return jax.shard_map(
        local, mesh=finer, in_specs=placed, out_specs=P(SP + TP, None), check_vma=False
    )
```

```python
import functools

import jax
import jax.numpy as jnp
from jax import lax
from jax.experimental import pallas as pl
from jax.experimental.pallas import tpu as pltpu
from jax.sharding import Mesh
from jax.sharding import PartitionSpec as P


SP = ("z", "x")
TP = ("y", "c")
TINY_NORM = 1e-06
TINY_VAR = 1e-05
CHUNK = 128
HALO = 32
STEPS = (0, 1, -1, 2)
GOES_TO = (0, 1, 4, 5, 2, 3, 6, 7)
F32 = jnp.float32
BF16 = jnp.bfloat16


def whole():
    return pl.BlockSpec(memory_space=pltpu.VMEM)


def hbm():
    return pl.BlockSpec(memory_space=pltpu.HBM)


def anywhere():
    return pl.BlockSpec(memory_space=pl.ANY)


def home(array):
    return pltpu.with_memory_space_constraint(array, pltpu.HBM)


def near_core(array):
    return pltpu.with_memory_space_constraint(array, pltpu.VMEM)


def fetch(sems, *pairs):
    copies = [pltpu.make_async_copy(a, b, sems.at[n]) for n, (a, b) in enumerate(pairs)]
    for one in copies:
        one.start()
    return copies


def scalars():
    return pl.BlockSpec(memory_space=pltpu.SMEM)


def params(mib):
    return pltpu.CompilerParams(vmem_limit_bytes=min(mib * 1024 * 1024, 67043328))


def cost(flops, bytes_accessed):
    return pl.CostEstimate(flops=flops, bytes_accessed=bytes_accessed, transcendentals=0)


def dot(a, b):
    return jnp.dot(a, b, preferred_element_type=F32)


def dot_nt(a, b):
    return lax.dot_general(a, b, (((1,), (1,)), ((), ())), preferred_element_type=F32)


def dot_tn(a, b):
    return lax.dot_general(a, b, (((0,), (0,)), ((), ())), preferred_element_type=F32)


def low(a):
    return a.astype(BF16)


def split_two(a):
    high = a.astype(BF16)
    return high, (a - high.astype(F32)).astype(BF16)


def split_three(a):
    high = a.astype(BF16)
    rest = a - high.astype(F32)
    middle = rest.astype(BF16)
    return high, middle, (rest - middle.astype(F32)).astype(BF16)


def dot_fine(a, b):
    a_high, a_low = split_two(a)
    b_high, b_low = split_two(b)
    return dot(a_high, b_high) + (dot(a_high, b_low) + dot(a_low, b_high))


def project_kernel(width_all, head_size, block_ref, rate_ref, *refs):
    own, sw, r1, sr1, l1, sl1, fa, sfa, fb, sfb = refs[:10]
    sides = refs[10:18]
    q_ref, k_ref, v_ref, bl_ref, tail_ref, dg_hbm, gu_hbm, cg_hbm = refs[18:26]
    gathered, weights, factors, dg_ref, gu_ref, cg_ref, sems, out_sems = refs[26:]
    rows, piece_width = own.shape[0], own.shape[1]
    half = rows // 2
    places = [slice(0, half), slice(half, rows)]

    def columns(slot):
        return pl.ds(pl.multiple_of(block_ref[slot] * piece_width, piece_width), piece_width)

    moves = [[], []]
    for n, here in enumerate(places):
        for slot, ref in enumerate((own, sw, r1, sr1, l1, sl1)):
            moves[n].append((ref.at[here, :], gathered.at[here, columns(slot)]))
        for slot, ref in enumerate(((fa, sfa), (fb, sfb))[n]):
            moves[n].append((ref, gathered.at[here, columns(6 + slot)]))
    parts = [
        (ref, weights.at[n // 2, :, pl.ds(n % 2 * 128, 128)]) for n, ref in enumerate(sides)
    ]
    first = fetch(sems, *moves[0])
    loads = fetch(sems.at[pl.ds(16, 2)], *parts[:2])
    second = fetch(sems.at[pl.ds(8, 8)], *moves[1])
    loads += fetch(sems.at[pl.ds(18, 6)], *parts[2:])

    def unit_rows(raw):
        wide = low(raw).astype(F32)
        return wide * lax.rsqrt(jnp.sum(wide * wide, axis=-1, keepdims=True) + TINY_NORM)

    def pair(n, here):
        both = dot(gathered[here, :], weights[n]) * factors[here, :]
        return both[:, :128], both[:, 128:]

    def each_half(body):
        def step(n, carry):
            body(n, pl.ds(pl.multiple_of(n * half, half), half))
            return carry

        lax.fori_loop(0, 2, step, 0)

    def gated(n, here):
        for which, pieces in enumerate((first + loads[:2], second)):

            @pl.when(n == which)
            def _():
                for one in pieces:
                    one.wait()

        wide = gathered[here, :].astype(F32)
        squares = jnp.sum(wide * wide, axis=1, keepdims=True)
        factors[here, :] = lax.rsqrt(squares / width_all + TINY_NORM)
        gv, gg = pair(0, here)
        gu_ref[here, :] = low(low(gv).astype(F32) * jax.nn.sigmoid(low(gg).astype(F32)))

    def gates(n, here):
        dg, cg = pair(1, here)
        dg_ref[here, :] = low(dg)
        cg_ref[here, :] = low(cg)

    def queries(n, here):
        q, k = pair(2, here)
        q_ref[here, :] = low(unit_rows(q) * head_size ** (-0.5))
        k_ref[here, :] = low(unit_rows(k))

    def rest_of(n, here):
        v, bl = pair(3, here)
        v_ref[here, :] = low(v)
        lane = lax.broadcasted_iota(jnp.int32, bl.shape, 1)
        bl_ref[here, :] = jnp.where(
            lane == 0, jax.nn.sigmoid(bl), -rate_ref[0] * jax.nn.softplus(bl)
        )

    each_half(gated)
    tail_ref[...] = gu_ref[rows - HALO :, :]
    stores = fetch(out_sems, (gu_ref, gu_hbm))
    for n, body in enumerate((gates, queries, rest_of)):
        for one in loads[2 * n + 2 : 2 * n + 4]:
            one.wait()
        each_half(body)
        if n == 0:
            stores += fetch(out_sems.at[pl.ds(1, 2)], (dg_ref, dg_hbm), (cg_ref, cg_hbm))
    for one in stores:
        one.wait()


def project(pieces, weights, blocks, rate, width_all, head_size):
    rows = pieces[0].shape[0]
    kinds = [BF16] * 3 + [F32] + [BF16] * 3
    return pl.pallas_call(
        functools.partial(project_kernel, width_all, head_size),
        in_specs=[scalars(), scalars()] + [anywhere()] * 18,
        out_specs=[whole()] * 5 + [hbm()] * 3,
        out_shape=[pltpu.VMEM((rows, 128), kind) for kind in kinds[:4]]
        + [pltpu.VMEM((HALO, 128), BF16)]
        + [pltpu.HBM((rows, 128), kind) for kind in kinds[4:]],
        scratch_shapes=[
            pltpu.VMEM((rows, width_all), BF16),
            pltpu.VMEM((4, width_all, 256), BF16),
            pltpu.VMEM((rows, 1), F32),
        ]
        + [pltpu.VMEM((rows, 128), BF16)] * 3
        + [pltpu.SemaphoreType.DMA((24,)), pltpu.SemaphoreType.DMA((3,))],
        compiler_params=params(28),
        cost_estimate=cost(2 * rows * width_all * 1024, 12 << 20),
        name="project",
    )(blocks, rate, home(pieces[0]), *pieces[1:], *map(home, weights))


def write_state(ref, state):
    total, lost, made = state
    size = lost.shape[0]
    ref[0:size, 0:size] = low(lost)
    ref[0:size, size:] = low(made)
    row = lax.broadcasted_iota(jnp.int32, (16, 2 * size), 0)
    high, middle, rest = split_three(jnp.broadcast_to(total, (16, 2 * size)))
    packed = jnp.where(
        row == 0,
        high.astype(F32),
        jnp.where(row == 1, middle.astype(F32), rest.astype(F32)),
    )
    ref[size : size + 16, :] = low(packed)


def read_state(ref):
    size = ref.shape[1] // 2
    packed = ref[size : size + 16, 0:128].astype(F32)
    total = packed[0:1, 0:1] + packed[1:2, 0:1] + packed[2:3, 0:1]
    return (total, ref[0:size, 0:size].astype(F32), ref[0:size, size:].astype(F32))


def compose(later, earlier):
    total2, lost2, made2 = later
    total1, lost1, made1 = earlier
    size = lost1.shape[0]
    both = dot(low(lost2), low(jnp.concatenate([lost1, made1], axis=1)))
    lost = total2 * lost1 + total1 * lost2 - both[:, :size]
    made = total2 * made1 - both[:, size:] + made2
    return (total1 * total2, lost, made)


def delta_kernel(
    q_ref, k_ref, v_ref, bl_ref, coef_p_hbm, coef_q_hbm, state_ref, coef_p_ref, coef_q_ref, sems
):
    rows, size = q_ref.shape
    chunks = rows // CHUNK
    row = lax.broadcasted_iota(jnp.int32, (CHUNK, CHUNK), 0)
    column = lax.broadcasted_iota(jnp.int32, (CHUNK, CHUNK), 1)
    causal = row >= column
    strict = row > column
    ones = jnp.where(causal, 1.0, 0.0).astype(BF16)
    lowers, inverses, scores, grown, tails = [], [], [], [], []
    betas = []
    for n in range(chunks):
        here = slice(n * CHUNK, (n + 1) * CHUNK)
        both = bl_ref[here, :]
        beta = both[:, 0:1]
        high, middle, rest = split_three(both)
        sums = dot(ones, high) + (dot(ones, middle) + dot(ones, rest))
        log_sum = jnp.broadcast_to(sums[:, 1:2], (CHUNK, CHUNK))
        damping = jnp.where(causal, jnp.exp(jnp.minimum(log_sum - log_sum.T, 0.0)), 0.0)
        k = k_ref[here, :]
        lower = jnp.where(strict, dot_nt(k, k) * damping, 0.0) * beta
        scores.append(low(dot_nt(q_ref[here, :], k) * damping))
        lowers.append(lower)
        betas.append(beta)
        grown.append(log_sum)
        tails.append(log_sum[CHUNK - 1 : CHUNK, :])
        below = ((row & 1) == 1) & (column == row - 1)
        inverses.append(jnp.where(row == column, 1.0, 0.0) - jnp.where(below, lower, 0.0))
    level = 2
    while level < CHUNK:
        shift = level.bit_length() - 1
        part = row >> shift
        below = ((part & 1) == 1) & ((column >> shift) == part - 1)
        multiply = dot_fine if level >= 16 else (lambda a, b: dot(low(a), low(b)))
        moved = [
            multiply(inverse, jnp.where(below, lower, 0.0))
            for inverse, lower in zip(inverses, lowers)
        ]
        inverses = [
            inverse - multiply(middle, inverse) for inverse, middle in zip(inverses, moved)
        ]
        level *= 2
    queries, starts, losts, mades = [], [], [], []
    for n in range(chunks):
        here = slice(n * CHUNK, (n + 1) * CHUNK)
        k = k_ref[here, :].astype(F32)
        grow = jnp.exp(grown[n])
        right = jnp.concatenate(
            [v_ref[here, :].astype(F32) * betas[n], k * (betas[n] * grow)], axis=1
        )
        solved = low(dot(low(inverses[n]), low(right)))
        seen = dot(scores[n], solved)
        starts.append(seen[:, :size])
        queries.append(low(q_ref[here, :].astype(F32) * grow - seen[:, size:]))
        weighted = low(k * jnp.exp(tails[n] - grown[n]))
        written = dot_tn(weighted, solved)
        mades.append(written[:, :size])
        losts.append(low(written[:, size:]))
    carried = jnp.where(row == column, 1.0, 0.0)
    made = jnp.zeros((CHUNK, size), F32)
    log_total = jnp.zeros((1, CHUNK), F32)
    stores = []
    for n in range(chunks):
        here = slice(n * CHUNK, (n + 1) * CHUNK)
        rounded = low(jnp.concatenate([carried, made], axis=1))
        seen = dot(queries[n], rounded)
        coef_p_ref[here, :] = low(seen[:, :size])
        coef_q_ref[here, :] = seen[:, size:] + starts[n]
        stores += fetch(
            sems.at[n],
            (coef_p_ref.at[here, :], coef_p_hbm.at[here, :]),
            (coef_q_ref.at[here, :], coef_q_hbm.at[here, :]),
        )
        moved = dot(losts[n], rounded)
        keep = jnp.exp(tails[n])
        carried = carried * keep - moved[:, :size]
        made = made * keep - moved[:, size:] + mades[n]
        log_total = log_total + tails[n]
    total = jnp.exp(log_total)[:, 0:1]
    lost = jnp.where(row == column, total, 0.0) - carried
    write_state(state_ref, (total, lost, made))
    for one in stores:
        one.wait()


def delta(q, k, v, bl):
    rows, size = q.shape
    return pl.pallas_call(
        delta_kernel,
        in_specs=[whole()] * 4,
        out_specs=[hbm(), hbm(), whole()],
        out_shape=[
            pltpu.HBM((rows, size), BF16),
            pltpu.HBM((rows, size), F32),
            pltpu.VMEM((size + 16, 2 * size), BF16),
        ],
        scratch_shapes=[
            pltpu.VMEM((rows, size), BF16),
            pltpu.VMEM((rows, size), F32),
            pltpu.SemaphoreType.DMA((rows // CHUNK, 2)),
        ],
        compiler_params=params(16),
        cost_estimate=cost(2 * rows * size * size * 60, 3 << 20),
        name="delta",
    )(q, k, v, bl)


def along_kernel(which, place_ref, p0, p1, p2, p3, before_ref, total_ref, made_ref, held):
    me = place_ref[which]
    for j, piece in ((0, p0), (2, p1), (3, p2), (1, p3)):
        held[(me - j + 4) & 3] = piece[...]
    size = p0.shape[1] // 2
    nothing = (jnp.ones((1, 1), F32), jnp.zeros((size, size), F32), jnp.zeros((size, size), F32))
    before = nothing
    so_far = read_state(held.at[0])
    for m in range(1, 4):
        before = tuple(jnp.where(me == m, a, b) for a, b in zip(so_far, before))
        so_far = compose(read_state(held.at[m]), so_far)
    write_state(before_ref, before)
    write_state(total_ref, so_far)
    made_ref[...] = low(so_far[2])


def along(which, places, state, *others):
    return pl.pallas_call(
        functools.partial(along_kernel, which),
        in_specs=[scalars()] + [whole()] * 4,
        out_specs=[whole()] * 3,
        out_shape=[
            jax.ShapeDtypeStruct(state.shape, BF16),
            pltpu.VMEM(state.shape, BF16),
            pltpu.VMEM((state.shape[1] // 2,) * 2, BF16),
        ],
        scratch_shapes=[pltpu.VMEM((4,) + state.shape, BF16)],
        compiler_params=params(4),
        cost_estimate=cost(16 << 20, 1 << 18),
        name="along",
    )(places, *map(near_core, (state,) + others))


def cyclic(block, axis, distance):
    count = lax.axis_size(axis)
    return lax.ppermute(block, axis, [(i, (i + distance) % count) for i in range(count)])


def shifted(block, axis, distance):
    devices = range(lax.axis_size(axis))
    return lax.ppermute(block, axis, [(i, i + distance) for i in devices if i + distance in devices])


def swapped(block):
    return lax.ppermute(block, "c", [(0, 1), (1, 0)])


def exchanged(parts):
    got = [parts[0]]
    for slot in range(1, 8):
        step, side = STEPS[slot // 2], slot % 2
        route = [(y * 2 + c, (y + step) % 4 * 2 + (c ^ side)) for y in range(4) for c in range(2)]
        got.append(lax.ppermute(parts[slot], TP, route))
    return got


def finish_kernel(
    block_ref, coef_p_hbm, coef_q_hbm, dg_hbm, gain_ref, reach_any, far_any, before_hbm, *rest
):
    outs, scratch = rest[:8], rest[8:]
    coef_p_ref, coef_q_ref, dg_ref, reach_ref, far_ref, before_ref, sems = scratch
    loads = fetch(
        sems,
        (reach_any, reach_ref),
        (far_any, far_ref),
        (before_hbm, before_ref),
        (coef_p_hbm, coef_p_ref),
        (coef_q_hbm, coef_q_ref),
        (dg_hbm, dg_ref),
    )
    for one in loads[:3]:
        one.wait()
    total, lost, made = read_state(reach_ref)
    state = total * far_ref[...].astype(F32) - dot(low(lost), far_ref[...]) + made
    total, lost, made = read_state(before_ref)
    state = low(total * state - dot(low(lost), low(state)) + made)
    for one in loads[3:]:
        one.wait()
    step = outs[0].shape[0]
    for slot in range(8):
        here = pl.ds(pl.multiple_of(block_ref[GOES_TO[slot]] * step, step), step)
        result = coef_q_ref[here, :] + dot(coef_p_ref[here, :], state)
        mean = jnp.sum(result * result, axis=-1, keepdims=True) * (1.0 / result.shape[1])
        result = result * lax.rsqrt(mean + TINY_NORM) * gain_ref[...]
        outs[slot][...] = low(result * jax.nn.silu(dg_ref[here, :].astype(F32)))


def finish(blocks, coef_p, coef_q, dg, gain, reach, far, before):
    coef_p, coef_q, dg = map(home, (coef_p, coef_q, dg))
    rows, size = dg.shape
    args = (coef_p, coef_q, dg, gain, reach, far, before)
    copied = (coef_p, coef_q, dg, reach, far, before)
    return pl.pallas_call(
        finish_kernel,
        in_specs=[scalars(), hbm(), hbm(), hbm(), whole(), anywhere(), anywhere(), anywhere()],
        out_specs=[whole()] * 8,
        out_shape=[pltpu.VMEM((rows // 8, size), BF16)] * 8,
        scratch_shapes=[pltpu.VMEM(a.shape, a.dtype) for a in copied]
        + [pltpu.SemaphoreType.DMA((6,))],
        compiler_params=params(8),
        cost_estimate=cost(64 << 20, 2 << 20),
        name="finish",
    )(blocks, *args)


def conv_kernel(block_ref, gu_hbm, before_any, taps_ref, cg_hbm, *rest):
    outs = rest[:8]
    gu_ref, before_ref, padded, out_ref, cg_ref, sems = rest[8:]
    rows, size = gu_ref.shape
    head = before_ref.shape[0]
    count = taps_ref.shape[0]
    loads = fetch(sems, (gu_hbm, gu_ref), (before_any, before_ref), (cg_hbm, cg_ref))
    for one in loads[:2]:
        one.wait()
    padded[0:head, :] = before_ref[...].astype(F32)
    padded[head:, :] = gu_ref[...].astype(F32)
    taps = taps_ref[...].astype(F32)
    step = 64
    skip = head - (count - 1)

    def block(n, carry):
        base = pl.multiple_of(n * step, step)
        total = jnp.zeros((step, size), F32)
        for j in range(count):
            total = total + padded[pl.ds(base + skip + j, step), :] * taps[j : j + 1, :]
        out_ref[pl.ds(base, step), :] = low(total)
        return carry

    lax.fori_loop(0, rows // step, block, 0)
    loads[2].wait()
    part = rows // 8
    for slot in range(8):
        here = pl.ds(pl.multiple_of(block_ref[GOES_TO[slot]] * part, part), part)
        outs[slot][:, 0:size] = out_ref[here, :]
        outs[slot][:, size:] = cg_ref[here, :]


def conv(blocks, gu, before, taps, cg):
    rows, size = gu.shape
    return pl.pallas_call(
        conv_kernel,
        in_specs=[scalars(), hbm(), anywhere(), whole(), hbm()],
        out_specs=[whole()] * 8,
        out_shape=[pltpu.VMEM((rows // 8, 2 * size), BF16)] * 8,
        scratch_shapes=[
            pltpu.VMEM(gu.shape, BF16),
            pltpu.VMEM(before.shape, BF16),
            pltpu.VMEM((rows + before.shape[0], size), F32),
            pltpu.VMEM((rows, size), BF16),
            pltpu.VMEM((rows, size), BF16),
            pltpu.SemaphoreType.DMA((3,)),
        ],
        compiler_params=params(8),
        cost_estimate=cost(256 << 20, 1 << 20),
        name="conv",
    )(blocks, home(gu), before, taps, home(cg))


def add_slots(out_ref, slots, left, weights, start):
    size = weights.shape[1] - weights.shape[1] % 128

    def step(n, carry):
        here = pl.ds(pl.multiple_of(n * 512, 512), 512)
        acc = jnp.zeros((out_ref.shape[0], 512), F32) if start is None else start[:, here]
        for slot in slots:
            acc = acc + dot(left(slot), weights[slot, 0:size, here])
        out_ref[:, here] = acc.astype(out_ref.dtype)
        return carry

    lax.fori_loop(0, out_ref.shape[1] // 512, step, 0)


def cut_kernel(count, right_any, left_any, top_hbm, rest_hbm, top, rest, sems):
    inward = fetch(
        sems,
        (right_any.at[pl.ds(0, count), :], top),
        (left_any.at[pl.ds(count, rest.shape[0]), :], rest),
    )
    outward = []
    for n, pair in enumerate(((top, top_hbm), (rest, rest_hbm))):
        inward[n].wait()
        outward += fetch(sems.at[pl.ds(2 + n, 1)], pair)
    for one in outward:
        one.wait()


def cut(right, left, count):
    rows, width = right.shape
    shapes = [(count, width), (rows - count, width)]
    return pl.pallas_call(
        functools.partial(cut_kernel, count),
        in_specs=[anywhere()] * 2,
        out_specs=[hbm()] * 2,
        out_shape=[pltpu.HBM(shape, BF16) for shape in shapes],
        scratch_shapes=[pltpu.VMEM(shape, BF16) for shape in shapes]
        + [pltpu.SemaphoreType.DMA((4,))],
        compiler_params=params(4),
        cost_estimate=cost(1 << 20, 4 << 20),
        name="cut",
    )(right, left)


def conv_out_kernel(*refs):
    got, sources, delta_sources = refs[:8], refs[8:16], refs[16:24]
    out_ref, delta_weights = refs[24:26]
    got_ref, weights, mixed, sems = refs[26:]
    groups, rows, size = mixed.shape
    got_loads = fetch(
        sems.at[pl.ds(8, 8)], *((ref, got_ref.at[slot]) for slot, ref in enumerate(got))
    )
    loads = fetch(
        sems,
        *(
            (ref.at[pl.ds(0 if ref.shape[0] == size + 16 else size, size + 16), :], weights.at[slot])
            for slot, ref in enumerate(sources)
        ),
    )
    more = fetch(
        sems.at[pl.ds(16, 8)],
        *(
            (ref.at[pl.ds(0, size), :], delta_weights.at[slot])
            for slot, ref in enumerate(delta_sources)
        ),
    )
    for one in got_loads:
        one.wait()
    total = jnp.zeros((rows, size), F32)
    total_square = jnp.zeros((rows, size), F32)
    for g in range(groups):
        part = got_ref[g, :, 0:size].astype(F32)
        total = total + part
        total_square = total_square + part * part
    scale = 1.0 / (groups * size)
    center = jnp.sum(total, axis=1, keepdims=True) * scale
    second = jnp.sum(total_square, axis=1, keepdims=True) * scale
    factor = lax.rsqrt(jnp.maximum(second - center * center, 0.0) + TINY_VAR)
    for half in range(2):
        slots = range(half * 4, half * 4 + 4)
        for slot in slots:
            loads[slot].wait()
            extra = weights[slot, size : size + 16, :].astype(F32)
            gain = extra[0:1, 0:size] + extra[1:2, 0:size] + extra[2:3, 0:size]
            shift = extra[3:4, 0:size] + extra[4:5, 0:size] + extra[5:6, 0:size]
            normed = (got_ref[slot, :, 0:size].astype(F32) - center) * factor * gain + shift
            gate = got_ref[slot, :, size:].astype(F32)
            mixed[slot] = low(jax.nn.silu(normed) * jax.nn.silu(gate))
        add_slots(
            out_ref, slots, lambda slot: mixed[slot], weights, out_ref if half else None
        )
    for one in more:
        one.wait()


def conv_out(got, sources, delta_sources):
    groups = len(got)
    rows, both = got[0].shape
    size, width = both // 2, sources[0].shape[1]
    return pl.pallas_call(
        conv_out_kernel,
        in_specs=[anywhere()] * 24,
        out_specs=[whole()] * 2,
        out_shape=[pltpu.VMEM((rows, width), F32), pltpu.VMEM((groups, size, width), BF16)],
        scratch_shapes=[
            pltpu.VMEM((groups, rows, both), BF16),
            pltpu.VMEM((groups, size + 16, width), BF16),
            pltpu.VMEM((groups, rows, size), BF16),
            pltpu.SemaphoreType.DMA((24,)),
        ],
        compiler_params=params(12),
        cost_estimate=cost(2 * rows * 1024 * width, 6 << 20),
        name="conv_out",
    )(*got, *sources, *delta_sources)


def delta_out_kernel(conv_ref, weights, *refs):
    got, out_ref, got_ref, sems = refs[:8], refs[8], refs[9], refs[10]
    for one in fetch(sems, *((ref, got_ref.at[slot]) for slot, ref in enumerate(got))):
        one.wait()
    add_slots(out_ref, range(8), lambda slot: got_ref[slot], weights, conv_ref)


def delta_out(got, conv_part, weights):
    groups = len(got)
    rows, size = got[0].shape
    width = conv_part.shape[1]
    return pl.pallas_call(
        delta_out_kernel,
        in_specs=[whole()] * 2 + [anywhere()] * 8,
        out_specs=whole(),
        out_shape=jax.ShapeDtypeStruct((rows, width), BF16),
        scratch_shapes=[
            pltpu.VMEM((groups, rows, size), BF16),
            pltpu.SemaphoreType.DMA((8,)),
        ],
        compiler_params=params(12),
        cost_estimate=cost(2 * rows * 1024 * width, 6 << 20),
        name="delta_out",
    )(near_core(conv_part), near_core(weights), *got)


def local(
    tokens,
    w_query,
    w_key,
    w_value,
    w_delta_gate,
    w_glu_value,
    w_glu_gate,
    w_conv_gate,
    w_beta,
    w_decay,
    decay_log,
    head_gain,
    conv_taps,
    ln_gain,
    ln_shift,
    out_delta,
    out_conv,
):
    rows = tokens.shape[0]
    half = rows // 2
    size = w_query.shape[1]
    y, core = lax.axis_index("y"), lax.axis_index("c")
    x, z = lax.axis_index("x"), lax.axis_index("z")
    count_y = lax.axis_size("y")
    head = y * 2 + core
    chips = [y, (y - 1) % count_y, (y + 1) % count_y, (y + 2) % count_y]
    slots = [chip * 2 + side for chip in chips for side in (core, 1 - core)]
    blocks = jnp.stack(slots + [x, z % 4])
    blocks = blocks.astype(jnp.int32)

    beta_decay = jnp.concatenate(
        [
            lax.dynamic_slice_in_dim(w_beta, head, 1, 1),
            lax.dynamic_slice_in_dim(w_decay, head, 1, 1),
            jnp.zeros((w_beta.shape[0], 126), BF16),
        ],
        axis=1,
    )
    weights = (
        w_glu_value,
        w_glu_gate,
        w_delta_gate,
        w_conv_gate,
        w_query,
        w_key,
        w_value,
        beta_decay,
    )
    rate = jnp.exp(lax.dynamic_slice_in_dim(decay_log, head, 1, 0))

    def three(vector):
        high = lax.reduce_precision(vector, 8, 7)
        rest = vector - high
        middle = lax.reduce_precision(rest, 8, 7)
        return [high, middle, rest - middle]

    extra = jnp.stack(three(ln_gain) + three(ln_shift)).astype(BF16)
    extra = jnp.pad(extra, ((0, 10), (0, out_conv.shape[1] - extra.shape[1])))
    last = jnp.concatenate([out_delta, out_conv, extra], axis=0)

    own = tokens
    r1, l1 = cyclic(own, "y", 1), cyclic(own, "y", -1)
    sw = swapped(own)
    r1, l1, beta_decay, last, blocks, rate = lax.optimization_barrier(
        (r1, l1, beta_decay, last, blocks, rate)
    )
    weights = weights[:7] + (beta_decay,)
    r1_top, l1_rest = cut(r1, l1, half)
    fa, fb = cyclic(r1_top, "y", 1), cyclic(l1_rest, "y", -1)
    sr1, sl1 = swapped(r1), swapped(l1)
    sfa, sfb = swapped(fa), swapped(fb)
    pieces = [own, sw, r1, sr1, l1, sl1, fa, sfa, fb, sfb]
    wr, wl = cyclic(last, "y", 1), cyclic(last, "y", -1)
    q, k, v, bl, tail, dg, gu, cg = project(pieces, weights, blocks, rate, 2048, size)

    coef_p, coef_q, state = delta(q, k, v, bl)


    before, total, _ = along(8, blocks, state, *(cyclic(state, "x", j) for j in (2, 3, 1)))
    route = lambda j: [(h + i, h + (i + j) % 4) for h in (0, 4) for i in range(4)]
    around = []
    for j in (2, 3, 1):
        around.append(lax.ppermute(total, "z", route(j)))
    before_z, _, made_z = along(9, blocks, total, *around)
    far = shifted(made_z, "z", 4)

    ws = swapped(last)
    wr_top, wl_rest = cut(wr, wl, size)
    wfa, wfb = cyclic(wr_top, "y", 1), cyclic(wl_rest, "y", -1)
    wsr, wsl = swapped(wr), swapped(wl)
    wsfa, wsfb = swapped(wfa), swapped(wfb)
    near = [last, ws, wr, wsr, wl, wsl]
    delta_weights = near + [wfa, wsfa]
    conv_weights = near + [wfb, wsfb]

    halo = lax.ppermute(tail, SP, [(i, i + 1) for i in range(31)])
    filtered = conv(blocks, gu, halo, conv_taps, cg)
    got = exchanged(filtered)
    conv_part, kept = conv_out(got, conv_weights, delta_weights)

    mixed = finish(blocks, coef_p, coef_q, dg, head_gain[None, :], before_z, far, before)
    return delta_out(exchanged(mixed), conv_part, kept)


def solution(mesh):
    finer = Mesh(mesh.devices.reshape(8, 4, 4, 2), ("z", "x", "y", "c"))
    placed = (
        P(SP, TP),
        P(None, TP),
        P(None, TP),
        P(None, TP),
        P(None, TP),
        P(None, TP),
        P(None, TP),
        P(None, TP),
        P(),
        P(),
        P(),
        P(),
        P(None, TP),
        P(TP),
        P(TP),
        P(TP, None),
        P(TP, None),
    )
    return jax.shard_map(
        local, mesh=finer, in_specs=placed, out_specs=P(SP + TP, None), check_vma=False
    )
```

```python
import functools

import jax
import jax.numpy as jnp
from jax import lax
from jax.experimental import pallas as pl
from jax.experimental.pallas import tpu as pltpu
from jax.sharding import Mesh
from jax.sharding import PartitionSpec as P


SP = ("z", "x")
TP = ("y", "c")
TINY_NORM = 1e-06
TINY_VAR = 1e-05
CHUNK = 128
HALO = 32
STEPS = (0, 1, -1, 2)
GOES_TO = (0, 1, 4, 5, 2, 3, 6, 7)
F32 = jnp.float32
BF16 = jnp.bfloat16


def whole():
    return pl.BlockSpec(memory_space=pltpu.VMEM)


def hbm():
    return pl.BlockSpec(memory_space=pltpu.HBM)


def anywhere():
    return pl.BlockSpec(memory_space=pl.ANY)


def home(array):
    return pltpu.with_memory_space_constraint(array, pltpu.HBM)


def near_core(array):
    return pltpu.with_memory_space_constraint(array, pltpu.VMEM)


def fetch(sems, *pairs):
    copies = [pltpu.make_async_copy(a, b, sems.at[n]) for n, (a, b) in enumerate(pairs)]
    for one in copies:
        one.start()
    return copies


def scalars():
    return pl.BlockSpec(memory_space=pltpu.SMEM)


def params(mib):
    return pltpu.CompilerParams(vmem_limit_bytes=min(mib * 1024 * 1024, 67043328))


def cost(flops, bytes_accessed):
    return pl.CostEstimate(flops=flops, bytes_accessed=bytes_accessed, transcendentals=0)


def dot(a, b):
    return jnp.dot(a, b, preferred_element_type=F32)


def dot_nt(a, b):
    return lax.dot_general(a, b, (((1,), (1,)), ((), ())), preferred_element_type=F32)


def dot_tn(a, b):
    return lax.dot_general(a, b, (((0,), (0,)), ((), ())), preferred_element_type=F32)


def low(a):
    return a.astype(BF16)


def split_two(a):
    high = a.astype(BF16)
    return high, (a - high.astype(F32)).astype(BF16)


def split_three(a):
    high = a.astype(BF16)
    rest = a - high.astype(F32)
    middle = rest.astype(BF16)
    return high, middle, (rest - middle.astype(F32)).astype(BF16)


def dot_fine(a, b):
    a_high, a_low = split_two(a)
    b_high, b_low = split_two(b)
    return dot(a_high, b_high) + (dot(a_high, b_low) + dot(a_low, b_high))


def pack_kernel(*refs):
    sides, packed, sems = refs[:8], refs[8], refs[9]
    for one in fetch(
        sems,
        *((ref, packed.at[n // 2, :, pl.ds(n % 2 * 128, 128)]) for n, ref in enumerate(sides)),
    ):
        one.wait()


def pack(weights):
    depth, width = weights[0].shape
    return pl.pallas_call(
        pack_kernel,
        in_specs=[anywhere()] * 8,
        out_specs=whole(),
        out_shape=pltpu.VMEM((4, depth, 2 * width), BF16),
        scratch_shapes=[pltpu.SemaphoreType.DMA((8,))],
        compiler_params=params(4),
        cost_estimate=cost(1 << 20, 8 << 20),
        name="pack",
    )(*map(home, weights))


def project_kernel(width_all, head_size, block_ref, rate_ref, *refs):
    near, (fa, sfa, fb, sfb), weights = refs[:6], refs[6:10], refs[10]
    q_ref, k_ref, v_ref, bl_ref, tail_ref, dg_ref, gu_ref, cg_ref = refs[11:19]
    far, factors, sems = refs[19:]
    rows, piece_width = near[0].shape
    half = rows // 2
    moves = fetch(
        sems,
        *(
            (ref, far.at[side, pl.ds(n * half, half), :])
            for n, pair in enumerate(((fa, sfa), (fb, sfb)))
            for side, ref in enumerate(pair)
        ),
    )

    def unit_rows(raw):
        wide = low(raw).astype(F32)
        return wide * lax.rsqrt(jnp.sum(wide * wide, axis=-1, keepdims=True) + TINY_NORM)

    def product(n, here, slots):
        total = None
        for slot in slots:
            piece = near[slot][here, :] if slot < 6 else far[slot - 6, here, :]
            offset = pl.multiple_of(block_ref[slot] * piece_width, piece_width)
            term = dot(piece, weights[n, pl.ds(offset, piece_width), :])
            total = term if total is None else total + term
        return total

    def pair(n, here):
        both = product(n, here, range(8)) * factors[here, :]
        return both[:, :128], both[:, 128:]

    def each_half(body):
        def step(n, carry):
            body(pl.ds(pl.multiple_of(n * half, half), half))
            return carry

        lax.fori_loop(0, 2, step, 0)

    def gated(here):
        squares = jnp.zeros((half, piece_width), F32)
        for slot in range(8):
            piece = near[slot][here, :] if slot < 6 else far[slot - 6, here, :]
            wide = piece.astype(F32)
            squares = squares + wide * wide
        squares = jnp.sum(squares, axis=1, keepdims=True)
        factors[here, :] = lax.rsqrt(squares / width_all + TINY_NORM)
        gv, gg = pair(0, here)
        gu_ref[here, :] = low(low(gv).astype(F32) * jax.nn.sigmoid(low(gg).astype(F32)))

    def gates(here):
        dg, cg = pair(1, here)
        dg_ref[here, :] = low(dg)
        cg_ref[here, :] = low(cg)

    def queries(here):
        q, k = pair(2, here)
        q_ref[here, :] = low(unit_rows(q) * head_size ** (-0.5))
        k_ref[here, :] = low(unit_rows(k))

    def rest_of(here):
        v, bl = pair(3, here)
        v_ref[here, :] = low(v)
        lane = lax.broadcasted_iota(jnp.int32, bl.shape, 1)
        bl_ref[here, :] = jnp.where(
            lane == 0, jax.nn.sigmoid(bl), -rate_ref[0] * jax.nn.softplus(bl)
        )

    for one in moves:
        one.wait()
    for body in (gated, gates, queries, rest_of):
        each_half(body)
    tail_ref[...] = gu_ref[rows - HALO :, :]


def project(pieces, weights, blocks, rate, width_all, head_size):
    rows, piece_width = pieces[0].shape
    kinds = [BF16] * 3 + [F32] + [BF16] * 3
    return pl.pallas_call(
        functools.partial(project_kernel, width_all, head_size),
        in_specs=[scalars(), scalars()] + [whole()] * 11,
        out_specs=[whole()] * 8,
        out_shape=[pltpu.VMEM((rows, 128), kind) for kind in kinds[:4]]
        + [pltpu.VMEM((HALO, 128), BF16)]
        + [pltpu.VMEM((rows, 128), kind) for kind in kinds[4:]],
        scratch_shapes=[
            pltpu.VMEM((2, rows, piece_width), BF16),
            pltpu.VMEM((rows, 1), F32),
            pltpu.SemaphoreType.DMA((4,)),
        ],
        compiler_params=params(20),
        cost_estimate=cost(2 * rows * width_all * 1024, 12 << 20),
        name="project",
    )(blocks, rate, *map(near_core, pieces), near_core(weights))


def write_state(ref, state):
    total, lost, made = state
    size = lost.shape[0]
    ref[0:size, 0:size] = low(lost)
    ref[0:size, size:] = low(made)
    row = lax.broadcasted_iota(jnp.int32, (16, 2 * size), 0)
    high, middle, rest = split_three(jnp.broadcast_to(total, (16, 2 * size)))
    packed = jnp.where(
        row == 0,
        high.astype(F32),
        jnp.where(row == 1, middle.astype(F32), rest.astype(F32)),
    )
    ref[size : size + 16, :] = low(packed)


def read_state(ref):
    size = ref.shape[1] // 2
    packed = ref[size : size + 16, 0:128].astype(F32)
    total = packed[0:1, 0:1] + packed[1:2, 0:1] + packed[2:3, 0:1]
    return (total, ref[0:size, 0:size].astype(F32), ref[0:size, size:].astype(F32))


def compose(later, earlier):
    total2, lost2, made2 = later
    total1, lost1, made1 = earlier
    size = lost1.shape[0]
    both = dot(low(lost2), low(jnp.concatenate([lost1, made1], axis=1)))
    lost = total2 * lost1 + total1 * lost2 - both[:, :size]
    made = total2 * made1 - both[:, size:] + made2
    return (total1 * total2, lost, made)


def delta_kernel(
    q_ref, k_ref, v_ref, bl_ref, coef_p_ref, coef_q_ref, state_ref
):
    rows, size = q_ref.shape
    chunks = rows // CHUNK
    row = lax.broadcasted_iota(jnp.int32, (CHUNK, CHUNK), 0)
    column = lax.broadcasted_iota(jnp.int32, (CHUNK, CHUNK), 1)
    causal = row >= column
    strict = row > column
    ones = jnp.where(causal, 1.0, 0.0).astype(BF16)
    lowers, inverses, scores, grown, tails = [], [], [], [], []
    betas = []
    for n in range(chunks):
        here = slice(n * CHUNK, (n + 1) * CHUNK)
        both = bl_ref[here, :]
        beta = both[:, 0:1]
        high, middle, rest = split_three(both)
        sums = dot(ones, high) + (dot(ones, middle) + dot(ones, rest))
        log_sum = jnp.broadcast_to(sums[:, 1:2], (CHUNK, CHUNK))
        damping = jnp.where(causal, jnp.exp(jnp.minimum(log_sum - log_sum.T, 0.0)), 0.0)
        k = k_ref[here, :]
        lower = jnp.where(strict, dot_nt(k, k) * damping, 0.0) * beta
        scores.append(low(dot_nt(q_ref[here, :], k) * damping))
        lowers.append(lower)
        betas.append(beta)
        grown.append(log_sum)
        tails.append(log_sum[CHUNK - 1 : CHUNK, :])
        below = ((row & 1) == 1) & (column == row - 1)
        inverses.append(jnp.where(row == column, 1.0, 0.0) - jnp.where(below, lower, 0.0))
    level = 2
    while level < CHUNK:
        shift = level.bit_length() - 1
        part = row >> shift
        below = ((part & 1) == 1) & ((column >> shift) == part - 1)
        multiply = dot_fine if level >= 16 else (lambda a, b: dot(low(a), low(b)))
        moved = [
            multiply(inverse, jnp.where(below, lower, 0.0))
            for inverse, lower in zip(inverses, lowers)
        ]
        inverses = [
            inverse - multiply(middle, inverse) for inverse, middle in zip(inverses, moved)
        ]
        level *= 2
    queries, starts, losts, mades = [], [], [], []
    for n in range(chunks):
        here = slice(n * CHUNK, (n + 1) * CHUNK)
        k = k_ref[here, :].astype(F32)
        grow = jnp.exp(grown[n])
        right = jnp.concatenate(
            [v_ref[here, :].astype(F32) * betas[n], k * (betas[n] * grow)], axis=1
        )
        solved = low(dot(low(inverses[n]), low(right)))
        seen = dot(scores[n], solved)
        starts.append(seen[:, :size])
        queries.append(low(q_ref[here, :].astype(F32) * grow - seen[:, size:]))
        weighted = low(k * jnp.exp(tails[n] - grown[n]))
        written = dot_tn(weighted, solved)
        mades.append(written[:, :size])
        losts.append(low(written[:, size:]))
    carried = jnp.where(row == column, 1.0, 0.0)
    made = jnp.zeros((CHUNK, size), F32)
    log_total = jnp.zeros((1, CHUNK), F32)
    for n in range(chunks):
        here = slice(n * CHUNK, (n + 1) * CHUNK)
        rounded = low(jnp.concatenate([carried, made], axis=1))
        seen = dot(queries[n], rounded)
        coef_p_ref[here, :] = low(seen[:, :size])
        coef_q_ref[here, :] = seen[:, size:] + starts[n]
        moved = dot(losts[n], rounded)
        keep = jnp.exp(tails[n])
        carried = carried * keep - moved[:, :size]
        made = made * keep - moved[:, size:] + mades[n]
        log_total = log_total + tails[n]
    total = jnp.exp(log_total)[:, 0:1]
    lost = jnp.where(row == column, total, 0.0) - carried
    write_state(state_ref, (total, lost, made))


def delta(q, k, v, bl):
    rows, size = q.shape
    return pl.pallas_call(
        delta_kernel,
        in_specs=[whole()] * 4,
        out_specs=[whole()] * 3,
        out_shape=[
            pltpu.VMEM((rows, size), BF16),
            pltpu.VMEM((rows, size), F32),
            pltpu.VMEM((size + 16, 2 * size), BF16),
        ],
        compiler_params=params(16),
        cost_estimate=cost(2 * rows * size * size * 60, 3 << 20),
        name="delta",
    )(*map(near_core, (q, k, v, bl)))


def along_kernel(which, place_ref, p0, p1, p2, p3, before_ref, total_ref, made_ref, held):
    me = place_ref[which]
    for j, piece in ((0, p0), (2, p1), (3, p2), (1, p3)):
        held[(me - j + 4) & 3] = piece[...]
    size = p0.shape[1] // 2
    nothing = (jnp.ones((1, 1), F32), jnp.zeros((size, size), F32), jnp.zeros((size, size), F32))
    before = nothing
    so_far = read_state(held.at[0])
    for m in range(1, 4):
        before = tuple(jnp.where(me == m, a, b) for a, b in zip(so_far, before))
        so_far = compose(read_state(held.at[m]), so_far)
    write_state(before_ref, before)
    write_state(total_ref, so_far)
    made_ref[...] = low(so_far[2])


def along(which, places, state, *others):
    return pl.pallas_call(
        functools.partial(along_kernel, which),
        in_specs=[scalars()] + [whole()] * 4,
        out_specs=[whole()] * 3,
        out_shape=[
            jax.ShapeDtypeStruct(state.shape, BF16),
            pltpu.VMEM(state.shape, BF16),
            pltpu.VMEM((state.shape[1] // 2,) * 2, BF16),
        ],
        scratch_shapes=[pltpu.VMEM((4,) + state.shape, BF16)],
        compiler_params=params(4),
        cost_estimate=cost(16 << 20, 1 << 18),
        name="along",
    )(places, *map(near_core, (state,) + others))


def cyclic(block, axis, distance):
    count = lax.axis_size(axis)
    return lax.ppermute(block, axis, [(i, (i + distance) % count) for i in range(count)])


def shifted(block, axis, distance):
    devices = range(lax.axis_size(axis))
    return lax.ppermute(block, axis, [(i, i + distance) for i in devices if i + distance in devices])


def swapped(block):
    return lax.ppermute(block, "c", [(0, 1), (1, 0)])


def exchanged(parts):
    got = [parts[0]]
    for slot in range(1, 8):
        step, side = STEPS[slot // 2], slot % 2
        route = [(y * 2 + c, (y + step) % 4 * 2 + (c ^ side)) for y in range(4) for c in range(2)]
        got.append(lax.ppermute(parts[slot], TP, route))
    return got


def finish_kernel(
    block_ref, coef_p_ref, coef_q_ref, dg_ref, gain_ref, reach_ref, far_ref, before_ref, *outs
):
    total, lost, made = read_state(reach_ref)
    state = total * far_ref[...].astype(F32) - dot(low(lost), far_ref[...]) + made
    total, lost, made = read_state(before_ref)
    state = low(total * state - dot(low(lost), low(state)) + made)
    step = outs[0].shape[0]
    for slot in range(8):
        here = pl.ds(pl.multiple_of(block_ref[GOES_TO[slot]] * step, step), step)
        result = coef_q_ref[here, :] + dot(coef_p_ref[here, :], state)
        mean = jnp.sum(result * result, axis=-1, keepdims=True) * (1.0 / result.shape[1])
        result = result * lax.rsqrt(mean + TINY_NORM) * gain_ref[...]
        outs[slot][...] = low(result * jax.nn.silu(dg_ref[here, :].astype(F32)))


def finish(blocks, *args):
    rows, size = args[0].shape
    return pl.pallas_call(
        finish_kernel,
        in_specs=[scalars()] + [whole()] * 7,
        out_specs=[whole()] * 8,
        out_shape=[pltpu.VMEM((rows // 8, size), BF16)] * 8,
        compiler_params=params(6),
        cost_estimate=cost(64 << 20, 2 << 20),
        name="finish",
    )(blocks, *map(near_core, args))


def conv_kernel(block_ref, gu_ref, before_ref, taps_ref, cg_ref, *rest):
    outs, (padded, out_ref) = rest[:8], rest[8:]
    rows, size = gu_ref.shape
    head = before_ref.shape[0]
    count = taps_ref.shape[0]
    padded[0:head, :] = before_ref[...].astype(F32)
    padded[head:, :] = gu_ref[...].astype(F32)
    taps = taps_ref[...].astype(F32)
    step = 64
    skip = head - (count - 1)

    def block(n, carry):
        base = pl.multiple_of(n * step, step)
        total = jnp.zeros((step, size), F32)
        for j in range(count):
            total = total + padded[pl.ds(base + skip + j, step), :] * taps[j : j + 1, :]
        out_ref[pl.ds(base, step), :] = low(total)
        return carry

    lax.fori_loop(0, rows // step, block, 0)
    part = rows // 8
    for slot in range(8):
        here = pl.ds(pl.multiple_of(block_ref[GOES_TO[slot]] * part, part), part)
        outs[slot][:, 0:size] = out_ref[here, :]
        outs[slot][:, size:] = cg_ref[here, :]


def conv(blocks, gu, before, taps, cg):
    rows, size = gu.shape
    return pl.pallas_call(
        conv_kernel,
        in_specs=[scalars()] + [whole()] * 4,
        out_specs=[whole()] * 8,
        out_shape=[pltpu.VMEM((rows // 8, 2 * size), BF16)] * 8,
        scratch_shapes=[
            pltpu.VMEM((rows + before.shape[0], size), F32),
            pltpu.VMEM((rows, size), BF16),
        ],
        compiler_params=params(8),
        cost_estimate=cost(256 << 20, 1 << 20),
        name="conv",
    )(blocks, *map(near_core, (gu, before, taps, cg)))


def add_slots(out_ref, left, weights, tops, start):
    size = left[0].shape[1]

    def step(n, carry):
        here = pl.ds(pl.multiple_of(n * 512, 512), 512)
        acc = jnp.zeros((out_ref.shape[0], 512), F32) if start is None else start[:, here]
        for part, ref, top in zip(left, weights, tops):
            acc = acc + dot(part[...], ref[top : top + size, here])
        out_ref[:, here] = acc.astype(out_ref.dtype)
        return carry

    lax.fori_loop(0, out_ref.shape[1] // 512, step, 0)


def cut_kernel(count, right_any, left_any, top_hbm, rest_hbm, top, rest, sems):
    inward = fetch(
        sems,
        (right_any.at[pl.ds(0, count), :], top),
        (left_any.at[pl.ds(count, rest.shape[0]), :], rest),
    )
    outward = []
    for n, pair in enumerate(((top, top_hbm), (rest, rest_hbm))):
        inward[n].wait()
        outward += fetch(sems.at[pl.ds(2 + n, 1)], pair)
    for one in outward:
        one.wait()


def cut(right, left, count):
    rows, width = right.shape
    shapes = [(count, width), (rows - count, width)]
    return pl.pallas_call(
        functools.partial(cut_kernel, count),
        in_specs=[anywhere()] * 2,
        out_specs=[hbm()] * 2,
        out_shape=[pltpu.HBM(shape, BF16) for shape in shapes],
        scratch_shapes=[pltpu.VMEM(shape, BF16) for shape in shapes]
        + [pltpu.SemaphoreType.DMA((4,))],
        compiler_params=params(4),
        cost_estimate=cost(1 << 20, 4 << 20),
        name="cut",
    )(right, left)


def conv_out_kernel(*refs):
    got, weights, out_ref, mixed = refs[:8], refs[8:16], refs[16], refs[17]
    groups, rows, size = mixed.shape
    tops = [0 if ref.shape[0] == size + 16 else size for ref in weights]
    total = jnp.zeros((rows, size), F32)
    total_square = jnp.zeros((rows, size), F32)
    for ref in got:
        part = ref[:, 0:size].astype(F32)
        total = total + part
        total_square = total_square + part * part
    scale = 1.0 / (groups * size)
    center = jnp.sum(total, axis=1, keepdims=True) * scale
    second = jnp.sum(total_square, axis=1, keepdims=True) * scale
    factor = lax.rsqrt(jnp.maximum(second - center * center, 0.0) + TINY_VAR)
    for slot in range(groups):
        top = tops[slot] + size
        extra = weights[slot][top : top + 16, :].astype(F32)
        gain = extra[0:1, 0:size] + extra[1:2, 0:size] + extra[2:3, 0:size]
        shift = extra[3:4, 0:size] + extra[4:5, 0:size] + extra[5:6, 0:size]
        normed = (got[slot][:, 0:size].astype(F32) - center) * factor * gain + shift
        gate = got[slot][:, size:].astype(F32)
        mixed[slot] = low(jax.nn.silu(normed) * jax.nn.silu(gate))
    add_slots(out_ref, [mixed.at[slot] for slot in range(groups)], weights, tops, None)


def conv_out(got, weights):
    groups = len(got)
    rows, both = got[0].shape
    size, width = both // 2, weights[0].shape[1]
    return pl.pallas_call(
        conv_out_kernel,
        in_specs=[whole()] * 16,
        out_specs=whole(),
        out_shape=pltpu.VMEM((rows, width), F32),
        scratch_shapes=[pltpu.VMEM((groups, rows, size), BF16)],
        compiler_params=params(8),
        cost_estimate=cost(2 * rows * 1024 * width, 6 << 20),
        name="conv_out",
    )(*map(near_core, got), *map(near_core, weights))


def delta_out_kernel(conv_ref, *refs):
    add_slots(refs[16], refs[:8], refs[8:16], [0] * 8, conv_ref)


def delta_out(got, conv_part, weights):
    rows, width = conv_part.shape
    return pl.pallas_call(
        delta_out_kernel,
        in_specs=[whole()] * 17,
        out_specs=whole(),
        out_shape=jax.ShapeDtypeStruct((rows, width), BF16),
        compiler_params=params(8),
        cost_estimate=cost(2 * rows * 1024 * width, 6 << 20),
        name="delta_out",
    )(near_core(conv_part), *map(near_core, got), *map(near_core, weights))


def local(
    tokens,
    w_query,
    w_key,
    w_value,
    w_delta_gate,
    w_glu_value,
    w_glu_gate,
    w_conv_gate,
    w_beta,
    w_decay,
    decay_log,
    head_gain,
    conv_taps,
    ln_gain,
    ln_shift,
    out_delta,
    out_conv,
):
    rows = tokens.shape[0]
    half = rows // 2
    size = w_query.shape[1]
    y, core = lax.axis_index("y"), lax.axis_index("c")
    x, z = lax.axis_index("x"), lax.axis_index("z")
    count_y = lax.axis_size("y")
    head = y * 2 + core
    chips = [y, (y - 1) % count_y, (y + 1) % count_y, (y + 2) % count_y]
    slots = [chip * 2 + side for chip in chips for side in (core, 1 - core)]
    blocks = jnp.stack(slots + [x, z % 4])
    blocks = blocks.astype(jnp.int32)

    beta_decay = jnp.concatenate(
        [
            lax.dynamic_slice_in_dim(w_beta, head, 1, 1),
            lax.dynamic_slice_in_dim(w_decay, head, 1, 1),
            jnp.zeros((w_beta.shape[0], 126), BF16),
        ],
        axis=1,
    )
    weights = (
        w_glu_value,
        w_glu_gate,
        w_delta_gate,
        w_conv_gate,
        w_query,
        w_key,
        w_value,
        beta_decay,
    )
    rate = jnp.exp(lax.dynamic_slice_in_dim(decay_log, head, 1, 0))

    def three(vector):
        high = lax.reduce_precision(vector, 8, 7)
        rest = vector - high
        middle = lax.reduce_precision(rest, 8, 7)
        return [high, middle, rest - middle]

    extra = jnp.stack(three(ln_gain) + three(ln_shift)).astype(BF16)
    extra = jnp.pad(extra, ((0, 10), (0, out_conv.shape[1] - extra.shape[1])))
    last = jnp.concatenate([out_delta, out_conv, extra], axis=0)

    own = tokens
    r1, l1 = cyclic(own, "y", 1), cyclic(own, "y", -1)
    sw = swapped(own)
    blocks, rate, last, beta_decay = lax.optimization_barrier((blocks, rate, last, beta_decay))
    weights = pack(weights[:7] + (beta_decay,))
    r1_top, l1_rest = cut(r1, l1, half)
    fa, fb = cyclic(r1_top, "y", 1), cyclic(l1_rest, "y", -1)
    sr1, sl1 = swapped(r1), swapped(l1)
    sfa, sfb = swapped(fa), swapped(fb)
    pieces = [own, sw, r1, sr1, l1, sl1, fa, sfa, fb, sfb]
    wr, wl = cyclic(last, "y", 1), cyclic(last, "y", -1)
    q, k, v, bl, tail, dg, gu, cg = project(pieces, weights, blocks, rate, 2048, size)

    coef_p, coef_q, state = delta(q, k, v, bl)


    before, total, _ = along(8, blocks, state, *(cyclic(state, "x", j) for j in (2, 3, 1)))
    route = lambda j: [(h + i, h + (i + j) % 4) for h in (0, 4) for i in range(4)]
    around = []
    for j in (2, 3, 1):
        around.append(lax.ppermute(total, "z", route(j)))
    before_z, _, made_z = along(9, blocks, total, *around)
    far = shifted(made_z, "z", 4)

    ws = swapped(last)
    wr_top, wl_rest = cut(wr, wl, size)
    wfa, wfb = cyclic(wr_top, "y", 1), cyclic(wl_rest, "y", -1)
    wsr, wsl = swapped(wr), swapped(wl)
    wsfa, wsfb = swapped(wfa), swapped(wfb)
    near = [last, ws, wr, wsr, wl, wsl]
    delta_weights = near + [wfa, wsfa]
    conv_weights = near + [wfb, wsfb]

    halo = lax.ppermute(tail, SP, [(i, i + 1) for i in range(31)])
    filtered = conv(blocks, gu, halo, conv_taps, cg)
    got = exchanged(filtered)
    conv_part = conv_out(got, conv_weights)

    mixed = finish(blocks, coef_p, coef_q, dg, head_gain[None, :], before_z, far, before)
    return delta_out(exchanged(mixed), conv_part, delta_weights)


def solution(mesh):
    finer = Mesh(mesh.devices.reshape(8, 4, 4, 2), ("z", "x", "y", "c"))
    placed = (
        P(SP, TP),
        P(None, TP),
        P(None, TP),
        P(None, TP),
        P(None, TP),
        P(None, TP),
        P(None, TP),
        P(None, TP),
        P(),
        P(),
        P(),
        P(),
        P(None, TP),
        P(TP),
        P(TP),
        P(TP, None),
        P(TP, None),
    )
    return jax.shard_map(
        local, mesh=finer, in_specs=placed, out_specs=P(SP + TP, None), check_vma=False
    )
```

```python
import functools

import jax
import jax.numpy as jnp
from jax import lax
from jax.experimental import pallas as pl
from jax.experimental.pallas import tpu as pltpu
from jax.sharding import Mesh
from jax.sharding import PartitionSpec as P


SP = ("z", "x")
TP = ("y", "c")
TINY_NORM = 1e-06
TINY_VAR = 1e-05
CHUNK = 128
HALO = 32
STEPS = (0, 1, -1, 2)
GOES_TO = (0, 1, 4, 5, 2, 3, 6, 7)
F32 = jnp.float32
BF16 = jnp.bfloat16


def whole():
    return pl.BlockSpec(memory_space=pltpu.VMEM)


def hbm():
    return pl.BlockSpec(memory_space=pltpu.HBM)


def anywhere():
    return pl.BlockSpec(memory_space=pl.ANY)


def home(array):
    return pltpu.with_memory_space_constraint(array, pltpu.HBM)


def near_core(array):
    return pltpu.with_memory_space_constraint(array, pltpu.VMEM)


def fetch(sems, *pairs):
    copies = [pltpu.make_async_copy(a, b, sems.at[n]) for n, (a, b) in enumerate(pairs)]
    for one in copies:
        one.start()
    return copies


def scalars():
    return pl.BlockSpec(memory_space=pltpu.SMEM)


def params(mib):
    return pltpu.CompilerParams(vmem_limit_bytes=min(mib * 1024 * 1024, 67043328))


def cost(flops, bytes_accessed):
    return pl.CostEstimate(flops=flops, bytes_accessed=bytes_accessed, transcendentals=0)


def dot(a, b):
    return jnp.dot(a, b, preferred_element_type=F32)


def dot_nt(a, b):
    return lax.dot_general(a, b, (((1,), (1,)), ((), ())), preferred_element_type=F32)


def dot_tn(a, b):
    return lax.dot_general(a, b, (((0,), (0,)), ((), ())), preferred_element_type=F32)


def low(a):
    return a.astype(BF16)


def split_two(a):
    high = a.astype(BF16)
    return high, (a - high.astype(F32)).astype(BF16)


def split_three(a):
    high = a.astype(BF16)
    rest = a - high.astype(F32)
    middle = rest.astype(BF16)
    return high, middle, (rest - middle.astype(F32)).astype(BF16)


def dot_fine(a, b):
    a_high, a_low = split_two(a)
    b_high, b_low = split_two(b)
    return dot(a_high, b_high) + (dot(a_high, b_low) + dot(a_low, b_high))


def pack_kernel(*refs):
    sides, packed, sems = refs[:8], refs[8], refs[9]
    for one in fetch(
        sems,
        *((ref, packed.at[n // 2, :, pl.ds(n % 2 * 128, 128)]) for n, ref in enumerate(sides)),
    ):
        one.wait()


def pack(weights):
    depth, width = weights[0].shape
    return pl.pallas_call(
        pack_kernel,
        in_specs=[anywhere()] * 8,
        out_specs=whole(),
        out_shape=pltpu.VMEM((4, depth, 2 * width), BF16),
        scratch_shapes=[pltpu.SemaphoreType.DMA((8,))],
        compiler_params=params(4),
        cost_estimate=cost(1 << 20, 8 << 20),
        name="pack",
    )(*map(home, weights))


def project_kernel(width_all, head_size, block_ref, rate_ref, *refs):
    near, (fa, sfa, fb, sfb), weights = refs[:6], refs[6:10], refs[10]
    q_ref, k_ref, v_ref, bl_ref, tail_ref, dg_ref, gu_ref, cg_ref = refs[11:19]
    far, factors, sems = refs[19:]
    rows, piece_width = near[0].shape
    half = rows // 2
    moves = fetch(
        sems,
        *(
            (ref, far.at[side, pl.ds(n * half, half), :])
            for n, pair in enumerate(((fa, sfa), (fb, sfb)))
            for side, ref in enumerate(pair)
        ),
    )

    def unit_rows(raw):
        wide = low(raw).astype(F32)
        return wide * lax.rsqrt(jnp.sum(wide * wide, axis=-1, keepdims=True) + TINY_NORM)

    def product(n, here, slots):
        total = None
        for slot in slots:
            piece = near[slot][here, :] if slot < 6 else far[slot - 6, here, :]
            offset = pl.multiple_of(block_ref[slot] * piece_width, piece_width)
            term = dot(piece, weights[n, pl.ds(offset, piece_width), :])
            total = term if total is None else total + term
        return total

    def pair(n, here):
        both = product(n, here, range(8)) * factors[here, :]
        return both[:, :128], both[:, 128:]

    def each_half(body):
        def step(n, carry):
            body(pl.ds(pl.multiple_of(n * half, half), half))
            return carry

        lax.fori_loop(0, 2, step, 0)

    def gated(here):
        squares = jnp.zeros((half, piece_width), F32)
        for slot in range(8):
            piece = near[slot][here, :] if slot < 6 else far[slot - 6, here, :]
            wide = piece.astype(F32)
            squares = squares + wide * wide
        squares = jnp.sum(squares, axis=1, keepdims=True)
        factors[here, :] = lax.rsqrt(squares / width_all + TINY_NORM)
        gv, gg = pair(0, here)
        gu_ref[here, :] = low(low(gv).astype(F32) * jax.nn.sigmoid(low(gg).astype(F32)))

    def gates(here):
        dg, cg = pair(1, here)
        dg_ref[here, :] = low(dg)
        cg_ref[here, :] = low(cg)

    def queries(here):
        q, k = pair(2, here)
        q_ref[here, :] = low(unit_rows(q) * head_size ** (-0.5))
        k_ref[here, :] = low(unit_rows(k))

    def rest_of(here):
        v, bl = pair(3, here)
        v_ref[here, :] = low(v)
        lane = lax.broadcasted_iota(jnp.int32, bl.shape, 1)
        bl_ref[here, :] = jnp.where(
            lane == 0, jax.nn.sigmoid(bl), -rate_ref[0] * jax.nn.softplus(bl)
        )

    for one in moves:
        one.wait()

    def everything(here):
        for body in (gated, gates, queries, rest_of):
            body(here)

    each_half(everything)
    tail_ref[...] = gu_ref[rows - HALO :, :]


def project(pieces, weights, blocks, rate, width_all, head_size):
    rows, piece_width = pieces[0].shape
    kinds = [BF16] * 3 + [F32] + [BF16] * 3
    return pl.pallas_call(
        functools.partial(project_kernel, width_all, head_size),
        in_specs=[scalars(), scalars()] + [whole()] * 11,
        out_specs=[whole()] * 8,
        out_shape=[pltpu.VMEM((rows, 128), kind) for kind in kinds[:4]]
        + [pltpu.VMEM((HALO, 128), BF16)]
        + [pltpu.VMEM((rows, 128), kind) for kind in kinds[4:]],
        scratch_shapes=[
            pltpu.VMEM((2, rows, piece_width), BF16),
            pltpu.VMEM((rows, 1), F32),
            pltpu.SemaphoreType.DMA((4,)),
        ],
        compiler_params=params(20),
        cost_estimate=cost(2 * rows * width_all * 1024, 12 << 20),
        name="project",
    )(blocks, rate, *map(near_core, pieces), near_core(weights))


def write_state(ref, state):
    total, lost, made = state
    size = lost.shape[0]
    ref[0:size, 0:size] = low(lost)
    ref[0:size, size:] = low(made)
    row = lax.broadcasted_iota(jnp.int32, (16, 2 * size), 0)
    high, middle, rest = split_three(jnp.broadcast_to(total, (16, 2 * size)))
    packed = jnp.where(
        row == 0,
        high.astype(F32),
        jnp.where(row == 1, middle.astype(F32), rest.astype(F32)),
    )
    ref[size : size + 16, :] = low(packed)


def read_state(ref):
    size = ref.shape[1] // 2
    packed = ref[size : size + 16, 0:128].astype(F32)
    total = packed[0:1, 0:1] + packed[1:2, 0:1] + packed[2:3, 0:1]
    return (total, ref[0:size, 0:size].astype(F32), ref[0:size, size:].astype(F32))


def compose(later, earlier):
    total2, lost2, made2 = later
    total1, lost1, made1 = earlier
    size = lost1.shape[0]
    both = dot(low(lost2), low(jnp.concatenate([lost1, made1], axis=1)))
    lost = total2 * lost1 + total1 * lost2 - both[:, :size]
    made = total2 * made1 - both[:, size:] + made2
    return (total1 * total2, lost, made)


def delta_kernel(
    q_ref, k_ref, v_ref, bl_ref, coef_p_ref, coef_q_ref, state_ref
):
    rows, size = q_ref.shape
    chunks = rows // CHUNK
    row = lax.broadcasted_iota(jnp.int32, (CHUNK, CHUNK), 0)
    column = lax.broadcasted_iota(jnp.int32, (CHUNK, CHUNK), 1)
    causal = row >= column
    strict = row > column
    ones = jnp.where(causal, 1.0, 0.0).astype(BF16)
    lowers, inverses, scores, grown, tails = [], [], [], [], []
    betas = []
    for n in range(chunks):
        here = slice(n * CHUNK, (n + 1) * CHUNK)
        both = bl_ref[here, :]
        beta = both[:, 0:1]
        high, middle, rest = split_three(both)
        sums = dot(ones, high) + (dot(ones, middle) + dot(ones, rest))
        log_sum = jnp.broadcast_to(sums[:, 1:2], (CHUNK, CHUNK))
        damping = jnp.where(causal, jnp.exp(jnp.minimum(log_sum - log_sum.T, 0.0)), 0.0)
        k = k_ref[here, :]
        lower = jnp.where(strict, dot_nt(k, k) * damping, 0.0) * beta
        scores.append(low(dot_nt(q_ref[here, :], k) * damping))
        lowers.append(lower)
        betas.append(beta)
        grown.append(log_sum)
        tails.append(log_sum[CHUNK - 1 : CHUNK, :])
        below = ((row & 1) == 1) & (column == row - 1)
        inverses.append(jnp.where(row == column, 1.0, 0.0) - jnp.where(below, lower, 0.0))
    level = 2
    while level < CHUNK:
        shift = level.bit_length() - 1
        part = row >> shift
        below = ((part & 1) == 1) & ((column >> shift) == part - 1)
        multiply = dot_fine if level >= 16 else (lambda a, b: dot(low(a), low(b)))
        moved = [
            multiply(inverse, jnp.where(below, lower, 0.0))
            for inverse, lower in zip(inverses, lowers)
        ]
        inverses = [
            inverse - multiply(middle, inverse) for inverse, middle in zip(inverses, moved)
        ]
        level *= 2
    queries, starts, losts, mades = [], [], [], []
    for n in range(chunks):
        here = slice(n * CHUNK, (n + 1) * CHUNK)
        k = k_ref[here, :].astype(F32)
        grow = jnp.exp(grown[n])
        right = jnp.concatenate(
            [v_ref[here, :].astype(F32) * betas[n], k * (betas[n] * grow)], axis=1
        )
        solved = low(dot(low(inverses[n]), low(right)))
        seen = dot(scores[n], solved)
        starts.append(seen[:, :size])
        queries.append(low(q_ref[here, :].astype(F32) * grow - seen[:, size:]))
        weighted = low(k * jnp.exp(tails[n] - grown[n]))
        written = dot_tn(weighted, solved)
        mades.append(written[:, :size])
        losts.append(low(written[:, size:]))
    carried = jnp.where(row == column, 1.0, 0.0)
    made = jnp.zeros((CHUNK, size), F32)
    log_total = jnp.zeros((1, CHUNK), F32)
    for n in range(chunks):
        here = slice(n * CHUNK, (n + 1) * CHUNK)
        rounded = low(jnp.concatenate([carried, made], axis=1))
        seen = dot(queries[n], rounded)
        coef_p_ref[here, :] = low(seen[:, :size])
        coef_q_ref[here, :] = seen[:, size:] + starts[n]
        moved = dot(losts[n], rounded)
        keep = jnp.exp(tails[n])
        carried = carried * keep - moved[:, :size]
        made = made * keep - moved[:, size:] + mades[n]
        log_total = log_total + tails[n]
    total = jnp.exp(log_total)[:, 0:1]
    lost = jnp.where(row == column, total, 0.0) - carried
    write_state(state_ref, (total, lost, made))


def delta(q, k, v, bl):
    rows, size = q.shape
    return pl.pallas_call(
        delta_kernel,
        in_specs=[whole()] * 4,
        out_specs=[whole()] * 3,
        out_shape=[
            pltpu.VMEM((rows, size), BF16),
            pltpu.VMEM((rows, size), F32),
            pltpu.VMEM((size + 16, 2 * size), BF16),
        ],
        compiler_params=params(16),
        cost_estimate=cost(2 * rows * size * size * 60, 3 << 20),
        name="delta",
    )(*map(near_core, (q, k, v, bl)))


def along_kernel(which, place_ref, p0, p1, p2, p3, before_ref, total_ref, made_ref, held):
    me = place_ref[which]
    for j, piece in ((0, p0), (2, p1), (3, p2), (1, p3)):
        held[(me - j + 4) & 3] = piece[...]
    size = p0.shape[1] // 2
    nothing = (jnp.ones((1, 1), F32), jnp.zeros((size, size), F32), jnp.zeros((size, size), F32))
    before = nothing
    so_far = read_state(held.at[0])
    for m in range(1, 4):
        before = tuple(jnp.where(me == m, a, b) for a, b in zip(so_far, before))
        so_far = compose(read_state(held.at[m]), so_far)
    write_state(before_ref, before)
    write_state(total_ref, so_far)
    made_ref[...] = low(so_far[2])


def along(which, places, state, *others):
    return pl.pallas_call(
        functools.partial(along_kernel, which),
        in_specs=[scalars()] + [whole()] * 4,
        out_specs=[whole()] * 3,
        out_shape=[
            jax.ShapeDtypeStruct(state.shape, BF16),
            pltpu.VMEM(state.shape, BF16),
            pltpu.VMEM((state.shape[1] // 2,) * 2, BF16),
        ],
        scratch_shapes=[pltpu.VMEM((4,) + state.shape, BF16)],
        compiler_params=params(4),
        cost_estimate=cost(16 << 20, 1 << 18),
        name="along",
    )(places, *map(near_core, (state,) + others))


def cyclic(block, axis, distance):
    count = lax.axis_size(axis)
    return lax.ppermute(block, axis, [(i, (i + distance) % count) for i in range(count)])


def shifted(block, axis, distance):
    devices = range(lax.axis_size(axis))
    return lax.ppermute(block, axis, [(i, i + distance) for i in devices if i + distance in devices])


def swapped(block):
    return lax.ppermute(block, "c", [(0, 1), (1, 0)])


def exchanged(parts):
    got = [parts[0]]
    for slot in range(1, 8):
        step, side = STEPS[slot // 2], slot % 2
        route = [(y * 2 + c, (y + step) % 4 * 2 + (c ^ side)) for y in range(4) for c in range(2)]
        got.append(lax.ppermute(parts[slot], TP, route))
    return got


def finish_kernel(
    block_ref, coef_p_ref, coef_q_ref, dg_ref, gain_ref, reach_ref, far_ref, before_ref, *outs
):
    total, lost, made = read_state(reach_ref)
    state = total * far_ref[...].astype(F32) - dot(low(lost), far_ref[...]) + made
    total, lost, made = read_state(before_ref)
    state = low(total * state - dot(low(lost), low(state)) + made)
    step = outs[0].shape[0]
    for slot in range(8):
        here = pl.ds(pl.multiple_of(block_ref[GOES_TO[slot]] * step, step), step)
        result = coef_q_ref[here, :] + dot(coef_p_ref[here, :], state)
        mean = jnp.sum(result * result, axis=-1, keepdims=True) * (1.0 / result.shape[1])
        result = result * lax.rsqrt(mean + TINY_NORM) * gain_ref[...]
        outs[slot][...] = low(result * jax.nn.silu(dg_ref[here, :].astype(F32)))


def finish(blocks, *args):
    rows, size = args[0].shape
    return pl.pallas_call(
        finish_kernel,
        in_specs=[scalars()] + [whole()] * 7,
        out_specs=[whole()] * 8,
        out_shape=[pltpu.VMEM((rows // 8, size), BF16)] * 8,
        compiler_params=params(6),
        cost_estimate=cost(64 << 20, 2 << 20),
        name="finish",
    )(blocks, *map(near_core, args))


def conv_kernel(block_ref, gu_ref, before_ref, taps_ref, cg_ref, *rest):
    outs, (padded, out_ref) = rest[:8], rest[8:]
    rows, size = gu_ref.shape
    head = before_ref.shape[0]
    count = taps_ref.shape[0]
    padded[0:head, :] = before_ref[...].astype(F32)
    padded[head:, :] = gu_ref[...].astype(F32)
    taps = taps_ref[...].astype(F32)
    step = 64
    skip = head - (count - 1)

    def block(n, carry):
        base = pl.multiple_of(n * step, step)
        total = jnp.zeros((step, size), F32)
        for j in range(count):
            total = total + padded[pl.ds(base + skip + j, step), :] * taps[j : j + 1, :]
        out_ref[pl.ds(base, step), :] = low(total)
        return carry

    lax.fori_loop(0, rows // step, block, 0)
    part = rows // 8
    for slot in range(8):
        here = pl.ds(pl.multiple_of(block_ref[GOES_TO[slot]] * part, part), part)
        outs[slot][:, 0:size] = out_ref[here, :]
        outs[slot][:, size:] = cg_ref[here, :]


def conv(blocks, gu, before, taps, cg):
    rows, size = gu.shape
    return pl.pallas_call(
        conv_kernel,
        in_specs=[scalars()] + [whole()] * 4,
        out_specs=[whole()] * 8,
        out_shape=[pltpu.VMEM((rows // 8, 2 * size), BF16)] * 8,
        scratch_shapes=[
            pltpu.VMEM((rows + before.shape[0], size), F32),
            pltpu.VMEM((rows, size), BF16),
        ],
        compiler_params=params(8),
        cost_estimate=cost(256 << 20, 1 << 20),
        name="conv",
    )(blocks, *map(near_core, (gu, before, taps, cg)))


def add_slots(out_ref, left, weights, tops, start):
    size = left[0].shape[1]

    def step(n, carry):
        here = pl.ds(pl.multiple_of(n * 512, 512), 512)
        acc = jnp.zeros((out_ref.shape[0], 512), F32) if start is None else start[:, here]
        for part, ref, top in zip(left, weights, tops):
            acc = acc + dot(part[...], ref[top : top + size, here])
        out_ref[:, here] = acc.astype(out_ref.dtype)
        return carry

    lax.fori_loop(0, out_ref.shape[1] // 512, step, 0)


def cut_kernel(count, right_any, left_any, top_ref, rest_ref, sems):
    for one in fetch(
        sems,
        (right_any.at[pl.ds(0, count), :], top_ref),
        (left_any.at[pl.ds(count, rest_ref.shape[0]), :], rest_ref),
    ):
        one.wait()


def cut(right, left, count):
    rows, width = right.shape
    return pl.pallas_call(
        functools.partial(cut_kernel, count),
        in_specs=[anywhere()] * 2,
        out_specs=[whole()] * 2,
        out_shape=[pltpu.VMEM((count, width), BF16), pltpu.VMEM((rows - count, width), BF16)],
        scratch_shapes=[pltpu.SemaphoreType.DMA((2,))],
        compiler_params=params(4),
        cost_estimate=cost(1 << 20, 4 << 20),
        name="cut",
    )(right, left)


def conv_out_kernel(*refs):
    got, weights, out_ref, mixed = refs[:8], refs[8:16], refs[16], refs[17]
    groups, rows, size = mixed.shape
    tops = [0 if ref.shape[0] == size + 16 else size for ref in weights]
    total = jnp.zeros((rows, size), F32)
    total_square = jnp.zeros((rows, size), F32)
    for ref in got:
        part = ref[:, 0:size].astype(F32)
        total = total + part
        total_square = total_square + part * part
    scale = 1.0 / (groups * size)
    center = jnp.sum(total, axis=1, keepdims=True) * scale
    second = jnp.sum(total_square, axis=1, keepdims=True) * scale
    factor = lax.rsqrt(jnp.maximum(second - center * center, 0.0) + TINY_VAR)
    for slot in range(groups):
        top = tops[slot] + size
        extra = weights[slot][top : top + 16, :].astype(F32)
        gain = extra[0:1, 0:size] + extra[1:2, 0:size] + extra[2:3, 0:size]
        shift = extra[3:4, 0:size] + extra[4:5, 0:size] + extra[5:6, 0:size]
        normed = (got[slot][:, 0:size].astype(F32) - center) * factor * gain + shift
        gate = got[slot][:, size:].astype(F32)
        mixed[slot] = low(jax.nn.silu(normed) * jax.nn.silu(gate))
    add_slots(out_ref, [mixed.at[slot] for slot in range(groups)], weights, tops, None)


def conv_out(got, weights):
    groups = len(got)
    rows, both = got[0].shape
    size, width = both // 2, weights[0].shape[1]
    return pl.pallas_call(
        conv_out_kernel,
        in_specs=[whole()] * 16,
        out_specs=whole(),
        out_shape=pltpu.VMEM((rows, width), F32),
        scratch_shapes=[pltpu.VMEM((groups, rows, size), BF16)],
        compiler_params=params(8),
        cost_estimate=cost(2 * rows * 1024 * width, 6 << 20),
        name="conv_out",
    )(*map(near_core, got), *map(near_core, weights))


def delta_out_kernel(conv_ref, *refs):
    got, weights, out_hbm, staged, sems = refs[:8], refs[8:16], refs[16], refs[17], refs[18]
    size = got[0].shape[1]
    stores = []
    for n, base in enumerate(range(0, staged.shape[1], 512)):
        here = slice(base, base + 512)
        acc = conv_ref[:, here]
        for part, ref in zip(got, weights):
            acc = acc + dot(part[...], ref[0:size, here])
        staged[:, here] = low(acc)
        stores += fetch(sems.at[pl.ds(n, 1)], (staged.at[:, here], out_hbm.at[:, here]))
    for one in stores:
        one.wait()


def delta_out(got, conv_part, weights):
    rows, width = conv_part.shape
    return pl.pallas_call(
        delta_out_kernel,
        in_specs=[whole()] * 17,
        out_specs=hbm(),
        out_shape=jax.ShapeDtypeStruct((rows, width), BF16),
        scratch_shapes=[pltpu.VMEM((rows, width), BF16), pltpu.SemaphoreType.DMA((4,))],
        compiler_params=params(8),
        cost_estimate=cost(2 * rows * 1024 * width, 6 << 20),
        name="delta_out",
    )(near_core(conv_part), *map(near_core, got), *map(near_core, weights))


def local(
    tokens,
    w_query,
    w_key,
    w_value,
    w_delta_gate,
    w_glu_value,
    w_glu_gate,
    w_conv_gate,
    w_beta,
    w_decay,
    decay_log,
    head_gain,
    conv_taps,
    ln_gain,
    ln_shift,
    out_delta,
    out_conv,
):
    rows = tokens.shape[0]
    half = rows // 2
    size = w_query.shape[1]
    y, core = lax.axis_index("y"), lax.axis_index("c")
    x, z = lax.axis_index("x"), lax.axis_index("z")
    count_y = lax.axis_size("y")
    head = y * 2 + core
    chips = [y, (y - 1) % count_y, (y + 1) % count_y, (y + 2) % count_y]
    slots = [chip * 2 + side for chip in chips for side in (core, 1 - core)]
    blocks = jnp.stack(slots + [x, z % 4])
    blocks = blocks.astype(jnp.int32)

    beta_decay = jnp.concatenate(
        [
            lax.dynamic_slice_in_dim(w_beta, head, 1, 1),
            lax.dynamic_slice_in_dim(w_decay, head, 1, 1),
            jnp.zeros((w_beta.shape[0], 126), BF16),
        ],
        axis=1,
    )
    weights = (
        w_glu_value,
        w_glu_gate,
        w_delta_gate,
        w_conv_gate,
        w_query,
        w_key,
        w_value,
        beta_decay,
    )
    rate = jnp.exp(lax.dynamic_slice_in_dim(decay_log, head, 1, 0))

    def three(vector):
        high = lax.reduce_precision(vector, 8, 7)
        rest = vector - high
        middle = lax.reduce_precision(rest, 8, 7)
        return [high, middle, rest - middle]

    extra = jnp.stack(three(ln_gain) + three(ln_shift)).astype(BF16)
    extra = jnp.pad(extra, ((0, 10), (0, out_conv.shape[1] - extra.shape[1])))
    last = jnp.concatenate([out_delta, out_conv, extra], axis=0)

    own = tokens
    r1, l1 = cyclic(own, "y", 1), cyclic(own, "y", -1)
    sw = swapped(own)
    blocks, rate, last, beta_decay = lax.optimization_barrier((blocks, rate, last, beta_decay))
    weights = pack(weights[:7] + (beta_decay,))
    r1_top, l1_rest = cut(r1, l1, half)
    fa, fb = cyclic(r1_top, "y", 1), cyclic(l1_rest, "y", -1)
    sr1, sl1 = swapped(r1), swapped(l1)
    sfa, sfb = swapped(fa), swapped(fb)
    pieces = [own, sw, r1, sr1, l1, sl1, fa, sfa, fb, sfb]
    wr, wl = cyclic(last, "y", 1), cyclic(last, "y", -1)
    q, k, v, bl, tail, dg, gu, cg = project(pieces, weights, blocks, rate, 2048, size)

    coef_p, coef_q, state = delta(q, k, v, bl)


    before, total, _ = along(8, blocks, state, *(cyclic(state, "x", j) for j in (2, 3, 1)))
    route = lambda j: [(h + i, h + (i + j) % 4) for h in (0, 4) for i in range(4)]
    around = []
    for j in (2, 3, 1):
        around.append(lax.ppermute(total, "z", route(j)))
    before_z, _, made_z = along(9, blocks, total, *around)
    far = shifted(made_z, "z", 4)

    ws = swapped(last)
    wr_top, wl_rest = cut(wr, wl, size)
    wfa, wfb = cyclic(wr_top, "y", 1), cyclic(wl_rest, "y", -1)
    wsr, wsl = swapped(wr), swapped(wl)
    wsfa, wsfb = swapped(wfa), swapped(wfb)
    near = [last, ws, wr, wsr, wl, wsl]
    delta_weights = near + [wfa, wsfa]
    conv_weights = near + [wfb, wsfb]

    halo = lax.ppermute(tail, SP, [(i, i + 1) for i in range(31)])
    filtered = conv(blocks, gu, halo, conv_taps, cg)
    got = exchanged(filtered)
    conv_part = conv_out(got, conv_weights)

    mixed = finish(blocks, coef_p, coef_q, dg, head_gain[None, :], before_z, far, before)
    return delta_out(exchanged(mixed), conv_part, delta_weights)


def solution(mesh):
    finer = Mesh(mesh.devices.reshape(8, 4, 4, 2), ("z", "x", "y", "c"))
    placed = (
        P(SP, TP),
        P(None, TP),
        P(None, TP),
        P(None, TP),
        P(None, TP),
        P(None, TP),
        P(None, TP),
        P(None, TP),
        P(),
        P(),
        P(),
        P(),
        P(None, TP),
        P(TP),
        P(TP),
        P(TP, None),
        P(TP, None),
    )
    return jax.shard_map(
        local, mesh=finer, in_specs=placed, out_specs=P(SP + TP, None), check_vma=False
    )
```

```python
import functools

import jax
import jax.numpy as jnp
from jax import lax
from jax.experimental import pallas as pl
from jax.experimental.pallas import tpu as pltpu
from jax.sharding import Mesh
from jax.sharding import PartitionSpec as P


SP = ("z", "x")
TP = ("y", "c")
TINY_NORM = 1e-06
TINY_VAR = 1e-05
CHUNK = 128
HALO = 32
STEPS = (0, 1, -1, 2)
GOES_TO = (0, 1, 4, 5, 2, 3, 6, 7)
F32 = jnp.float32
BF16 = jnp.bfloat16


def whole():
    return pl.BlockSpec(memory_space=pltpu.VMEM)


def hbm():
    return pl.BlockSpec(memory_space=pltpu.HBM)


def anywhere():
    return pl.BlockSpec(memory_space=pl.ANY)


def home(array):
    return pltpu.with_memory_space_constraint(array, pltpu.HBM)


def near_core(array):
    return pltpu.with_memory_space_constraint(array, pltpu.VMEM)


def fetch(sems, *pairs):
    copies = [pltpu.make_async_copy(a, b, sems.at[n]) for n, (a, b) in enumerate(pairs)]
    for one in copies:
        one.start()
    return copies


def scalars():
    return pl.BlockSpec(memory_space=pltpu.SMEM)


def params(mib):
    return pltpu.CompilerParams(vmem_limit_bytes=min(mib * 1024 * 1024, 67043328))


def cost(flops, bytes_accessed):
    return pl.CostEstimate(flops=flops, bytes_accessed=bytes_accessed, transcendentals=0)


def dot(a, b):
    return jnp.dot(a, b, preferred_element_type=F32)


def dot_nt(a, b):
    return lax.dot_general(a, b, (((1,), (1,)), ((), ())), preferred_element_type=F32)


def dot_tn(a, b):
    return lax.dot_general(a, b, (((0,), (0,)), ((), ())), preferred_element_type=F32)


def low(a):
    return a.astype(BF16)


def split_two(a):
    high = a.astype(BF16)
    return high, (a - high.astype(F32)).astype(BF16)


def split_three(a):
    high = a.astype(BF16)
    rest = a - high.astype(F32)
    middle = rest.astype(BF16)
    return high, middle, (rest - middle.astype(F32)).astype(BF16)


def dot_fine(a, b):
    a_high, a_low = split_two(a)
    b_high, b_low = split_two(b)
    return dot(a_high, b_high) + (dot(a_high, b_low) + dot(a_low, b_high))


def pack_kernel(*refs):
    sides, packed, sems = refs[:8], refs[8], refs[9]
    for one in fetch(
        sems,
        *((ref, packed.at[n // 2, :, pl.ds(n % 2 * 128, 128)]) for n, ref in enumerate(sides)),
    ):
        one.wait()


def pack(weights):
    depth, width = weights[0].shape
    return pl.pallas_call(
        pack_kernel,
        in_specs=[anywhere()] * 8,
        out_specs=whole(),
        out_shape=pltpu.VMEM((4, depth, 2 * width), BF16),
        scratch_shapes=[pltpu.SemaphoreType.DMA((8,))],
        compiler_params=params(4),
        cost_estimate=cost(1 << 20, 8 << 20),
        name="pack",
    )(*map(home, weights))


def project_kernel(width_all, head_size, block_ref, rate_ref, *refs):
    near, (fa, sfa, fb, sfb), weights = refs[:6], refs[6:10], refs[10]
    q_ref, k_ref, v_ref, bl_ref, tail_ref, dg_ref, gu_ref, cg_ref = refs[11:19]
    far, factors, sems = refs[19:]
    rows, piece_width = near[0].shape
    half = rows // 2
    moves = fetch(
        sems,
        *(
            (ref, far.at[side, pl.ds(n * half, half), :])
            for n, pair in enumerate(((fa, sfa), (fb, sfb)))
            for side, ref in enumerate(pair)
        ),
    )

    def unit_rows(raw):
        wide = low(raw).astype(F32)
        return wide * lax.rsqrt(jnp.sum(wide * wide, axis=-1, keepdims=True) + TINY_NORM)

    def product(n, here, slots):
        total = None
        for slot in slots:
            piece = near[slot][here, :] if slot < 6 else far[slot - 6, here, :]
            offset = pl.multiple_of(block_ref[slot] * piece_width, piece_width)
            term = dot(piece, weights[n, pl.ds(offset, piece_width), :])
            total = term if total is None else total + term
        return total

    def pair(n, here):
        both = product(n, here, range(8)) * factors[here, :]
        return both[:, :128], both[:, 128:]

    def each_half(body):
        def step(n, carry):
            for which in range(2):

                @pl.when(n == which)
                def _():
                    for one in moves[2 * which : 2 * which + 2]:
                        one.wait()

            body(pl.ds(pl.multiple_of(n * half, half), half))
            return carry

        lax.fori_loop(0, 2, step, 0)

    def gated(here):
        squares = jnp.zeros((half, piece_width), F32)
        for slot in range(8):
            piece = near[slot][here, :] if slot < 6 else far[slot - 6, here, :]
            wide = piece.astype(F32)
            squares = squares + wide * wide
        squares = jnp.sum(squares, axis=1, keepdims=True)
        factors[here, :] = lax.rsqrt(squares / width_all + TINY_NORM)
        gv, gg = pair(0, here)
        gu_ref[here, :] = low(low(gv).astype(F32) * jax.nn.sigmoid(low(gg).astype(F32)))

    def gates(here):
        dg, cg = pair(1, here)
        dg_ref[here, :] = low(dg)
        cg_ref[here, :] = low(cg)

    def queries(here):
        q, k = pair(2, here)
        q_ref[here, :] = low(unit_rows(q) * head_size ** (-0.5))
        k_ref[here, :] = low(unit_rows(k))

    def rest_of(here):
        v, bl = pair(3, here)
        v_ref[here, :] = low(v)
        lane = lax.broadcasted_iota(jnp.int32, bl.shape, 1)
        bl_ref[here, :] = jnp.where(
            lane == 0, jax.nn.sigmoid(bl), -rate_ref[0] * jax.nn.softplus(bl)
        )

    def everything(here):
        for body in (gated, gates, queries, rest_of):
            body(here)

    each_half(everything)
    tail_ref[...] = gu_ref[rows - HALO :, :]


def project(pieces, weights, blocks, rate, width_all, head_size):
    rows, piece_width = pieces[0].shape
    kinds = [BF16] * 3 + [F32] + [BF16] * 3
    return pl.pallas_call(
        functools.partial(project_kernel, width_all, head_size),
        in_specs=[scalars(), scalars()] + [whole()] * 11,
        out_specs=[whole()] * 8,
        out_shape=[pltpu.VMEM((rows, 128), kind) for kind in kinds[:4]]
        + [pltpu.VMEM((HALO, 128), BF16)]
        + [pltpu.VMEM((rows, 128), kind) for kind in kinds[4:]],
        scratch_shapes=[
            pltpu.VMEM((2, rows, piece_width), BF16),
            pltpu.VMEM((rows, 1), F32),
            pltpu.SemaphoreType.DMA((4,)),
        ],
        compiler_params=params(20),
        cost_estimate=cost(2 * rows * width_all * 1024, 12 << 20),
        name="project",
    )(blocks, rate, *map(near_core, pieces), near_core(weights))


def write_state(ref, state):
    total, lost, made = state
    size = lost.shape[0]
    ref[0:size, 0:size] = low(lost)
    ref[0:size, size:] = low(made)
    row = lax.broadcasted_iota(jnp.int32, (16, 2 * size), 0)
    high, middle, rest = split_three(jnp.broadcast_to(total, (16, 2 * size)))
    packed = jnp.where(
        row == 0,
        high.astype(F32),
        jnp.where(row == 1, middle.astype(F32), rest.astype(F32)),
    )
    ref[size : size + 16, :] = low(packed)


def read_state(ref):
    size = ref.shape[1] // 2
    packed = ref[size : size + 16, 0:128].astype(F32)
    total = packed[0:1, 0:1] + packed[1:2, 0:1] + packed[2:3, 0:1]
    return (total, ref[0:size, 0:size].astype(F32), ref[0:size, size:].astype(F32))


def compose(later, earlier):
    total2, lost2, made2 = later
    total1, lost1, made1 = earlier
    size = lost1.shape[0]
    both = dot(low(lost2), low(jnp.concatenate([lost1, made1], axis=1)))
    lost = total2 * lost1 + total1 * lost2 - both[:, :size]
    made = total2 * made1 - both[:, size:] + made2
    return (total1 * total2, lost, made)


def delta_kernel(
    q_ref, k_ref, v_ref, bl_ref, coef_p_ref, coef_q_ref, state_ref
):
    rows, size = q_ref.shape
    chunks = rows // CHUNK
    row = lax.broadcasted_iota(jnp.int32, (CHUNK, CHUNK), 0)
    column = lax.broadcasted_iota(jnp.int32, (CHUNK, CHUNK), 1)
    causal = row >= column
    strict = row > column
    ones = jnp.where(causal, 1.0, 0.0).astype(BF16)
    lowers, inverses, scores, grown, tails = [], [], [], [], []
    betas = []
    for n in range(chunks):
        here = slice(n * CHUNK, (n + 1) * CHUNK)
        both = bl_ref[here, :]
        beta = both[:, 0:1]
        high, middle, rest = split_three(both)
        sums = dot(ones, high) + (dot(ones, middle) + dot(ones, rest))
        log_sum = jnp.broadcast_to(sums[:, 1:2], (CHUNK, CHUNK))
        damping = jnp.where(causal, jnp.exp(jnp.minimum(log_sum - log_sum.T, 0.0)), 0.0)
        k = k_ref[here, :]
        lower = jnp.where(strict, dot_nt(k, k) * damping, 0.0) * beta
        scores.append(low(dot_nt(q_ref[here, :], k) * damping))
        lowers.append(lower)
        betas.append(beta)
        grown.append(log_sum)
        tails.append(log_sum[CHUNK - 1 : CHUNK, :])
        below = ((row & 1) == 1) & (column == row - 1)
        inverses.append(jnp.where(row == column, 1.0, 0.0) - jnp.where(below, lower, 0.0))
    level = 2
    while level < CHUNK:
        shift = level.bit_length() - 1
        part = row >> shift
        below = ((part & 1) == 1) & ((column >> shift) == part - 1)
        multiply = dot_fine if level >= 32 else (lambda a, b: dot(low(a), low(b)))
        moved = [
            multiply(inverse, jnp.where(below, lower, 0.0))
            for inverse, lower in zip(inverses, lowers)
        ]
        inverses = [
            inverse - multiply(middle, inverse) for inverse, middle in zip(inverses, moved)
        ]
        level *= 2
    queries, starts, losts, mades = [], [], [], []
    for n in range(chunks):
        here = slice(n * CHUNK, (n + 1) * CHUNK)
        k = k_ref[here, :].astype(F32)
        grow = jnp.exp(grown[n])
        right = jnp.concatenate(
            [v_ref[here, :].astype(F32) * betas[n], k * (betas[n] * grow)], axis=1
        )
        solved = low(dot(low(inverses[n]), low(right)))
        seen = dot(scores[n], solved)
        starts.append(seen[:, :size])
        queries.append(low(q_ref[here, :].astype(F32) * grow - seen[:, size:]))
        weighted = low(k * jnp.exp(tails[n] - grown[n]))
        written = dot_tn(weighted, solved)
        mades.append(written[:, :size])
        losts.append(low(written[:, size:]))
    carried = jnp.where(row == column, 1.0, 0.0)
    made = jnp.zeros((CHUNK, size), F32)
    log_total = jnp.zeros((1, CHUNK), F32)
    for n in range(chunks):
        here = slice(n * CHUNK, (n + 1) * CHUNK)
        rounded = low(jnp.concatenate([carried, made], axis=1))
        seen = dot(queries[n], rounded)
        coef_p_ref[here, :] = low(seen[:, :size])
        coef_q_ref[here, :] = seen[:, size:] + starts[n]
        moved = dot(losts[n], rounded)
        keep = jnp.exp(tails[n])
        carried = carried * keep - moved[:, :size]
        made = made * keep - moved[:, size:] + mades[n]
        log_total = log_total + tails[n]
    total = jnp.exp(log_total)[:, 0:1]
    lost = jnp.where(row == column, total, 0.0) - carried
    write_state(state_ref, (total, lost, made))


def delta(q, k, v, bl):
    rows, size = q.shape
    return pl.pallas_call(
        delta_kernel,
        in_specs=[whole()] * 4,
        out_specs=[whole()] * 3,
        out_shape=[
            pltpu.VMEM((rows, size), BF16),
            pltpu.VMEM((rows, size), F32),
            pltpu.VMEM((size + 16, 2 * size), BF16),
        ],
        compiler_params=params(16),
        cost_estimate=cost(2 * rows * size * size * 60, 3 << 20),
        name="delta",
    )(*map(near_core, (q, k, v, bl)))


def along_kernel(which, place_ref, p0, p1, p2, p3, before_ref, out_ref, held):
    me = place_ref[which]
    for j, piece in ((0, p0), (2, p1), (3, p2), (1, p3)):
        held[(me - j + 4) & 3] = piece[...]
    size = p0.shape[1] // 2
    nothing = (jnp.ones((1, 1), F32), jnp.zeros((size, size), F32), jnp.zeros((size, size), F32))
    before = nothing
    so_far = read_state(held.at[0])
    for m in range(1, 4):
        before = tuple(jnp.where(me == m, a, b) for a, b in zip(so_far, before))
        so_far = compose(read_state(held.at[m]), so_far)
    write_state(before_ref, before)
    if out_ref.shape == p0.shape:
        write_state(out_ref, so_far)
    else:
        out_ref[...] = low(so_far[2])


def along(which, places, out_shape, state, *others):
    return pl.pallas_call(
        functools.partial(along_kernel, which),
        in_specs=[scalars()] + [whole()] * 4,
        out_specs=[whole()] * 2,
        out_shape=[pltpu.VMEM(state.shape, BF16), pltpu.VMEM(out_shape, BF16)],
        scratch_shapes=[pltpu.VMEM((4,) + state.shape, BF16)],
        compiler_params=params(4),
        cost_estimate=cost(16 << 20, 1 << 18),
        name="along",
    )(places, *map(near_core, (state,) + others))


def cyclic(block, axis, distance):
    count = lax.axis_size(axis)
    return lax.ppermute(block, axis, [(i, (i + distance) % count) for i in range(count)])


def shifted(block, axis, distance):
    devices = range(lax.axis_size(axis))
    return lax.ppermute(block, axis, [(i, i + distance) for i in devices if i + distance in devices])


def swapped(block):
    return lax.ppermute(block, "c", [(0, 1), (1, 0)])


def exchanged(parts):
    got = [parts[0]]
    for slot in range(1, 8):
        step, side = STEPS[slot // 2], slot % 2
        route = [(y * 2 + c, (y + step) % 4 * 2 + (c ^ side)) for y in range(4) for c in range(2)]
        got.append(lax.ppermute(parts[slot], TP, route))
    return got


def finish_kernel(
    block_ref, coef_p_ref, coef_q_ref, dg_ref, gain_ref, reach_ref, far_ref, before_ref, *outs
):
    total, lost, made = read_state(reach_ref)
    state = total * far_ref[...].astype(F32) - dot(low(lost), far_ref[...]) + made
    total, lost, made = read_state(before_ref)
    state = low(total * state - dot(low(lost), low(state)) + made)
    step = outs[0].shape[0]
    for slot in range(8):
        here = pl.ds(pl.multiple_of(block_ref[GOES_TO[slot]] * step, step), step)
        result = coef_q_ref[here, :] + dot(coef_p_ref[here, :], state)
        mean = jnp.sum(result * result, axis=-1, keepdims=True) * (1.0 / result.shape[1])
        result = result * lax.rsqrt(mean + TINY_NORM) * gain_ref[...]
        outs[slot][...] = low(result * jax.nn.silu(dg_ref[here, :].astype(F32)))


def finish(blocks, *args):
    rows, size = args[0].shape
    return pl.pallas_call(
        finish_kernel,
        in_specs=[scalars()] + [whole()] * 7,
        out_specs=[whole()] * 8,
        out_shape=[pltpu.VMEM((rows // 8, size), BF16)] * 8,
        compiler_params=params(6),
        cost_estimate=cost(64 << 20, 2 << 20),
        name="finish",
    )(blocks, *map(near_core, args))


def conv_kernel(block_ref, gu_ref, before_ref, taps_ref, cg_ref, *rest):
    outs, (padded, out_ref) = rest[:8], rest[8:]
    rows, size = gu_ref.shape
    head = before_ref.shape[0]
    count = taps_ref.shape[0]
    padded[0:head, :] = before_ref[...].astype(F32)
    padded[head:, :] = gu_ref[...].astype(F32)
    taps = taps_ref[...].astype(F32)
    step = 64
    skip = head - (count - 1)

    def block(n, carry):
        base = pl.multiple_of(n * step, step)
        total = jnp.zeros((step, size), F32)
        for j in range(count):
            total = total + padded[pl.ds(base + skip + j, step), :] * taps[j : j + 1, :]
        out_ref[pl.ds(base, step), :] = low(total)
        return carry

    lax.fori_loop(0, rows // step, block, 0)
    part = rows // 8
    for slot in range(8):
        here = pl.ds(pl.multiple_of(block_ref[GOES_TO[slot]] * part, part), part)
        outs[slot][:, 0:size] = out_ref[here, :]
        outs[slot][:, size:] = cg_ref[here, :]


def conv(blocks, gu, before, taps, cg):
    rows, size = gu.shape
    return pl.pallas_call(
        conv_kernel,
        in_specs=[scalars()] + [whole()] * 4,
        out_specs=[whole()] * 8,
        out_shape=[pltpu.VMEM((rows // 8, 2 * size), BF16)] * 8,
        scratch_shapes=[
            pltpu.VMEM((rows + before.shape[0], size), F32),
            pltpu.VMEM((rows, size), BF16),
        ],
        compiler_params=params(8),
        cost_estimate=cost(256 << 20, 1 << 20),
        name="conv",
    )(blocks, *map(near_core, (gu, before, taps, cg)))


def add_slots(out_ref, left, weights, tops, start):
    size = left[0].shape[1]

    def step(n, carry):
        here = pl.ds(pl.multiple_of(n * 512, 512), 512)
        acc = jnp.zeros((out_ref.shape[0], 512), F32) if start is None else start[:, here]
        for part, ref, top in zip(left, weights, tops):
            acc = acc + dot(part[...], ref[top : top + size, here])
        out_ref[:, here] = acc.astype(out_ref.dtype)
        return carry

    lax.fori_loop(0, out_ref.shape[1] // 512, step, 0)


def cut_kernel(count, right_any, left_any, top_ref, rest_ref, sems):
    for one in fetch(
        sems,
        (right_any.at[pl.ds(0, count), :], top_ref),
        (left_any.at[pl.ds(count, rest_ref.shape[0]), :], rest_ref),
    ):
        one.wait()


def cut(right, left, count):
    rows, width = right.shape
    return pl.pallas_call(
        functools.partial(cut_kernel, count),
        in_specs=[anywhere()] * 2,
        out_specs=[whole()] * 2,
        out_shape=[pltpu.VMEM((count, width), BF16), pltpu.VMEM((rows - count, width), BF16)],
        scratch_shapes=[pltpu.SemaphoreType.DMA((2,))],
        compiler_params=params(4),
        cost_estimate=cost(1 << 20, 4 << 20),
        name="cut",
    )(right, left)


def conv_out_kernel(*refs):
    got, weights, out_ref, mixed = refs[:8], refs[8:16], refs[16], refs[17]
    groups, rows, size = mixed.shape
    tops = [0 if ref.shape[0] == size + 16 else size for ref in weights]
    total = jnp.zeros((rows, size), F32)
    total_square = jnp.zeros((rows, size), F32)
    for ref in got:
        part = ref[:, 0:size].astype(F32)
        total = total + part
        total_square = total_square + part * part
    scale = 1.0 / (groups * size)
    center = jnp.sum(total, axis=1, keepdims=True) * scale
    second = jnp.sum(total_square, axis=1, keepdims=True) * scale
    factor = lax.rsqrt(jnp.maximum(second - center * center, 0.0) + TINY_VAR)
    for slot in range(groups):
        top = tops[slot] + size
        extra = weights[slot][top : top + 16, :].astype(F32)
        gain = extra[0:1, 0:size] + extra[1:2, 0:size] + extra[2:3, 0:size]
        shift = extra[3:4, 0:size] + extra[4:5, 0:size] + extra[5:6, 0:size]
        normed = (got[slot][:, 0:size].astype(F32) - center) * factor * gain + shift
        gate = got[slot][:, size:].astype(F32)
        mixed[slot] = low(jax.nn.silu(normed) * jax.nn.silu(gate))
    add_slots(out_ref, [mixed.at[slot] for slot in range(groups)], weights, tops, None)


def conv_out(got, weights):
    groups = len(got)
    rows, both = got[0].shape
    size, width = both // 2, weights[0].shape[1]
    return pl.pallas_call(
        conv_out_kernel,
        in_specs=[whole()] * 16,
        out_specs=whole(),
        out_shape=pltpu.VMEM((rows, width), F32),
        scratch_shapes=[pltpu.VMEM((groups, rows, size), BF16)],
        compiler_params=params(8),
        cost_estimate=cost(2 * rows * 1024 * width, 6 << 20),
        name="conv_out",
    )(*map(near_core, got), *map(near_core, weights))


def delta_out_kernel(conv_ref, *refs):
    got, weights, out_hbm, staged, sems = refs[:8], refs[8:16], refs[16], refs[17], refs[18]
    size = got[0].shape[1]
    stores = []
    for n, base in enumerate(range(0, staged.shape[1], 512)):
        here = slice(base, base + 512)
        acc = conv_ref[:, here]
        for part, ref in zip(got, weights):
            acc = acc + dot(part[...], ref[0:size, here])
        staged[:, here] = low(acc)
        stores += fetch(sems.at[pl.ds(n, 1)], (staged.at[:, here], out_hbm.at[:, here]))
    for one in stores:
        one.wait()


def delta_out(got, conv_part, weights):
    rows, width = conv_part.shape
    return pl.pallas_call(
        delta_out_kernel,
        in_specs=[whole()] * 17,
        out_specs=hbm(),
        out_shape=jax.ShapeDtypeStruct((rows, width), BF16),
        scratch_shapes=[pltpu.VMEM((rows, width), BF16), pltpu.SemaphoreType.DMA((4,))],
        compiler_params=params(8),
        cost_estimate=cost(2 * rows * 1024 * width, 6 << 20),
        name="delta_out",
    )(near_core(conv_part), *map(near_core, got), *map(near_core, weights))


def local(
    tokens,
    w_query,
    w_key,
    w_value,
    w_delta_gate,
    w_glu_value,
    w_glu_gate,
    w_conv_gate,
    w_beta,
    w_decay,
    decay_log,
    head_gain,
    conv_taps,
    ln_gain,
    ln_shift,
    out_delta,
    out_conv,
):
    rows = tokens.shape[0]
    half = rows // 2
    size = w_query.shape[1]
    y, core = lax.axis_index("y"), lax.axis_index("c")
    x, z = lax.axis_index("x"), lax.axis_index("z")
    count_y = lax.axis_size("y")
    head = y * 2 + core
    chips = [y, (y - 1) % count_y, (y + 1) % count_y, (y + 2) % count_y]
    slots = [chip * 2 + side for chip in chips for side in (core, 1 - core)]
    blocks = jnp.stack(slots + [x, z % 4])
    blocks = blocks.astype(jnp.int32)

    beta_decay = jnp.concatenate(
        [
            lax.dynamic_slice_in_dim(w_beta, head, 1, 1),
            lax.dynamic_slice_in_dim(w_decay, head, 1, 1),
            jnp.zeros((w_beta.shape[0], 126), BF16),
        ],
        axis=1,
    )
    weights = (
        w_glu_value,
        w_glu_gate,
        w_delta_gate,
        w_conv_gate,
        w_query,
        w_key,
        w_value,
        beta_decay,
    )
    rate = jnp.exp(lax.dynamic_slice_in_dim(decay_log, head, 1, 0))

    def three(vector):
        high = lax.reduce_precision(vector, 8, 7)
        rest = vector - high
        middle = lax.reduce_precision(rest, 8, 7)
        return [high, middle, rest - middle]

    extra = jnp.stack(three(ln_gain) + three(ln_shift)).astype(BF16)
    extra = jnp.pad(extra, ((0, 10), (0, out_conv.shape[1] - extra.shape[1])))
    last = jnp.concatenate([out_delta, out_conv, extra], axis=0)

    own = tokens
    r1, l1 = cyclic(own, "y", 1), cyclic(own, "y", -1)
    sw = swapped(own)
    blocks, rate, last, beta_decay = lax.optimization_barrier((blocks, rate, last, beta_decay))
    weights = pack(weights[:7] + (beta_decay,))
    r1_top, l1_rest = cut(r1, l1, half)
    fa, fb = cyclic(r1_top, "y", 1), cyclic(l1_rest, "y", -1)
    sr1, sl1 = swapped(r1), swapped(l1)
    sfa, sfb = swapped(fa), swapped(fb)
    pieces = [own, sw, r1, sr1, l1, sl1, fa, sfa, fb, sfb]
    wr, wl = cyclic(last, "y", 1), cyclic(last, "y", -1)
    q, k, v, bl, tail, dg, gu, cg = project(pieces, weights, blocks, rate, 2048, size)

    coef_p, coef_q, state = delta(q, k, v, bl)


    before, total = along(8, blocks, state.shape, state, *(cyclic(state, "x", j) for j in (2, 3, 1)))
    route = lambda j: [(h + i, h + (i + j) % 4) for h in (0, 4) for i in range(4)]
    around = []
    for j in (2, 3, 1):
        around.append(lax.ppermute(total, "z", route(j)))
    before_z, made_z = along(9, blocks, (size, size), total, *around)
    far = shifted(made_z, "z", 4)

    ws = swapped(last)
    wr_top, wl_rest = cut(wr, wl, size)
    wfa, wfb = cyclic(wr_top, "y", 1), cyclic(wl_rest, "y", -1)
    wsr, wsl = swapped(wr), swapped(wl)
    wsfa, wsfb = swapped(wfa), swapped(wfb)
    near = [last, ws, wr, wsr, wl, wsl]
    delta_weights = near + [wfa, wsfa]
    conv_weights = near + [wfb, wsfb]

    halo = lax.ppermute(tail, SP, [(i, i + 1) for i in range(31)])
    filtered = conv(blocks, gu, halo, conv_taps, cg)
    got = exchanged(filtered)
    conv_part = conv_out(got, conv_weights)

    mixed = finish(blocks, coef_p, coef_q, dg, head_gain[None, :], before_z, far, before)
    return delta_out(exchanged(mixed), conv_part, delta_weights)


def solution(mesh):
    finer = Mesh(mesh.devices.reshape(8, 4, 4, 2), ("z", "x", "y", "c"))
    placed = (
        P(SP, TP),
        P(None, TP),
        P(None, TP),
        P(None, TP),
        P(None, TP),
        P(None, TP),
        P(None, TP),
        P(None, TP),
        P(),
        P(),
        P(),
        P(),
        P(None, TP),
        P(TP),
        P(TP),
        P(TP, None),
        P(TP, None),
    )
    return jax.shard_map(
        local, mesh=finer, in_specs=placed, out_specs=P(SP + TP, None), check_vma=False
    )
```

```python
import functools

import jax
import jax.numpy as jnp
from jax import lax
from jax.experimental import pallas as pl
from jax.experimental.pallas import tpu as pltpu
from jax.sharding import Mesh
from jax.sharding import PartitionSpec as P


SP = ("z", "x")
TP = ("y", "c")
TINY_NORM = 1e-06
TINY_VAR = 1e-05
CHUNK = 128
HALO = 32
STEPS = (0, 1, -1, 2)
GOES_TO = (0, 1, 4, 5, 2, 3, 6, 7)
F32 = jnp.float32
BF16 = jnp.bfloat16


def whole():
    return pl.BlockSpec(memory_space=pltpu.VMEM)


def hbm():
    return pl.BlockSpec(memory_space=pltpu.HBM)


def anywhere():
    return pl.BlockSpec(memory_space=pl.ANY)


def home(array):
    return pltpu.with_memory_space_constraint(array, pltpu.HBM)


def near_core(array):
    return pltpu.with_memory_space_constraint(array, pltpu.VMEM)


def fetch(sems, *pairs):
    copies = [pltpu.make_async_copy(a, b, sems.at[n]) for n, (a, b) in enumerate(pairs)]
    for one in copies:
        one.start()
    return copies


def scalars():
    return pl.BlockSpec(memory_space=pltpu.SMEM)


def params(mib):
    return pltpu.CompilerParams(vmem_limit_bytes=min(mib * 1024 * 1024, 67043328))


def cost(flops, bytes_accessed):
    return pl.CostEstimate(flops=flops, bytes_accessed=bytes_accessed, transcendentals=0)


def dot(a, b):
    return jnp.dot(a, b, preferred_element_type=F32)


def dot_nt(a, b):
    return lax.dot_general(a, b, (((1,), (1,)), ((), ())), preferred_element_type=F32)


def dot_tn(a, b):
    return lax.dot_general(a, b, (((0,), (0,)), ((), ())), preferred_element_type=F32)


def low(a):
    return a.astype(BF16)


def split_two(a):
    high = a.astype(BF16)
    return high, (a - high.astype(F32)).astype(BF16)


def split_three(a):
    high = a.astype(BF16)
    rest = a - high.astype(F32)
    middle = rest.astype(BF16)
    return high, middle, (rest - middle.astype(F32)).astype(BF16)


def dot_fine(a, b):
    a_high, a_low = split_two(a)
    b_high, b_low = split_two(b)
    return dot(a_high, b_high) + (dot(a_high, b_low) + dot(a_low, b_high))


def pack_kernel(*refs):
    sides, packed, sems = refs[:8], refs[8], refs[9]
    for one in fetch(
        sems,
        *((ref, packed.at[n // 2, :, pl.ds(n % 2 * 128, 128)]) for n, ref in enumerate(sides)),
    ):
        one.wait()


def pack(weights):
    depth, width = weights[0].shape
    return pl.pallas_call(
        pack_kernel,
        in_specs=[anywhere()] * 8,
        out_specs=whole(),
        out_shape=pltpu.VMEM((4, depth, 2 * width), BF16),
        scratch_shapes=[pltpu.SemaphoreType.DMA((8,))],
        compiler_params=params(4),
        cost_estimate=cost(1 << 20, 8 << 20),
        name="pack",
    )(*map(home, weights))


def project_kernel(width_all, head_size, block_ref, rate_ref, *refs):
    near, (fa, sfa, fb, sfb), weights = refs[:6], refs[6:10], refs[10]
    q_ref, k_ref, v_ref, bl_ref, tail_ref, dg_ref, gu_ref, cg_ref = refs[11:19]
    far, factors = refs[19:]
    rows, piece_width = near[0].shape
    half = rows // 2

    def unit_rows(raw):
        wide = low(raw).astype(F32)
        return wide * lax.rsqrt(jnp.sum(wide * wide, axis=-1, keepdims=True) + TINY_NORM)

    def product(n, here, slots):
        total = None
        for slot in slots:
            piece = near[slot][here, :] if slot < 6 else far[slot - 6]
            offset = pl.multiple_of(block_ref[slot] * piece_width, piece_width)
            term = dot(piece, weights[n, pl.ds(offset, piece_width), :])
            total = term if total is None else total + term
        return total

    def pair(n, here):
        both = product(n, here, range(8)) * factors[here, :]
        return both[:, :128], both[:, 128:]

    def each_half(body):
        def step(n, carry):
            far[0] = jnp.where(n == 0, fa[...], fb[...])
            far[1] = jnp.where(n == 0, sfa[...], sfb[...])
            body(pl.ds(pl.multiple_of(n * half, half), half))
            return carry

        lax.fori_loop(0, 2, step, 0)

    def gated(here):
        squares = jnp.zeros((half, piece_width), F32)
        for slot in range(8):
            piece = near[slot][here, :] if slot < 6 else far[slot - 6]
            wide = piece.astype(F32)
            squares = squares + wide * wide
        squares = jnp.sum(squares, axis=1, keepdims=True)
        factors[here, :] = lax.rsqrt(squares / width_all + TINY_NORM)
        gv, gg = pair(0, here)
        gu_ref[here, :] = low(low(gv).astype(F32) * jax.nn.sigmoid(low(gg).astype(F32)))

    def gates(here):
        dg, cg = pair(1, here)
        dg_ref[here, :] = low(dg)
        cg_ref[here, :] = low(cg)

    def queries(here):
        q, k = pair(2, here)
        q_ref[here, :] = low(unit_rows(q) * head_size ** (-0.5))
        k_ref[here, :] = low(unit_rows(k))

    def rest_of(here):
        v, bl = pair(3, here)
        v_ref[here, :] = low(v)
        lane = lax.broadcasted_iota(jnp.int32, bl.shape, 1)
        bl_ref[here, :] = jnp.where(
            lane == 0, jax.nn.sigmoid(bl), -rate_ref[0] * jax.nn.softplus(bl)
        )

    def everything(here):
        for body in (gated, gates, queries, rest_of):
            body(here)

    each_half(everything)
    tail_ref[...] = gu_ref[rows - HALO :, :]


def project(pieces, weights, blocks, rate, width_all, head_size):
    rows, piece_width = pieces[0].shape
    kinds = [BF16] * 3 + [F32] + [BF16] * 3
    return pl.pallas_call(
        functools.partial(project_kernel, width_all, head_size),
        in_specs=[scalars(), scalars()] + [whole()] * 11,
        out_specs=[whole()] * 8,
        out_shape=[pltpu.VMEM((rows, 128), kind) for kind in kinds[:4]]
        + [pltpu.VMEM((HALO, 128), BF16)]
        + [pltpu.VMEM((rows, 128), kind) for kind in kinds[4:]],
        scratch_shapes=[
            pltpu.VMEM((2, rows // 2, piece_width), BF16),
            pltpu.VMEM((rows, 1), F32),
        ],
        compiler_params=params(20),
        cost_estimate=cost(2 * rows * width_all * 1024, 12 << 20),
        name="project",
    )(blocks, rate, *map(near_core, pieces), near_core(weights))


def write_state(ref, state):
    total, lost, made = state
    size = lost.shape[0]
    ref[0:size, 0:size] = low(lost)
    ref[0:size, size:] = low(made)
    row = lax.broadcasted_iota(jnp.int32, (16, 2 * size), 0)
    high, middle, rest = split_three(jnp.broadcast_to(total, (16, 2 * size)))
    packed = jnp.where(
        row == 0,
        high.astype(F32),
        jnp.where(row == 1, middle.astype(F32), rest.astype(F32)),
    )
    ref[size : size + 16, :] = low(packed)


def read_state(ref):
    size = ref.shape[1] // 2
    packed = ref[size : size + 16, 0:128].astype(F32)
    total = packed[0:1, 0:1] + packed[1:2, 0:1] + packed[2:3, 0:1]
    return (total, ref[0:size, 0:size].astype(F32), ref[0:size, size:].astype(F32))


def compose(later, earlier):
    total2, lost2, made2 = later
    total1, lost1, made1 = earlier
    size = lost1.shape[0]
    both = dot(low(lost2), low(jnp.concatenate([lost1, made1], axis=1)))
    lost = total2 * lost1 + total1 * lost2 - both[:, :size]
    made = total2 * made1 - both[:, size:] + made2
    return (total1 * total2, lost, made)


def delta_kernel(
    q_ref, k_ref, v_ref, bl_ref, coef_p_ref, coef_q_ref, state_ref
):
    rows, size = q_ref.shape
    chunks = rows // CHUNK
    row = lax.broadcasted_iota(jnp.int32, (CHUNK, CHUNK), 0)
    column = lax.broadcasted_iota(jnp.int32, (CHUNK, CHUNK), 1)
    causal = row >= column
    strict = row > column
    ones = jnp.where(causal, 1.0, 0.0).astype(BF16)
    lowers, inverses, scores, grown, tails = [], [], [], [], []
    betas = []
    for n in range(chunks):
        here = slice(n * CHUNK, (n + 1) * CHUNK)
        both = bl_ref[here, :]
        beta = both[:, 0:1]
        high, middle, rest = split_three(both)
        sums = dot(ones, high) + (dot(ones, middle) + dot(ones, rest))
        log_sum = jnp.broadcast_to(sums[:, 1:2], (CHUNK, CHUNK))
        damping = jnp.where(causal, jnp.exp(jnp.minimum(log_sum - log_sum.T, 0.0)), 0.0)
        k = k_ref[here, :]
        lower = jnp.where(strict, dot_nt(k, k) * damping, 0.0) * beta
        scores.append(low(dot_nt(q_ref[here, :], k) * damping))
        lowers.append(lower)
        betas.append(beta)
        grown.append(log_sum)
        tails.append(log_sum[CHUNK - 1 : CHUNK, :])
        below = ((row & 1) == 1) & (column == row - 1)
        inverses.append(jnp.where(row == column, 1.0, 0.0) - jnp.where(below, lower, 0.0))
    level = 2
    while level < CHUNK:
        shift = level.bit_length() - 1
        part = row >> shift
        below = ((part & 1) == 1) & ((column >> shift) == part - 1)
        multiply = dot_fine if level >= 32 else (lambda a, b: dot(low(a), low(b)))
        moved = [
            multiply(inverse, jnp.where(below, lower, 0.0))
            for inverse, lower in zip(inverses, lowers)
        ]
        inverses = [
            inverse - multiply(middle, inverse) for inverse, middle in zip(inverses, moved)
        ]
        level *= 2
    queries, starts, losts, mades = [], [], [], []
    for n in range(chunks):
        here = slice(n * CHUNK, (n + 1) * CHUNK)
        k = k_ref[here, :].astype(F32)
        grow = jnp.exp(grown[n])
        right = jnp.concatenate(
            [v_ref[here, :].astype(F32) * betas[n], k * (betas[n] * grow)], axis=1
        )
        solved = low(dot(low(inverses[n]), low(right)))
        seen = dot(scores[n], solved)
        starts.append(seen[:, :size])
        queries.append(low(q_ref[here, :].astype(F32) * grow - seen[:, size:]))
        weighted = low(k * jnp.exp(tails[n] - grown[n]))
        written = dot_tn(weighted, solved)
        mades.append(written[:, :size])
        losts.append(low(written[:, size:]))
    carried = jnp.where(row == column, 1.0, 0.0)
    made = jnp.zeros((CHUNK, size), F32)
    log_total = jnp.zeros((1, CHUNK), F32)
    for n in range(chunks):
        here = slice(n * CHUNK, (n + 1) * CHUNK)
        rounded = low(jnp.concatenate([carried, made], axis=1))
        seen = dot(queries[n], rounded)
        coef_p_ref[here, :] = low(seen[:, :size])
        coef_q_ref[here, :] = seen[:, size:] + starts[n]
        moved = dot(losts[n], rounded)
        keep = jnp.exp(tails[n])
        carried = carried * keep - moved[:, :size]
        made = made * keep - moved[:, size:] + mades[n]
        log_total = log_total + tails[n]
    total = jnp.exp(log_total)[:, 0:1]
    lost = jnp.where(row == column, total, 0.0) - carried
    write_state(state_ref, (total, lost, made))


def delta(q, k, v, bl):
    rows, size = q.shape
    return pl.pallas_call(
        delta_kernel,
        in_specs=[whole()] * 4,
        out_specs=[whole()] * 3,
        out_shape=[
            pltpu.VMEM((rows, size), BF16),
            pltpu.VMEM((rows, size), F32),
            pltpu.VMEM((size + 16, 2 * size), BF16),
        ],
        compiler_params=params(16),
        cost_estimate=cost(2 * rows * size * size * 60, 3 << 20),
        name="delta",
    )(*map(near_core, (q, k, v, bl)))


def along_kernel(which, place_ref, p0, p1, p2, p3, before_ref, out_ref, held):
    me = place_ref[which]
    for j, piece in ((0, p0), (2, p1), (3, p2), (1, p3)):
        held[(me - j + 4) & 3] = piece[...]
    size = p0.shape[1] // 2
    nothing = (jnp.ones((1, 1), F32), jnp.zeros((size, size), F32), jnp.zeros((size, size), F32))
    before = nothing
    so_far = read_state(held.at[0])
    for m in range(1, 4):
        before = tuple(jnp.where(me == m, a, b) for a, b in zip(so_far, before))
        so_far = compose(read_state(held.at[m]), so_far)
    write_state(before_ref, before)
    if out_ref.shape == p0.shape:
        write_state(out_ref, so_far)
    else:
        out_ref[...] = low(so_far[2])


def along(which, places, out_shape, state, *others):
    return pl.pallas_call(
        functools.partial(along_kernel, which),
        in_specs=[scalars()] + [whole()] * 4,
        out_specs=[whole()] * 2,
        out_shape=[pltpu.VMEM(state.shape, BF16), pltpu.VMEM(out_shape, BF16)],
        scratch_shapes=[pltpu.VMEM((4,) + state.shape, BF16)],
        compiler_params=params(4),
        cost_estimate=cost(16 << 20, 1 << 18),
        name="along",
    )(places, *map(near_core, (state,) + others))


def cyclic(block, axis, distance):
    count = lax.axis_size(axis)
    return lax.ppermute(block, axis, [(i, (i + distance) % count) for i in range(count)])


def shifted(block, axis, distance):
    devices = range(lax.axis_size(axis))
    return lax.ppermute(block, axis, [(i, i + distance) for i in devices if i + distance in devices])


def swapped(block):
    return lax.ppermute(block, "c", [(0, 1), (1, 0)])


def exchanged(parts):
    got = [parts[0]]
    for slot in range(1, 8):
        step, side = STEPS[slot // 2], slot % 2
        route = [(y * 2 + c, (y + step) % 4 * 2 + (c ^ side)) for y in range(4) for c in range(2)]
        got.append(lax.ppermute(parts[slot], TP, route))
    return got


def finish_kernel(
    block_ref, coef_p_ref, coef_q_ref, dg_ref, gain_ref, reach_ref, far_ref, before_ref, *outs
):
    total, lost, made = read_state(reach_ref)
    state = total * far_ref[...].astype(F32) - dot(low(lost), far_ref[...]) + made
    total, lost, made = read_state(before_ref)
    state = low(total * state - dot(low(lost), low(state)) + made)
    step = outs[0].shape[0]
    for slot in range(8):
        here = pl.ds(pl.multiple_of(block_ref[GOES_TO[slot]] * step, step), step)
        result = coef_q_ref[here, :] + dot(coef_p_ref[here, :], state)
        mean = jnp.sum(result * result, axis=-1, keepdims=True) * (1.0 / result.shape[1])
        result = result * lax.rsqrt(mean + TINY_NORM) * gain_ref[...]
        outs[slot][...] = low(result * jax.nn.silu(dg_ref[here, :].astype(F32)))


def finish(blocks, *args):
    rows, size = args[0].shape
    return pl.pallas_call(
        finish_kernel,
        in_specs=[scalars()] + [whole()] * 7,
        out_specs=[whole()] * 8,
        out_shape=[pltpu.VMEM((rows // 8, size), BF16)] * 8,
        compiler_params=params(6),
        cost_estimate=cost(64 << 20, 2 << 20),
        name="finish",
    )(blocks, *map(near_core, args))


def conv_kernel(block_ref, gu_ref, before_ref, taps_ref, cg_ref, *rest):
    outs, (padded, out_ref) = rest[:4], rest[4:]
    rows, size = gu_ref.shape
    head = before_ref.shape[0]
    count = taps_ref.shape[0]
    padded[0:head, :] = before_ref[...].astype(F32)
    padded[head:, :] = gu_ref[...].astype(F32)
    taps = taps_ref[...].astype(F32)
    step = 64
    skip = head - (count - 1)

    def block(n, carry):
        base = pl.multiple_of(n * step, step)
        total = jnp.zeros((step, size), F32)
        for j in range(count):
            total = total + padded[pl.ds(base + skip + j, step), :] * taps[j : j + 1, :]
        out_ref[pl.ds(base, step), :] = low(total)
        return carry

    lax.fori_loop(0, rows // step, block, 0)
    part = rows // 8
    for slot in range(8):
        here = pl.ds(pl.multiple_of(block_ref[GOES_TO[slot]] * part, part), part)
        there = slice(slot % 2 * part, (slot % 2 + 1) * part)
        outs[slot // 2][there, 0:size] = out_ref[here, :]
        outs[slot // 2][there, size:] = cg_ref[here, :]


def conv(blocks, gu, before, taps, cg):
    rows, size = gu.shape
    return pl.pallas_call(
        conv_kernel,
        in_specs=[scalars()] + [whole()] * 4,
        out_specs=[whole()] * 4,
        out_shape=[pltpu.VMEM((rows // 4, 2 * size), BF16)] * 4,
        scratch_shapes=[
            pltpu.VMEM((rows + before.shape[0], size), F32),
            pltpu.VMEM((rows, size), BF16),
        ],
        compiler_params=params(8),
        cost_estimate=cost(256 << 20, 1 << 20),
        name="conv",
    )(blocks, *map(near_core, (gu, before, taps, cg)))


def add_slots(out_ref, left, weights, tops, start):
    size = left[0].shape[1]

    def step(n, carry):
        here = pl.ds(pl.multiple_of(n * 512, 512), 512)
        acc = jnp.zeros((out_ref.shape[0], 512), F32) if start is None else start[:, here]
        for part, ref, top in zip(left, weights, tops):
            acc = acc + dot(part[...], ref[top : top + size, here])
        out_ref[:, here] = acc.astype(out_ref.dtype)
        return carry

    lax.fori_loop(0, out_ref.shape[1] // 512, step, 0)


def cut_kernel(count, right_any, left_any, top_ref, rest_ref, sems):
    for one in fetch(
        sems,
        (right_any.at[pl.ds(0, count), :], top_ref),
        (left_any.at[pl.ds(count, rest_ref.shape[0]), :], rest_ref),
    ):
        one.wait()


def cut(right, left, count):
    rows, width = right.shape
    return pl.pallas_call(
        functools.partial(cut_kernel, count),
        in_specs=[anywhere()] * 2,
        out_specs=[whole()] * 2,
        out_shape=[pltpu.VMEM((count, width), BF16), pltpu.VMEM((rows - count, width), BF16)],
        scratch_shapes=[pltpu.SemaphoreType.DMA((2,))],
        compiler_params=params(4),
        cost_estimate=cost(1 << 20, 4 << 20),
        name="cut",
    )(right, left)


def conv_out_kernel(*refs):
    both, weights, out_ref, mixed = refs[:8], refs[8:16], refs[16], refs[17]
    groups, rows, size = mixed.shape
    got = [ref.at[slot % 2 * rows : (slot % 2 + 1) * rows, :] for slot, ref in enumerate(both)]
    tops = [0 if ref.shape[0] == size + 16 else size for ref in weights]
    total = jnp.zeros((rows, size), F32)
    total_square = jnp.zeros((rows, size), F32)
    for ref in got:
        part = ref[:, 0:size].astype(F32)
        total = total + part
        total_square = total_square + part * part
    scale = 1.0 / (groups * size)
    center = jnp.sum(total, axis=1, keepdims=True) * scale
    second = jnp.sum(total_square, axis=1, keepdims=True) * scale
    factor = lax.rsqrt(jnp.maximum(second - center * center, 0.0) + TINY_VAR)
    for slot in range(groups):
        top = tops[slot] + size
        extra = weights[slot][top : top + 16, :].astype(F32)
        gain = extra[0:1, 0:size] + extra[1:2, 0:size] + extra[2:3, 0:size]
        shift = extra[3:4, 0:size] + extra[4:5, 0:size] + extra[5:6, 0:size]
        normed = (got[slot][:, 0:size].astype(F32) - center) * factor * gain + shift
        gate = got[slot][:, size:].astype(F32)
        mixed[slot] = low(jax.nn.silu(normed) * jax.nn.silu(gate))
    add_slots(out_ref, [mixed.at[slot] for slot in range(groups)], weights, tops, None)


def conv_out(got, weights):
    groups = len(got)
    rows, both = got[0].shape
    rows, size, width = rows // 2, both // 2, weights[0].shape[1]
    return pl.pallas_call(
        conv_out_kernel,
        in_specs=[whole()] * 16,
        out_specs=whole(),
        out_shape=pltpu.VMEM((rows, width), F32),
        scratch_shapes=[pltpu.VMEM((groups, rows, size), BF16)],
        compiler_params=params(8),
        cost_estimate=cost(2 * rows * 1024 * width, 6 << 20),
        name="conv_out",
    )(*map(near_core, got), *map(near_core, weights))


def delta_out_kernel(conv_ref, *refs):
    got, weights, out_hbm, staged, sems = refs[:8], refs[8:16], refs[16], refs[17], refs[18]
    size = got[0].shape[1]
    stores = []
    for n, base in enumerate(range(0, staged.shape[1], 512)):
        here = slice(base, base + 512)
        acc = conv_ref[:, here]
        for part, ref in zip(got, weights):
            acc = acc + dot(part[...], ref[0:size, here])
        staged[:, here] = low(acc)
        stores += fetch(sems.at[pl.ds(n, 1)], (staged.at[:, here], out_hbm.at[:, here]))
    for one in stores:
        one.wait()


def delta_out(got, conv_part, weights):
    rows, width = conv_part.shape
    return pl.pallas_call(
        delta_out_kernel,
        in_specs=[whole()] * 17,
        out_specs=hbm(),
        out_shape=jax.ShapeDtypeStruct((rows, width), BF16),
        scratch_shapes=[pltpu.VMEM((rows, width), BF16), pltpu.SemaphoreType.DMA((4,))],
        compiler_params=params(8),
        cost_estimate=cost(2 * rows * 1024 * width, 6 << 20),
        name="delta_out",
    )(near_core(conv_part), *map(near_core, got), *map(near_core, weights))


def local(
    tokens,
    w_query,
    w_key,
    w_value,
    w_delta_gate,
    w_glu_value,
    w_glu_gate,
    w_conv_gate,
    w_beta,
    w_decay,
    decay_log,
    head_gain,
    conv_taps,
    ln_gain,
    ln_shift,
    out_delta,
    out_conv,
):
    rows = tokens.shape[0]
    half = rows // 2
    size = w_query.shape[1]
    y, core = lax.axis_index("y"), lax.axis_index("c")
    x, z = lax.axis_index("x"), lax.axis_index("z")
    count_y = lax.axis_size("y")
    head = y * 2 + core
    chips = [y, (y - 1) % count_y, (y + 1) % count_y, (y + 2) % count_y]
    slots = [chip * 2 + side for chip in chips for side in (core, 1 - core)]
    blocks = jnp.stack(slots + [x, z % 4])
    blocks = blocks.astype(jnp.int32)

    beta_decay = jnp.concatenate(
        [
            lax.dynamic_slice_in_dim(w_beta, head, 1, 1),
            lax.dynamic_slice_in_dim(w_decay, head, 1, 1),
            jnp.zeros((w_beta.shape[0], 126), BF16),
        ],
        axis=1,
    )
    weights = (
        w_glu_value,
        w_glu_gate,
        w_delta_gate,
        w_conv_gate,
        w_query,
        w_key,
        w_value,
        beta_decay,
    )
    rate = jnp.exp(lax.dynamic_slice_in_dim(decay_log, head, 1, 0))

    def three(vector):
        high = lax.reduce_precision(vector, 8, 7)
        rest = vector - high
        middle = lax.reduce_precision(rest, 8, 7)
        return [high, middle, rest - middle]

    extra = jnp.stack(three(ln_gain) + three(ln_shift)).astype(BF16)
    extra = jnp.pad(extra, ((0, 10), (0, out_conv.shape[1] - extra.shape[1])))
    last = jnp.concatenate([out_delta, out_conv, extra], axis=0)

    own = tokens
    r1, l1 = cyclic(own, "y", 1), cyclic(own, "y", -1)
    sw = swapped(own)
    blocks, rate, last, beta_decay = lax.optimization_barrier((blocks, rate, last, beta_decay))
    weights = pack(weights[:7] + (beta_decay,))
    r1_top, l1_rest = cut(r1, l1, half)
    fa, fb = cyclic(r1_top, "y", 1), cyclic(l1_rest, "y", -1)
    sr1, sl1 = swapped(r1), swapped(l1)
    sfa, sfb = swapped(fa), swapped(fb)
    pieces = [own, sw, r1, sr1, l1, sl1, fa, sfa, fb, sfb]
    wr, wl = cyclic(last, "y", 1), cyclic(last, "y", -1)
    q, k, v, bl, tail, dg, gu, cg = project(pieces, weights, blocks, rate, 2048, size)

    coef_p, coef_q, state = delta(q, k, v, bl)


    before, total = along(8, blocks, state.shape, state, *(cyclic(state, "x", j) for j in (2, 3, 1)))
    route = lambda j: [(h + i, h + (i + j) % 4) for h in (0, 4) for i in range(4)]
    around = []
    for j in (2, 3, 1):
        around.append(lax.ppermute(total, "z", route(j)))
    before_z, made_z = along(9, blocks, (size, size), total, *around)
    far = shifted(made_z, "z", 4)

    ws = swapped(last)
    wr_top, wl_rest = cut(wr, wl, size)
    wfa, wfb = cyclic(wr_top, "y", 1), cyclic(wl_rest, "y", -1)
    wsr, wsl = swapped(wr), swapped(wl)
    wsfa, wsfb = swapped(wfa), swapped(wfb)
    near = [last, ws, wr, wsr, wl, wsl]
    delta_weights = near + [wfa, wsfa]
    conv_weights = near + [wfb, wsfb]

    halo = lax.ppermute(tail, SP, [(i, i + 1) for i in range(31)])
    filtered = conv(blocks, gu, halo, conv_taps, cg)
    got = []
    for chip, part in enumerate(filtered):
        if chip:
            part = cyclic(part, "y", STEPS[chip])
        got += [part, swapped(part)]
    conv_part = conv_out(got, conv_weights)

    mixed = finish(blocks, coef_p, coef_q, dg, head_gain[None, :], before_z, far, before)
    return delta_out(exchanged(mixed), conv_part, delta_weights)


def solution(mesh):
    finer = Mesh(mesh.devices.reshape(8, 4, 4, 2), ("z", "x", "y", "c"))
    placed = (
        P(SP, TP),
        P(None, TP),
        P(None, TP),
        P(None, TP),
        P(None, TP),
        P(None, TP),
        P(None, TP),
        P(None, TP),
        P(),
        P(),
        P(),
        P(),
        P(None, TP),
        P(TP),
        P(TP),
        P(TP, None),
        P(TP, None),
    )
    return jax.shard_map(
        local, mesh=finer, in_specs=placed, out_specs=P(SP + TP, None), check_vma=False
    )
```

```python
import functools

import jax
import jax.numpy as jnp
from jax import lax
from jax.experimental import pallas as pl
from jax.experimental.pallas import tpu as pltpu
from jax.sharding import Mesh
from jax.sharding import PartitionSpec as P


SP = ("z", "x")
TP = ("y", "c")
TINY_NORM = 1e-06
TINY_VAR = 1e-05
CHUNK = 128
HALO = 32
STEPS = (0, 1, -1, 2)
GOES_TO = (0, 1, 4, 5, 2, 3, 6, 7)
F32 = jnp.float32
BF16 = jnp.bfloat16


def whole():
    return pl.BlockSpec(memory_space=pltpu.VMEM)


def hbm():
    return pl.BlockSpec(memory_space=pltpu.HBM)


def anywhere():
    return pl.BlockSpec(memory_space=pl.ANY)


def home(array):
    return pltpu.with_memory_space_constraint(array, pltpu.HBM)


def near_core(array):
    return pltpu.with_memory_space_constraint(array, pltpu.VMEM)


def fetch(sems, *pairs):
    copies = [pltpu.make_async_copy(a, b, sems.at[n]) for n, (a, b) in enumerate(pairs)]
    for one in copies:
        one.start()
    return copies


def scalars():
    return pl.BlockSpec(memory_space=pltpu.SMEM)


def params(mib):
    return pltpu.CompilerParams(vmem_limit_bytes=min(mib * 1024 * 1024, 67043328))


def cost(flops, bytes_accessed):
    return pl.CostEstimate(flops=flops, bytes_accessed=bytes_accessed, transcendentals=0)


def dot(a, b):
    return jnp.dot(a, b, preferred_element_type=F32)


def dot_nt(a, b):
    return lax.dot_general(a, b, (((1,), (1,)), ((), ())), preferred_element_type=F32)


def dot_tn(a, b):
    return lax.dot_general(a, b, (((0,), (0,)), ((), ())), preferred_element_type=F32)


def low(a):
    return a.astype(BF16)


def split_two(a):
    high = a.astype(BF16)
    return high, (a - high.astype(F32)).astype(BF16)


def split_three(a):
    high = a.astype(BF16)
    rest = a - high.astype(F32)
    middle = rest.astype(BF16)
    return high, middle, (rest - middle.astype(F32)).astype(BF16)


def dot_fine(a, b):
    a_high, a_low = split_two(a)
    b_high, b_low = split_two(b)
    return dot(a_high, b_high) + (dot(a_high, b_low) + dot(a_low, b_high))


def pack_kernel(*refs):
    sides, packed, sems = refs[:8], refs[8], refs[9]
    for one in fetch(
        sems,
        *((ref, packed.at[n // 2, :, pl.ds(n % 2 * 128, 128)]) for n, ref in enumerate(sides)),
    ):
        one.wait()


def pack(weights):
    depth, width = weights[0].shape
    return pl.pallas_call(
        pack_kernel,
        in_specs=[anywhere()] * 8,
        out_specs=whole(),
        out_shape=pltpu.VMEM((4, depth, 2 * width), BF16),
        scratch_shapes=[pltpu.SemaphoreType.DMA((8,))],
        compiler_params=params(4),
        cost_estimate=cost(1 << 20, 8 << 20),
        name="pack",
    )(*map(home, weights))


def project_kernel(width_all, head_size, block_ref, rate_ref, *refs):
    near, (fa, sfa, fb, sfb), weights = refs[:6], refs[6:10], refs[10]
    q_ref, k_ref, v_ref, bl_ref, tail_ref, dg_ref, gu_ref, cg_ref = refs[11:19]
    far, factors = refs[19:]
    rows, piece_width = near[0].shape
    half = rows // 2

    def unit_rows(raw):
        wide = low(raw).astype(F32)
        return wide * lax.rsqrt(jnp.sum(wide * wide, axis=-1, keepdims=True) + TINY_NORM)

    def product(n, here, slots):
        total = None
        for slot in slots:
            piece = near[slot][here, :] if slot < 6 else far[slot - 6]
            offset = pl.multiple_of(block_ref[slot] * piece_width, piece_width)
            term = dot(piece, weights[n, pl.ds(offset, piece_width), :])
            total = term if total is None else total + term
        return total

    def pair(n, here):
        both = product(n, here, range(8)) * factors[here, :]
        return both[:, :128], both[:, 128:]

    def each_half(body):
        def step(n, carry):
            far[0] = jnp.where(n == 0, fa[...], fb[...])
            far[1] = jnp.where(n == 0, sfa[...], sfb[...])
            body(pl.ds(pl.multiple_of(n * half, half), half))
            return carry

        lax.fori_loop(0, 2, step, 0)

    def gated(here):
        squares = jnp.zeros((half, piece_width), F32)
        for slot in range(8):
            piece = near[slot][here, :] if slot < 6 else far[slot - 6]
            wide = piece.astype(F32)
            squares = squares + wide * wide
        squares = jnp.sum(squares, axis=1, keepdims=True)
        factors[here, :] = lax.rsqrt(squares / width_all + TINY_NORM)
        gv, gg = pair(0, here)
        gu_ref[here, :] = low(low(gv).astype(F32) * jax.nn.sigmoid(low(gg).astype(F32)))

    def gates(here):
        dg, cg = pair(1, here)
        dg_ref[here, :] = low(dg)
        cg_ref[here, :] = low(cg)

    def queries(here):
        q, k = pair(2, here)
        q_ref[here, :] = low(unit_rows(q) * head_size ** (-0.5))
        k_ref[here, :] = low(unit_rows(k))

    def rest_of(here):
        v, bl = pair(3, here)
        v_ref[here, :] = low(v)
        lane = lax.broadcasted_iota(jnp.int32, bl.shape, 1)
        bl_ref[here, :] = jnp.where(
            lane == 0, jax.nn.sigmoid(bl), -rate_ref[0] * jax.nn.softplus(bl)
        )

    def everything(here):
        for body in (gated, gates, queries, rest_of):
            body(here)

    each_half(everything)
    tail_ref[...] = gu_ref[rows - HALO :, :]


def project(pieces, weights, blocks, rate, width_all, head_size):
    rows, piece_width = pieces[0].shape
    kinds = [BF16] * 3 + [F32] + [BF16] * 3
    return pl.pallas_call(
        functools.partial(project_kernel, width_all, head_size),
        in_specs=[scalars(), scalars()] + [whole()] * 11,
        out_specs=[whole()] * 8,
        out_shape=[pltpu.VMEM((rows, 128), kind) for kind in kinds[:4]]
        + [pltpu.VMEM((HALO, 128), BF16)]
        + [pltpu.VMEM((rows, 128), kind) for kind in kinds[4:]],
        scratch_shapes=[
            pltpu.VMEM((2, rows // 2, piece_width), BF16),
            pltpu.VMEM((rows, 1), F32),
        ],
        compiler_params=params(20),
        cost_estimate=cost(2 * rows * width_all * 1024, 12 << 20),
        name="project",
    )(blocks, rate, *map(near_core, pieces), near_core(weights))


def write_state(ref, state):
    total, lost, made = state
    size = lost.shape[0]
    ref[0:size, 0:size] = low(lost)
    ref[0:size, size:] = low(made)
    row = lax.broadcasted_iota(jnp.int32, (16, 2 * size), 0)
    high, middle, rest = split_three(jnp.broadcast_to(total, (16, 2 * size)))
    packed = jnp.where(
        row == 0,
        high.astype(F32),
        jnp.where(row == 1, middle.astype(F32), rest.astype(F32)),
    )
    ref[size : size + 16, :] = low(packed)


def read_state(ref):
    size = ref.shape[1] // 2
    packed = ref[size : size + 16, 0:128].astype(F32)
    total = packed[0:1, 0:1] + packed[1:2, 0:1] + packed[2:3, 0:1]
    return (total, ref[0:size, 0:size].astype(F32), ref[0:size, size:].astype(F32))


def compose(later, earlier):
    total2, lost2, made2 = later
    total1, lost1, made1 = earlier
    size = lost1.shape[0]
    both = dot(low(lost2), low(jnp.concatenate([lost1, made1], axis=1)))
    lost = total2 * lost1 + total1 * lost2 - both[:, :size]
    made = total2 * made1 - both[:, size:] + made2
    return (total1 * total2, lost, made)


def delta_kernel(
    q_ref, k_ref, v_ref, bl_ref, coef_p_ref, coef_q_ref, state_ref
):
    rows, size = q_ref.shape
    chunks = rows // CHUNK
    row = lax.broadcasted_iota(jnp.int32, (CHUNK, CHUNK), 0)
    column = lax.broadcasted_iota(jnp.int32, (CHUNK, CHUNK), 1)
    causal = row >= column
    strict = row > column
    ones = jnp.where(causal, 1.0, 0.0).astype(BF16)
    lowers, inverses, scores, grown, tails = [], [], [], [], []
    betas = []
    for n in range(chunks):
        here = slice(n * CHUNK, (n + 1) * CHUNK)
        both = bl_ref[here, :]
        beta = both[:, 0:1]
        high, middle, rest = split_three(both)
        sums = dot(ones, high) + (dot(ones, middle) + dot(ones, rest))
        log_sum = jnp.broadcast_to(sums[:, 1:2], (CHUNK, CHUNK))
        damping = jnp.where(causal, jnp.exp(jnp.minimum(log_sum - log_sum.T, 0.0)), 0.0)
        k = k_ref[here, :]
        lower = jnp.where(strict, dot_nt(k, k) * damping, 0.0) * beta
        scores.append(low(dot_nt(q_ref[here, :], k) * damping))
        lowers.append(lower)
        betas.append(beta)
        grown.append(log_sum)
        tails.append(log_sum[CHUNK - 1 : CHUNK, :])
        below = ((row & 1) == 1) & (column == row - 1)
        inverses.append(jnp.where(row == column, 1.0, 0.0) - jnp.where(below, lower, 0.0))
    level = 2
    while level < CHUNK:
        shift = level.bit_length() - 1
        part = row >> shift
        below = ((part & 1) == 1) & ((column >> shift) == part - 1)
        multiply = dot_fine if level >= 32 else (lambda a, b: dot(low(a), low(b)))
        moved = [
            multiply(inverse, jnp.where(below, lower, 0.0))
            for inverse, lower in zip(inverses, lowers)
        ]
        inverses = [
            inverse - multiply(middle, inverse) for inverse, middle in zip(inverses, moved)
        ]
        level *= 2
    queries, starts, losts, mades = [], [], [], []
    for n in range(chunks):
        here = slice(n * CHUNK, (n + 1) * CHUNK)
        k = k_ref[here, :].astype(F32)
        grow = jnp.exp(grown[n])
        right = jnp.concatenate(
            [v_ref[here, :].astype(F32) * betas[n], k * (betas[n] * grow)], axis=1
        )
        solved = low(dot(low(inverses[n]), low(right)))
        seen = dot(scores[n], solved)
        starts.append(seen[:, :size])
        queries.append(low(q_ref[here, :].astype(F32) * grow - seen[:, size:]))
        weighted = low(k * jnp.exp(tails[n] - grown[n]))
        written = dot_tn(weighted, solved)
        mades.append(written[:, :size])
        losts.append(low(written[:, size:]))
    carried = jnp.where(row == column, 1.0, 0.0)
    made = jnp.zeros((CHUNK, size), F32)
    log_total = jnp.zeros((1, CHUNK), F32)
    for n in range(chunks):
        here = slice(n * CHUNK, (n + 1) * CHUNK)
        rounded = low(jnp.concatenate([carried, made], axis=1))
        seen = dot(queries[n], rounded)
        coef_p_ref[here, :] = low(seen[:, :size])
        coef_q_ref[here, :] = seen[:, size:] + starts[n]
        moved = dot(losts[n], rounded)
        keep = jnp.exp(tails[n])
        carried = carried * keep - moved[:, :size]
        made = made * keep - moved[:, size:] + mades[n]
        log_total = log_total + tails[n]
    total = jnp.exp(log_total)[:, 0:1]
    lost = jnp.where(row == column, total, 0.0) - carried
    write_state(state_ref, (total, lost, made))


def delta(q, k, v, bl):
    rows, size = q.shape
    return pl.pallas_call(
        delta_kernel,
        in_specs=[whole()] * 4,
        out_specs=[whole()] * 3,
        out_shape=[
            pltpu.VMEM((rows, size), BF16),
            pltpu.VMEM((rows, size), F32),
            pltpu.VMEM((size + 16, 2 * size), BF16),
        ],
        compiler_params=params(16),
        cost_estimate=cost(2 * rows * size * size * 60, 3 << 20),
        name="delta",
    )(*map(near_core, (q, k, v, bl)))


def along_kernel(which, place_ref, p0, p1, p2, p3, before_ref, out_ref, held):
    me = place_ref[which]
    for j, piece in ((0, p0), (2, p1), (3, p2), (1, p3)):
        held[(me - j + 4) & 3] = piece[...]
    size = p0.shape[1] // 2
    nothing = (jnp.ones((1, 1), F32), jnp.zeros((size, size), F32), jnp.zeros((size, size), F32))
    before = nothing
    so_far = read_state(held.at[0])
    for m in range(1, 4):
        before = tuple(jnp.where(me == m, a, b) for a, b in zip(so_far, before))
        so_far = compose(read_state(held.at[m]), so_far)
    write_state(before_ref, before)
    if out_ref.shape == p0.shape:
        write_state(out_ref, so_far)
    else:
        out_ref[...] = low(so_far[2])


def along(which, places, out_shape, state, *others):
    return pl.pallas_call(
        functools.partial(along_kernel, which),
        in_specs=[scalars()] + [whole()] * 4,
        out_specs=[whole()] * 2,
        out_shape=[pltpu.VMEM(state.shape, BF16), pltpu.VMEM(out_shape, BF16)],
        scratch_shapes=[pltpu.VMEM((4,) + state.shape, BF16)],
        compiler_params=params(4),
        cost_estimate=cost(16 << 20, 1 << 18),
        name="along",
    )(places, *map(near_core, (state,) + others))


def cyclic(block, axis, distance):
    count = lax.axis_size(axis)
    return lax.ppermute(block, axis, [(i, (i + distance) % count) for i in range(count)])


def shifted(block, axis, distance):
    devices = range(lax.axis_size(axis))
    return lax.ppermute(block, axis, [(i, i + distance) for i in devices if i + distance in devices])


def swapped(block):
    return lax.ppermute(block, "c", [(0, 1), (1, 0)])


def exchanged(parts):
    got = []
    for chip, part in enumerate(parts):
        if chip:
            part = cyclic(part, "y", STEPS[chip])
        got += [part, swapped(part)]
    return got


def finish_kernel(
    block_ref, coef_p_ref, coef_q_ref, dg_ref, gain_ref, reach_ref, far_ref, before_ref, *outs
):
    total, lost, made = read_state(reach_ref)
    state = total * far_ref[...].astype(F32) - dot(low(lost), far_ref[...]) + made
    total, lost, made = read_state(before_ref)
    state = low(total * state - dot(low(lost), low(state)) + made)
    step = outs[0].shape[0] // 2
    for slot in range(8):
        here = pl.ds(pl.multiple_of(block_ref[GOES_TO[slot]] * step, step), step)
        result = coef_q_ref[here, :] + dot(coef_p_ref[here, :], state)
        mean = jnp.sum(result * result, axis=-1, keepdims=True) * (1.0 / result.shape[1])
        result = result * lax.rsqrt(mean + TINY_NORM) * gain_ref[...]
        there = slice(slot % 2 * step, (slot % 2 + 1) * step)
        outs[slot // 2][there, :] = low(result * jax.nn.silu(dg_ref[here, :].astype(F32)))


def finish(blocks, *args):
    rows, size = args[0].shape
    return pl.pallas_call(
        finish_kernel,
        in_specs=[scalars()] + [whole()] * 7,
        out_specs=[whole()] * 4,
        out_shape=[pltpu.VMEM((rows // 4, size), BF16)] * 4,
        compiler_params=params(6),
        cost_estimate=cost(64 << 20, 2 << 20),
        name="finish",
    )(blocks, *map(near_core, args))


def conv_kernel(block_ref, gu_ref, before_ref, taps_ref, cg_ref, *rest):
    outs, (padded, out_ref) = rest[:4], rest[4:]
    rows, size = gu_ref.shape
    head = before_ref.shape[0]
    count = taps_ref.shape[0]
    padded[0:head, :] = before_ref[...].astype(F32)
    padded[head:, :] = gu_ref[...].astype(F32)
    taps = taps_ref[...].astype(F32)
    step = 64
    skip = head - (count - 1)

    def block(n, carry):
        base = pl.multiple_of(n * step, step)
        total = jnp.zeros((step, size), F32)
        for j in range(count):
            total = total + padded[pl.ds(base + skip + j, step), :] * taps[j : j + 1, :]
        out_ref[pl.ds(base, step), :] = low(total)
        return carry

    lax.fori_loop(0, rows // step, block, 0)
    part = rows // 8
    for slot in range(8):
        here = pl.ds(pl.multiple_of(block_ref[GOES_TO[slot]] * part, part), part)
        there = slice(slot % 2 * part, (slot % 2 + 1) * part)
        outs[slot // 2][there, 0:size] = out_ref[here, :]
        outs[slot // 2][there, size:] = cg_ref[here, :]


def conv(blocks, gu, before, taps, cg):
    rows, size = gu.shape
    return pl.pallas_call(
        conv_kernel,
        in_specs=[scalars()] + [whole()] * 4,
        out_specs=[whole()] * 4,
        out_shape=[pltpu.VMEM((rows // 4, 2 * size), BF16)] * 4,
        scratch_shapes=[
            pltpu.VMEM((rows + before.shape[0], size), F32),
            pltpu.VMEM((rows, size), BF16),
        ],
        compiler_params=params(8),
        cost_estimate=cost(256 << 20, 1 << 20),
        name="conv",
    )(blocks, *map(near_core, (gu, before, taps, cg)))


def add_slots(out_ref, left, weights, tops, start):
    size = left[0].shape[1]

    def step(n, carry):
        here = pl.ds(pl.multiple_of(n * 512, 512), 512)
        acc = jnp.zeros((out_ref.shape[0], 512), F32) if start is None else start[:, here]
        for part, ref, top in zip(left, weights, tops):
            acc = acc + dot(part[...], ref[top : top + size, here])
        out_ref[:, here] = acc.astype(out_ref.dtype)
        return carry

    lax.fori_loop(0, out_ref.shape[1] // 512, step, 0)


def cut_kernel(count, right_any, left_any, top_ref, rest_ref, sems):
    for one in fetch(
        sems,
        (right_any.at[pl.ds(0, count), :], top_ref),
        (left_any.at[pl.ds(count, rest_ref.shape[0]), :], rest_ref),
    ):
        one.wait()


def cut(right, left, count):
    rows, width = right.shape
    return pl.pallas_call(
        functools.partial(cut_kernel, count),
        in_specs=[anywhere()] * 2,
        out_specs=[whole()] * 2,
        out_shape=[pltpu.VMEM((count, width), BF16), pltpu.VMEM((rows - count, width), BF16)],
        scratch_shapes=[pltpu.SemaphoreType.DMA((2,))],
        compiler_params=params(4),
        cost_estimate=cost(1 << 20, 4 << 20),
        name="cut",
    )(right, left)


def conv_out_kernel(*refs):
    both, weights, out_ref, mixed = refs[:8], refs[8:16], refs[16], refs[17]
    groups, rows, size = mixed.shape
    got = [ref.at[slot % 2 * rows : (slot % 2 + 1) * rows, :] for slot, ref in enumerate(both)]
    tops = [0 if ref.shape[0] == size + 16 else size for ref in weights]
    total = jnp.zeros((rows, size), F32)
    total_square = jnp.zeros((rows, size), F32)
    for ref in got:
        part = ref[:, 0:size].astype(F32)
        total = total + part
        total_square = total_square + part * part
    scale = 1.0 / (groups * size)
    center = jnp.sum(total, axis=1, keepdims=True) * scale
    second = jnp.sum(total_square, axis=1, keepdims=True) * scale
    factor = lax.rsqrt(jnp.maximum(second - center * center, 0.0) + TINY_VAR)
    for slot in range(groups):
        top = tops[slot] + size
        extra = weights[slot][top : top + 16, :].astype(F32)
        gain = extra[0:1, 0:size] + extra[1:2, 0:size] + extra[2:3, 0:size]
        shift = extra[3:4, 0:size] + extra[4:5, 0:size] + extra[5:6, 0:size]
        normed = (got[slot][:, 0:size].astype(F32) - center) * factor * gain + shift
        gate = got[slot][:, size:].astype(F32)
        mixed[slot] = low(jax.nn.silu(normed) * jax.nn.silu(gate))
    add_slots(out_ref, [mixed.at[slot] for slot in range(groups)], weights, tops, None)


def conv_out(got, weights):
    groups = len(got)
    rows, both = got[0].shape
    rows, size, width = rows // 2, both // 2, weights[0].shape[1]
    return pl.pallas_call(
        conv_out_kernel,
        in_specs=[whole()] * 16,
        out_specs=whole(),
        out_shape=pltpu.VMEM((rows, width), F32),
        scratch_shapes=[pltpu.VMEM((groups, rows, size), BF16)],
        compiler_params=params(8),
        cost_estimate=cost(2 * rows * 1024 * width, 6 << 20),
        name="conv_out",
    )(*map(near_core, got), *map(near_core, weights))


def delta_out_kernel(conv_ref, *refs):
    got, weights, out_hbm, staged, sems = refs[:8], refs[8:16], refs[16], refs[17], refs[18]
    rows, size = staged.shape[0], got[0].shape[1]
    stores = []
    for n, base in enumerate(range(0, staged.shape[1], 512)):
        here = slice(base, base + 512)
        acc = conv_ref[:, here]
        for slot, (part, ref) in enumerate(zip(got, weights)):
            top = slot % 2 * rows
            acc = acc + dot(part[top : top + rows, :], ref[0:size, here])
        staged[:, here] = low(acc)
        stores += fetch(sems.at[pl.ds(n, 1)], (staged.at[:, here], out_hbm.at[:, here]))
    for one in stores:
        one.wait()


def delta_out(got, conv_part, weights):
    rows, width = conv_part.shape
    return pl.pallas_call(
        delta_out_kernel,
        in_specs=[whole()] * 17,
        out_specs=hbm(),
        out_shape=jax.ShapeDtypeStruct((rows, width), BF16),
        scratch_shapes=[pltpu.VMEM((rows, width), BF16), pltpu.SemaphoreType.DMA((4,))],
        compiler_params=params(8),
        cost_estimate=cost(2 * rows * 1024 * width, 6 << 20),
        name="delta_out",
    )(near_core(conv_part), *map(near_core, got), *map(near_core, weights))


def local(
    tokens,
    w_query,
    w_key,
    w_value,
    w_delta_gate,
    w_glu_value,
    w_glu_gate,
    w_conv_gate,
    w_beta,
    w_decay,
    decay_log,
    head_gain,
    conv_taps,
    ln_gain,
    ln_shift,
    out_delta,
    out_conv,
):
    rows = tokens.shape[0]
    half = rows // 2
    size = w_query.shape[1]
    y, core = lax.axis_index("y"), lax.axis_index("c")
    x, z = lax.axis_index("x"), lax.axis_index("z")
    count_y = lax.axis_size("y")
    head = y * 2 + core
    chips = [y, (y - 1) % count_y, (y + 1) % count_y, (y + 2) % count_y]
    slots = [chip * 2 + side for chip in chips for side in (core, 1 - core)]
    blocks = jnp.stack(slots + [x, z % 4])
    blocks = blocks.astype(jnp.int32)

    beta_decay = jnp.concatenate(
        [
            lax.dynamic_slice_in_dim(w_beta, head, 1, 1),
            lax.dynamic_slice_in_dim(w_decay, head, 1, 1),
            jnp.zeros((w_beta.shape[0], 126), BF16),
        ],
        axis=1,
    )
    weights = (
        w_glu_value,
        w_glu_gate,
        w_delta_gate,
        w_conv_gate,
        w_query,
        w_key,
        w_value,
        beta_decay,
    )
    rate = jnp.exp(lax.dynamic_slice_in_dim(decay_log, head, 1, 0))

    def three(vector):
        high = lax.reduce_precision(vector, 8, 7)
        rest = vector - high
        middle = lax.reduce_precision(rest, 8, 7)
        return [high, middle, rest - middle]

    extra = jnp.stack(three(ln_gain) + three(ln_shift)).astype(BF16)
    extra = jnp.pad(extra, ((0, 10), (0, out_conv.shape[1] - extra.shape[1])))
    last = jnp.concatenate([out_delta, out_conv, extra], axis=0)

    own = tokens
    r1, l1 = cyclic(own, "y", 1), cyclic(own, "y", -1)
    sw = swapped(own)
    blocks, rate, last, beta_decay = lax.optimization_barrier((blocks, rate, last, beta_decay))
    weights = pack(weights[:7] + (beta_decay,))
    r1_top, l1_rest = cut(r1, l1, half)
    fa, fb = cyclic(r1_top, "y", 1), cyclic(l1_rest, "y", -1)
    sr1, sl1 = swapped(r1), swapped(l1)
    sfa, sfb = swapped(fa), swapped(fb)
    pieces = [own, sw, r1, sr1, l1, sl1, fa, sfa, fb, sfb]
    wr, wl = cyclic(last, "y", 1), cyclic(last, "y", -1)
    q, k, v, bl, tail, dg, gu, cg = project(pieces, weights, blocks, rate, 2048, size)

    coef_p, coef_q, state = delta(q, k, v, bl)


    before, total = along(8, blocks, state.shape, state, *(cyclic(state, "x", j) for j in (2, 3, 1)))
    route = lambda j: [(h + i, h + (i + j) % 4) for h in (0, 4) for i in range(4)]
    around = []
    for j in (2, 3, 1):
        around.append(lax.ppermute(total, "z", route(j)))
    before_z, made_z = along(9, blocks, (size, size), total, *around)
    far = shifted(made_z, "z", 4)

    ws = swapped(last)
    wr_top, wl_rest = cut(wr, wl, size)
    wfa, wfb = cyclic(wr_top, "y", 1), cyclic(wl_rest, "y", -1)
    wsr, wsl = swapped(wr), swapped(wl)
    wsfa, wsfb = swapped(wfa), swapped(wfb)
    near = [last, ws, wr, wsr, wl, wsl]
    delta_weights = near + [wfa, wsfa]
    conv_weights = near + [wfb, wsfb]

    halo = lax.ppermute(tail, SP, [(i, i + 1) for i in range(31)])
    filtered = conv(blocks, gu, halo, conv_taps, cg)
    got = exchanged(filtered)
    conv_part = conv_out(got, conv_weights)

    mixed = finish(blocks, coef_p, coef_q, dg, head_gain[None, :], before_z, far, before)
    return delta_out(exchanged(mixed), conv_part, delta_weights)


def solution(mesh):
    finer = Mesh(mesh.devices.reshape(8, 4, 4, 2), ("z", "x", "y", "c"))
    placed = (
        P(SP, TP),
        P(None, TP),
        P(None, TP),
        P(None, TP),
        P(None, TP),
        P(None, TP),
        P(None, TP),
        P(None, TP),
        P(),
        P(),
        P(),
        P(),
        P(None, TP),
        P(TP),
        P(TP),
        P(TP, None),
        P(TP, None),
    )
    return jax.shard_map(
        local, mesh=finer, in_specs=placed, out_specs=P(SP + TP, None), check_vma=False
    )
```
